256 devices in a mesh: sp: 64 (over z, y, core), tp: 4 (over x).
Axes of the slice: x: 4, y: 4, z: 8, core: 2. Of those that a mesh axis runs over, the one named last changes fastest.
Arguments:
- mixer_input: bfloat16 [16384, 1024], P('sp', 'tp'), may hold values from -6 to 6
- retention: float32 [64, 16384], P('tp', 'sp'), may hold values from -1 to 0
- decay_real: float32 [64, 64], P('tp'), may hold values from -0.7 to -0.3
- decay_freq: float32 [64, 64], P('tp'), may hold values from 0 to 26
- log_step: float32 [64], P('tp')
- input_real: float32 [64, 64, 16], P('tp')
- input_imag: float32 [64, 64, 16], P('tp')
- readout_real: float32 [64, 16, 64], P('tp'), may hold values from -0.5 to 0.5
- readout_imaginary: float32 [64, 16, 64], P('tp'), may hold values from -0.5 to 0.5
- skip_weight: float32 [64, 16], P('tp'), may hold values from -4 to 4
- norm_gain: float32 [1024], replicated, may hold values from 0.1 to 1.9
- projection: bfloat16 [1024, 2048], P('tp'), may hold values from -0.1875 to 0.1875
- residual: bfloat16 [16384, 2048], P(('sp', 'tp')), may hold values from -6 to 6
- mix_gain: float32 [2048], replicated, may hold values from 0.1 to 1.9
- routes: int32 [16384, 2], P(('sp', 'tp')), may hold values from 0 to 63, all different within a row; in each aligned block of 64 rows (0 to 63, 64 to 127, ...) at most 4 rows name the same one
- route_weight: float32 [16384, 2], P(('sp', 'tp')), may hold values from 0.5 to 2
- expert_gate: bfloat16 [64, 2048, 512], P('sp'), may hold values from -0.125 to 0.125
- expert_up: bfloat16 [64, 2048, 512], P('sp'), may hold values from -0.125 to 0.125
- expert_down: bfloat16 [64, 512, 2048], P('sp'), may hold values from -0.25 to 0.25
- final_gain: float32 [2048], replicated, may hold values from 0.1 to 1.9
Outputs:
- layer_out: bfloat16 [16384, 2048], P(('sp', 'tp'))
The draws below stay inside these ranges and needn't reach their ends.
Inputs may be any that keep to these rules, and one draw needn't show every extreme that they name: `routes`: in each aligned block of 64 rows no expert is named by more than 4 rows, and in some blocks one is named by exactly 4 rows; each row names 2 different experts.
All inputs are finite; a program needn't handle non-finite values.
Results may differ from the reference program's by a relative error of at most 0.017.
Values may be sent and summed in bfloat16 or wider, within the bound.
A program may use at most 64 MiB of HBM per device.

```python
import math
import jax
import jax.numpy as jnp
import numpy as np
from jax import lax

WIDTH = 2048
GROUPS = 64
CHANNELS = 16
STATE = 64
EXPERT_HIDDEN = 512
PICKS = 2
SHARD_TOKENS = 256
MIX_WIDTH = 1024
SEQUENCE_TOKENS = 16384
DEVICE_ROWS = 64
EXPERTS = 64
CAPACITY = 4


def decay_plan(key):
    folded_values = jax.random.fold_in(key, 7)
    slow_share = 0.5
    slow_group = jax.random.uniform(jax.random.fold_in(folded_values, 1), (GROUPS,), jnp.float32) < slow_share
    decay_real = -jax.random.uniform(jax.random.fold_in(folded_values, 2), (GROUPS, STATE), jnp.float32, 0.3, 0.7)
    decay_freq = jax.random.uniform(jax.random.fold_in(folded_values, 3), (GROUPS, STATE), jnp.float32, 0.0, 8.0 * math.pi)
    fast_log = jax.random.uniform(jax.random.fold_in(folded_values, 4), (GROUPS,), jnp.float32, math.log(0.04), math.log(0.12))
    slow_log = jax.random.uniform(jax.random.fold_in(folded_values, 5), (GROUPS,), jnp.float32, math.log(0.2 / SEQUENCE_TOKENS), math.log(0.6 / SEQUENCE_TOKENS))
    log_step = jnp.where(slow_group, slow_log, fast_log)
    stride = jnp.exp(log_step)[:, None]
    growth = decay_real * stride
    turning = decay_freq * stride
    upper_real = jnp.expm1(growth) * jnp.cos(turning) - 2.0 * jnp.sin(0.5 * turning) ** 2
    upper_imag = jnp.exp(growth) * jnp.sin(turning)
    magnitude = jnp.sqrt(upper_real * upper_real + upper_imag * upper_imag)
    magnitude = magnitude / jnp.sqrt(decay_real * decay_real + decay_freq * decay_freq)
    scaling = jnp.sqrt(-2.0 * growth) / magnitude / math.sqrt(CHANNELS)
    return (decay_real, decay_freq, log_step, scaling)


def draw_decay_real(key, part):
    return decay_plan(key)[0]


def draw_decay_freq(key, part):
    return decay_plan(key)[1]


def draw_log_step(key, part):
    return decay_plan(key)[2]


def draw_input_real(key, part):
    scaling = decay_plan(key)[3]
    return scaling[:, :, None] * jax.random.normal(jax.random.fold_in(key, 21), (GROUPS, STATE, CHANNELS), jnp.float32)


def draw_input_imag(key, part):
    scaling = decay_plan(key)[3]
    return scaling[:, :, None] * jax.random.normal(jax.random.fold_in(key, 22), (GROUPS, STATE, CHANNELS), jnp.float32)


def draw_retention(key, part):
    folded_values = jax.random.fold_in(key, 13)
    blocks = SEQUENCE_TOKENS // SHARD_TOKENS
    factor = jnp.exp(jax.random.uniform(jax.random.fold_in(folded_values, 1), (GROUPS, blocks), jnp.float32, 0.0, math.log(4.0)))
    roughness = jax.random.uniform(jax.random.fold_in(folded_values, 2), (GROUPS, SEQUENCE_TOKENS), jnp.float32, 0.5, 1.5)
    base_level = 0.2
    steady_state = -(base_level / SEQUENCE_TOKENS) * jnp.repeat(factor, SHARD_TOKENS, axis=1) * roughness
    spike_locations = jax.random.randint(jax.random.fold_in(folded_values, 3), (3,), 0, SEQUENCE_TOKENS)
    loss_values = jnp.log(jax.random.uniform(jax.random.fold_in(folded_values, 4), (3, GROUPS), jnp.float32, 0.65, 0.8))
    spike_mask = (jnp.arange(SEQUENCE_TOKENS)[None, :] == spike_locations[:, None]).astype(jnp.float32)
    return steady_state + jnp.einsum('aw,ay->wy', loss_values, spike_mask)


def steps_of(rng, dims, pieces, low, largest):
    loudness, own = 1.0, jax.random.fold_in(rng, 6)
    for dim, parts in pieces:
        heights = jnp.exp(jax.random.uniform(jax.random.fold_in(own, dim), (parts,), jnp.float32, low / len(pieces), largest / len(pieces)))
        loudness = loudness * jnp.repeat(heights, dims[dim] // parts).reshape([-1 if axis == dim else 1 for axis in range(len(dims))])
    return loudness


def shared_out(rng, own, number, rows, amount, top, most, skew):
    sequence = jax.random.permutation(rng, amount)
    heavy_load, usual = portions_of(amount, rows * top, most, skew, True), portions_of(amount, rows * top, most, skew, False)
    places = jnp.arange(amount)

    def named(tallies, turn):
        used = int((tallies > 0).sum())
        fixed = max(1, used // 4)
        moved = fixed + (places - fixed + turn * (used - fixed)) % max(1, amount - fixed)
        return jnp.zeros((amount,), jnp.int32).at[sequence[jnp.where(places < fixed, places, moved)]].set(jnp.asarray(tallies, jnp.int32))

    tallies = jnp.where(number % 4 == 0, named(heavy_load, number // 4), named(usual, number - number // 4 - 1))
    mixed = jax.random.permutation(jax.random.fold_in(own, 3), amount)
    source_of, receiver = mixed[0:amount // 2 * 2:2], mixed[1:amount // 2 * 2:2]
    margin = jnp.minimum(tallies[source_of] - 1, most - tallies[receiver]) // 2
    margin = jnp.where((source_of == sequence[0]) | (receiver == sequence[0]) | (tallies[receiver] == 0), 0, jnp.maximum(margin, 0))
    moved = jax.random.randint(jax.random.fold_in(own, 4), (amount // 2,), 0, 1 << 20) % (margin + 1)
    tallies = tallies.at[source_of].add(-moved).at[receiver].add(moved)
    labels = jnp.searchsorted(jnp.cumsum(tallies), jnp.arange(rows * top), side="right").astype(jnp.int32)
    listing = labels.reshape(top, rows).T
    listing = listing[jax.random.permutation(jax.random.fold_in(own, 1), rows)]
    turn = jax.random.randint(jax.random.fold_in(own, 2), (rows, 1), 0, top)
    return jnp.take_along_axis(listing, (jnp.arange(top)[None, :] + turn) % top, axis=1)


def portions_of(amount, total, most, slope, full):
    loads = [(1 << 20) // math.isqrt(rank ** slope) + 1 for rank in range(1, amount + 1)]
    largest = most if full else min(most, max(-(-total // amount), total * loads[0] // sum(loads)))
    least = 1 if total - largest >= amount - 1 else 0
    given, surplus = [largest] + [least] * (amount - 1), total - largest - least * (amount - 1)
    while surplus > 0:
        candidates = [i for i in range(1, amount) if given[i] < largest] or [i for i in range(1, amount) if given[i] < most]
        mass, budget = sum([loads[i] for i in candidates]), surplus
        for i in candidates:
            more = min(most - given[i], max(1, budget * loads[i] // mass), surplus)
            given[i] = given[i] + more
            surplus = surplus - more
    return np.array(given)


def noise(own_key, shape, width, reach, split=(), kind=jnp.bfloat16):
    gain = steps_of(own_key, shape, split, -0.22, 0.18) if split else 1.0
    drawn = jax.random.normal(own_key, shape, jnp.float32) * width * gain
    return jnp.minimum(jnp.maximum(drawn, -reach), reach).astype(kind)


def setup_inputs(seed: int = 0) -> dict:
    seeds = jax.random.split(jax.random.key(seed), 21)
    mixer_input = noise(seeds[0], (SEQUENCE_TOKENS, MIX_WIDTH), 1.0, 6.0, ((0, 64), (1, 4)))
    retention = draw_retention(jax.random.fold_in(seeds[20], 71), 0)
    decay_real = draw_decay_real(jax.random.fold_in(seeds[20], 71), 0)
    decay_freq = draw_decay_freq(jax.random.fold_in(seeds[20], 71), 0)
    log_step = draw_log_step(jax.random.fold_in(seeds[20], 71), 0)
    input_real = draw_input_real(jax.random.fold_in(seeds[20], 71), 0)
    input_imag = draw_input_imag(jax.random.fold_in(seeds[20], 71), 0)
    readout_real = noise(seeds[7], (GROUPS, CHANNELS, STATE), (2 * STATE) ** -0.5, 0.5, ((0, 4),), jnp.float32)
    readout_imaginary = noise(seeds[8], (GROUPS, CHANNELS, STATE), (2 * STATE) ** -0.5, 0.5, ((0, 4),), jnp.float32)
    skip_weight = noise(seeds[9], (GROUPS, CHANNELS), 1.0, 4.0, ((0, 4),), jnp.float32)
    norm_gain = jnp.clip(1.0 + 0.18 * jax.random.normal(seeds[10], (MIX_WIDTH,), jnp.float32), 0.1, 1.9)
    projection = noise(seeds[11], (MIX_WIDTH, WIDTH), MIX_WIDTH ** -0.5, 0.1875, ((0, 4),))
    residual = noise(seeds[12], (SEQUENCE_TOKENS, WIDTH), 1.0, 6.0, ((0, 256),))
    mix_gain = jnp.clip(1.0 + 0.18 * jax.random.normal(seeds[13], (WIDTH,), jnp.float32), 0.1, 1.9)
    routes_keys = jax.random.split(jax.random.fold_in(seeds[14], 1), SEQUENCE_TOKENS // DEVICE_ROWS)
    routes_turns = jax.random.permutation(jax.random.fold_in(seeds[14], 3), SEQUENCE_TOKENS // DEVICE_ROWS)
    routes = jax.vmap(lambda own, number: shared_out(jax.random.fold_in(seeds[14], 2), own, number, DEVICE_ROWS, EXPERTS, PICKS, CAPACITY, 2))(routes_keys, routes_turns).reshape((SEQUENCE_TOKENS, PICKS))
    route_weight = jnp.clip(0.5 + 1.5 * jax.random.uniform(seeds[15], (SEQUENCE_TOKENS, PICKS), jnp.float32) ** steps_of(seeds[15], (SEQUENCE_TOKENS, PICKS), ((0, 256),), -0.2, 0.2), 0.5, 2.0)
    expert_gate = noise(seeds[16], (EXPERTS, WIDTH, EXPERT_HIDDEN), WIDTH ** -0.5, 0.125, ((0, 64),))
    expert_up = noise(seeds[17], (EXPERTS, WIDTH, EXPERT_HIDDEN), WIDTH ** -0.5, 0.125, ((0, 64),))
    expert_down = noise(seeds[18], (EXPERTS, EXPERT_HIDDEN, WIDTH), EXPERT_HIDDEN ** -0.5, 0.25, ((0, 64),))
    final_gain = jnp.clip(1.0 + 0.18 * jax.random.normal(seeds[19], (WIDTH,), jnp.float32), 0.1, 1.9)
    return dict(mixer_input=mixer_input, retention=retention, decay_real=decay_real, decay_freq=decay_freq, log_step=log_step, input_real=input_real, input_imag=input_imag, readout_real=readout_real, readout_imaginary=readout_imaginary, skip_weight=skip_weight, norm_gain=norm_gain, projection=projection, residual=residual, mix_gain=mix_gain, routes=routes, route_weight=route_weight, expert_gate=expert_gate, expert_up=expert_up, expert_down=expert_down, final_gain=final_gain)


deep_alpha = 2.0 ** 0.25
highest_precision = lax.Precision.HIGHEST
row_block = 512

def input_factor(decay_real, decay_freq, log_step):
    stride = jnp.exp(log_step)[:, None]
    growth = decay_real * stride
    turning = decay_freq * stride
    upper_real = jnp.expm1(growth) * jnp.cos(turning) - 2.0 * jnp.sin(0.5 * turning) ** 2
    upper_imag = jnp.exp(growth) * jnp.sin(turning)
    denominator = decay_real * decay_real + decay_freq * decay_freq
    factor_real = (upper_real * decay_real + upper_imag * decay_freq) / denominator
    factor_imag = (upper_imag * decay_real - upper_real * decay_freq) / denominator
    return (growth, turning, factor_real, factor_imag)

def layer_norm(values, scales):
    centered = values - lax.optimization_barrier(jnp.mean(values, axis=-1, keepdims=True))
    variance = lax.optimization_barrier(jnp.mean(centered * centered, axis=-1, keepdims=True))
    return centered * lax.rsqrt(variance + 1e-05) * scales

def reference(mixer_input, retention, decay_real, decay_freq, log_step, input_real, input_imag, readout_real, readout_imaginary, skip_weight, norm_gain, projection, residual, mix_gain, routes, route_weight, expert_gate, expert_up, expert_down, final_gain):
    growth, turning, factor_real, factor_imag = input_factor(decay_real, decay_freq, log_step)
    keep_real = jnp.exp(growth) * jnp.cos(turning)
    keep_imag = jnp.exp(growth) * jnp.sin(turning)
    bar_real = factor_real[:, :, None] * input_real - factor_imag[:, :, None] * input_imag
    bar_imag = factor_real[:, :, None] * input_imag + factor_imag[:, :, None] * input_real
    inputs = mixer_input.reshape(SEQUENCE_TOKENS, GROUPS, CHANNELS)
    held_log = jnp.transpose(retention)

    def advance(carried, position):
        state_real_part, state_imaginary = carried
        current, kept_log = position
        current = current.astype(jnp.float32)
        shrink = jnp.exp(kept_log)[:, None]
        drive_real = jnp.einsum('gpc,gc->gp', bar_real, current, precision=highest_precision)
        drive_imag = jnp.einsum('gpc,gc->gp', bar_imag, current, precision=highest_precision)
        following_real = shrink * (keep_real * state_real_part - keep_imag * state_imaginary) + drive_real
        following_imaginary = shrink * (keep_real * state_imaginary + keep_imag * state_real_part) + drive_imag
        readout_result = jnp.einsum('zhy,zy->zh', readout_real, following_real, precision=highest_precision)
        readout_result = readout_result - jnp.einsum('zhy,zy->zh', readout_imaginary, following_imaginary, precision=highest_precision)
        readout_result = readout_result + skip_weight * current
        return ((following_real, following_imaginary), jax.nn.gelu(readout_result).astype(jnp.bfloat16))
    zero_state = jnp.zeros((GROUPS, STATE), jnp.float32)
    ignored_state, mixed_seq = lax.scan(advance, (zero_state, zero_state), (inputs, held_log))
    mixed_seq = mixed_seq.reshape(SEQUENCE_TOKENS, MIX_WIDTH)
    mixed_float = mixed_seq.astype(jnp.float32)
    row_square = lax.optimization_barrier(jnp.mean(mixed_float * mixed_float, axis=1))
    scaled = (mixed_float * norm_gain).astype(jnp.bfloat16)
    mix = jnp.dot(scaled, projection, preferred_element_type=jnp.float32) * lax.rsqrt(row_square + 1e-06)[:, None]
    hidden = layer_norm(deep_alpha * residual.astype(jnp.float32) + mix, mix_gain).astype(jnp.bfloat16)
    hidden_pad = jnp.concatenate([hidden, jnp.zeros((1, WIDTH), hidden.dtype)], axis=0)
    assigned = routes.reshape(-1).astype(jnp.int32)
    sort_order = jnp.argsort(assigned, stable=True).astype(jnp.int32)
    sorted_expert = assigned[sort_order]
    sorted_token = (sort_order // PICKS).astype(jnp.int32)
    sorted_weight = route_weight.reshape(-1)[sort_order]
    expert_load = lax.optimization_barrier(jnp.sum((assigned[:, None] == jnp.arange(EXPERTS, dtype=jnp.int32)[None, :]).astype(jnp.int32), axis=0))
    padded_rows = (expert_load + row_block - 1) // row_block * row_block
    padded_end = jnp.cumsum(padded_rows).astype(jnp.int32)
    padded_start = padded_end - padded_rows
    first_sorted = (jnp.cumsum(expert_load) - expert_load).astype(jnp.int32)
    assigned_count = SEQUENCE_TOKENS * PICKS
    dest_slot = padded_start[sorted_expert] + jnp.arange(assigned_count, dtype=jnp.int32) - first_sorted[sorted_expert]
    block_total = (assigned_count + EXPERTS * row_block) // row_block + 1
    buffer_rows = block_total * row_block
    token_buffer = jnp.full((buffer_rows,), SEQUENCE_TOKENS, jnp.int32).at[dest_slot].set(sorted_token)
    weight_buffer = jnp.zeros((buffer_rows,), route_weight.dtype).at[dest_slot].set(sorted_weight)
    block_starts = jnp.arange(block_total, dtype=jnp.int32) * row_block
    block_expert = lax.optimization_barrier(jnp.sum((padded_end[None, :] <= block_starts[:, None]).astype(jnp.int32), axis=1))
    block_expert = jnp.minimum(block_expert, EXPERTS - 1).astype(jnp.int32)

    def one_block(running, block_items):
        tokens_here, weights_here, expert_here = block_items
        rows_here = hidden_pad[tokens_here]
        gate_act = jnp.dot(rows_here, expert_gate[expert_here], preferred_element_type=jnp.float32)
        up_act = jnp.dot(rows_here, expert_up[expert_here], preferred_element_type=jnp.float32)
        active = (jax.nn.silu(gate_act) * up_act).astype(jnp.bfloat16)
        produced = jnp.dot(active, expert_down[expert_here], preferred_element_type=jnp.float32).astype(jnp.bfloat16)
        return (running.at[tokens_here].add(weights_here[:, None] * produced.astype(jnp.float32)), None)
    mix_init = jnp.zeros((SEQUENCE_TOKENS + 1, WIDTH), jnp.float32)
    expert_mix, ignored = lax.scan(one_block, mix_init, (token_buffer.reshape(block_total, row_block), weight_buffer.reshape(block_total, row_block), block_expert))
    layer_out = layer_norm(deep_alpha * hidden.astype(jnp.float32) + expert_mix[:SEQUENCE_TOKENS], final_gain)
    return layer_out.astype(jnp.bfloat16)
```

```python
import jax
import jax.numpy as jnp
from jax import lax
from jax.experimental import pallas as pl
from jax.experimental.pallas import tpu as pltpu
from jax.sharding import PartitionSpec as P

PICKS = 2
MIX_WIDTH = 1024
MESH = pl.DeviceIdType.MESH

deep_alpha = 2.0**0.25

TOKENS = 256
GROUPS = 16
CHANNELS = 16
STATE = 64
WIDTH = 2048
ROWS = 64
PLANES = 8
PLANE = 8
TP = 4
PIECE = 64


def times(ar, ai, br, bi):
    return ar * br - ai * bi, ar * bi + ai * br


def layer_norm(values, scales):
    centered = values - jnp.mean(values, axis=-1, keepdims=True)
    variance = jnp.mean(centered * centered, axis=-1, keepdims=True)
    return centered * lax.rsqrt(variance + 1e-05) * scales


def pair_rows(ref):
    return jnp.concatenate(
        [ref[pl.ds(0, 8, stride=2), :], ref[pl.ds(1, 8, stride=2), :]], axis=1
    )


def remote(src, dst, send_sem, recv_sem, **where):
    return pltpu.make_async_remote_copy(
        src_ref=src,
        dst_ref=dst,
        send_sem=send_sem,
        recv_sem=recv_sem,
        device_id=where,
        device_id_type=MESH,
    )


def mixer_kernel(
    x_ref,
    ret_ref,
    real_ref,
    freq_ref,
    step_ref,
    in_real_ref,
    in_imag_ref,
    out_real_ref,
    out_imag_ref,
    skip_ref,
    gain_ref,
    proj_ref,
    residual_ref,
    mix_gain_ref,
    hidden_ref,
    drive_w,
    read_w,
    drive_re,
    drive_im,
    shrink,
    states,
    mine,
    plane_buf,
    plane_sum,
    column_buf,
    mixed,
    whole,
    gathered,
    param_buf,
    plane_send,
    plane_recv,
    column_send,
    column_recv,
    tp_send,
    tp_recv,
    own_sem,
    ring_send,
    ring_recv,
    twin_send,
    twin_recv,
):
    sp = lax.axis_index("sp")
    tp = lax.axis_index("tp")
    plane = lax.div(sp, PLANE)
    place = lax.rem(sp, PLANE)
    core = lax.rem(sp, 2)
    twin = sp + 1 - 2 * core
    right = lax.rem(tp + 1, TP)
    left = lax.rem(tp + TP - 1, TP)
    across = lax.rem(tp + 2, TP)

    barrier = pltpu.get_barrier_semaphore()

    def greet_plane(k, _):
        peer = plane * PLANE + lax.rem(place + k, PLANE)
        pl.semaphore_signal(barrier, inc=1, device_id={"sp": peer}, device_id_type=MESH)
        return 0

    def greet_column(k, _):
        peer = lax.rem(plane + k, PLANES) * PLANE + place
        pl.semaphore_signal(barrier, inc=1, device_id={"sp": peer}, device_id_type=MESH)
        return 0

    def greet_tp(k, _):
        pl.semaphore_signal(
            barrier, inc=1, device_id={"tp": lax.rem(tp + k, TP)}, device_id_type=MESH
        )
        return 0

    lax.fori_loop(1, TP, greet_tp, 0)
    lax.fori_loop(1, PLANE, greet_plane, 0)
    lax.fori_loop(1, PLANES, greet_column, 0)

    own_copy = pltpu.make_async_copy(proj_ref, gathered.at[tp], own_sem)
    own_copy.start()

    group_row = lax.broadcasted_iota(jnp.int32, (GROUPS, STATE), 0)
    log_step = jnp.zeros((GROUPS, STATE), jnp.float32)
    for g in range(GROUPS):
        log_step = jnp.where(group_row == g, step_ref[g], log_step)
    stride = jnp.exp(log_step)
    decay_real = real_ref[...]
    decay_freq = freq_ref[...]
    growth = decay_real * stride
    turning = decay_freq * stride
    grown = jnp.exp(growth)
    cosine = jnp.cos(turning)
    sine = jnp.sin(turning)
    half_sine = jnp.sin(0.5 * turning)
    expm1 = jnp.tanh(0.5 * growth) * (grown + 1.0)
    upper_real = expm1 * cosine - 2.0 * half_sine * half_sine
    upper_imag = grown * sine
    denominator = decay_real * decay_real + decay_freq * decay_freq
    factor_real = (upper_real * decay_real + upper_imag * decay_freq) / denominator
    factor_imag = (upper_imag * decay_real - upper_real * decay_freq) / denominator
    param_buf[0] = grown * cosine
    param_buf[1] = grown * sine
    keep_re = pair_rows(param_buf.at[0])
    keep_im = pair_rows(param_buf.at[1])

    nothing = jnp.zeros((CHANNELS, STATE), jnp.float32)
    drive_w[...] = jnp.zeros(drive_w.shape, jnp.bfloat16)
    for g in range(GROUPS):
        rows = pl.ds(g * CHANNELS, CHANNELS)
        b_re = jnp.transpose(in_real_ref[g])
        b_im = jnp.transpose(in_imag_ref[g])
        c_re = out_real_ref[g]
        c_im = out_imag_ref[g]
        f_re = factor_real[g : g + 1, :]
        f_im = factor_imag[g : g + 1, :]
        r_re = c_re * f_re - c_im * f_im
        r_im = -(c_re * f_im + c_im * f_re)
        if g % 2 == 0:
            b_row = [b_re, nothing, b_im, nothing]
            r_row = [r_re, nothing, r_im, nothing]
        else:
            b_row = [nothing, b_re, nothing, b_im]
            r_row = [nothing, r_re, nothing, r_im]
        b_row = jnp.concatenate(b_row, axis=1)
        drive_w[g // 2, rows, :] = b_row.astype(jnp.bfloat16)
        read_w[rows, :] = jnp.concatenate(r_row, axis=1).astype(jnp.bfloat16)

    kept = jnp.transpose(jnp.exp(ret_ref[...]))
    kept_hi = kept.astype(jnp.bfloat16)
    rest = kept - kept_hi.astype(jnp.float32)
    kept_mid = rest.astype(jnp.bfloat16)
    kept_lo = (rest - kept_mid.astype(jnp.float32)).astype(jnp.bfloat16)
    select_row = lax.broadcasted_iota(jnp.int32, (GROUPS, 8 * 128), 0)
    select_lane = lax.broadcasted_iota(jnp.int32, (GROUPS, 8 * 128), 1)
    select = (select_row == lax.div(select_lane, STATE)).astype(jnp.bfloat16)
    spread = (
        jnp.dot(kept_hi, select, preferred_element_type=jnp.float32)
        + jnp.dot(kept_mid, select, preferred_element_type=jnp.float32)
        + jnp.dot(kept_lo, select, preferred_element_type=jnp.float32)
    )
    x = x_ref[...]
    for j in range(8):
        at = pl.ds(j, TOKENS, stride=8)
        driven = jnp.dot(x, drive_w[j], preferred_element_type=jnp.float32)
        drive_re[at, :] = driven[:, :128]
        drive_im[at, :] = driven[:, 128:]
        shrink[at, :] = spread[:, j * 128 : (j + 1) * 128]

    pl.semaphore_wait(barrier, (TP - 1) + (PLANE - 1) + (PLANES - 1))

    half = core * (2 * PIECE)
    piece_lo = pl.ds(pl.multiple_of(half, PIECE), PIECE)
    piece_hi = pl.ds(pl.multiple_of(half + PIECE, PIECE), PIECE)

    def ring(block, piece, way, slot):
        to = right if way == 0 else left
        return remote(
            gathered.at[block, piece, :],
            gathered.at[block, piece, :],
            ring_send.at[slot],
            ring_recv.at[slot],
            tp=to,
        )

    own_copy.wait()
    to_right_lo = ring(tp, piece_lo, 0, 0)
    to_left_hi = ring(tp, piece_hi, 1, 1)
    to_right_hi = ring(tp, piece_hi, 0, 2)
    to_left_lo = ring(tp, piece_lo, 1, 3)
    to_right_lo.start()
    to_left_hi.start()
    to_right_hi.start()
    to_left_lo.start()

    def advance(t, carried):
        s_re, s_im, decay = carried
        row = pl.ds(pl.multiple_of(t * 8, 8), 8)
        shr = shrink[row, :]
        a_re = shr * keep_re
        a_im = shr * keep_im
        n_re = (a_re * s_re - a_im * s_im) + drive_re[row, :]
        n_im = (a_re * s_im + a_im * s_re) + drive_im[row, :]
        return n_re, n_im, decay * shr

    zero = jnp.zeros((8, 128), jnp.float32)
    one = jnp.ones((8, 128), jnp.float32)
    end_re, end_im, decay = lax.fori_loop(0, TOKENS, advance, (zero, zero, one), unroll=8)
    mine[0] = end_re
    mine[1] = end_im
    mine[2] = decay

    power_re, power_im = keep_re, keep_im
    for _ in range(8):
        power_re, power_im = times(power_re, power_im, power_re, power_im)
    plane_re, plane_im = power_re, power_im
    for _ in range(3):
        plane_re, plane_im = times(plane_re, plane_im, plane_re, plane_im)

    def plane_copy(k):
        peer = plane * PLANE + lax.rem(place + k, PLANE)
        return remote(mine, plane_buf.at[place], plane_send.at[k], plane_recv.at[place], sp=peer)

    def send_plane(k, _):
        plane_copy(k).start()
        return 0

    def plane_arrived(k, _):
        source = lax.rem(place + k, PLANE)
        remote(
            mine, plane_buf.at[source], plane_send.at[k], plane_recv.at[source], sp=plane * PLANE + source
        ).wait_recv()
        return 0

    lax.fori_loop(1, PLANE, send_plane, 0)
    lax.fori_loop(1, PLANE, plane_arrived, 0)
    plane_buf[place] = mine[...]

    def join(buf, k, carried, p_re, p_im):
        s_re, s_im, decay = carried
        d = buf[k, 2]
        m_re, m_im = times(d * p_re, d * p_im, s_re, s_im)
        return m_re + buf[k, 0], m_im + buf[k, 1], decay * d

    def join_place(k, carried):
        return join(plane_buf, k, carried, power_re, power_im)

    total = lax.fori_loop(0, PLANE, join_place, (zero, zero, one))
    plane_sum[0] = total[0]
    plane_sum[1] = total[1]
    plane_sum[2] = total[2]

    def column_copy(p):
        return remote(
            plane_sum, column_buf.at[plane], column_send.at[p], column_recv.at[plane], sp=p * PLANE + place
        )

    def send_column(p, _):
        column_copy(p).start()
        return 0

    def column_arrived(p, _):
        remote(
            plane_sum, column_buf.at[p], column_send.at[p], column_recv.at[p], sp=p * PLANE + place
        ).wait_recv()
        return 0

    lax.fori_loop(plane + 1, PLANES, send_column, 0)

    def twin_copy(block, piece, slot):
        return remote(
            gathered.at[block, piece, :],
            gathered.at[block, piece, :],
            twin_send.at[slot],
            twin_recv.at[slot],
            sp=twin,
        )

    from_left_lo = ring(left, piece_lo, 0, 0)
    from_right_hi = ring(right, piece_hi, 1, 1)
    from_left_hi = ring(left, piece_hi, 0, 2)
    from_right_lo = ring(right, piece_lo, 1, 3)
    from_left_lo.wait_recv()
    pass_right = ring(left, piece_lo, 0, 4)
    pass_right.start()
    from_right_hi.wait_recv()
    pass_left = ring(right, piece_hi, 1, 5)
    pass_left.start()
    twin_left_lo = twin_copy(left, piece_lo, 0)
    twin_right_hi = twin_copy(right, piece_hi, 1)
    twin_left_lo.start()
    twin_right_hi.start()

    lax.fori_loop(0, plane, column_arrived, 0)

    def join_plane(p, carried):
        return join(column_buf, p, carried, plane_re, plane_im)

    carried = lax.fori_loop(0, plane, join_plane, (zero, zero, one))
    carried = lax.fori_loop(0, place, join_place, carried)

    def record(t, carried):
        s_re, s_im = carried
        row = pl.ds(pl.multiple_of(t * 8, 8), 8)
        shr = shrink[row, :]
        a_re = shr * keep_re
        a_im = shr * keep_im
        n_re = (a_re * s_re - a_im * s_im) + drive_re[row, :]
        n_im = (a_re * s_im + a_im * s_re) + drive_im[row, :]
        states[row, :128] = n_re
        states[row, 128:] = n_im
        return n_re, n_im

    lax.fori_loop(0, TOKENS, record, (carried[0], carried[1]), unroll=8)

    def read(k, _):
        at = pl.ds(pl.multiple_of(k * 256, 256), 256)
        product = lax.dot_general(
            states[at, :].astype(jnp.bfloat16),
            read_w[...],
            (((1,), (1,)), ((), ())),
            preferred_element_type=jnp.float32,
        )
        drive_re[at, :] = product[:, :128]
        drive_im[at, :] = product[:, 128:]
        return 0

    lax.fori_loop(0, 8, read, 0)
    lane = lax.broadcasted_iota(jnp.int32, (TOKENS, 128), 1)
    for side, buf in ((0, drive_re), (1, drive_im)):
        picked = jnp.zeros((TOKENS, 128), jnp.float32)
        for j in range(4):
            value = buf[pl.ds(side * 4 + j, TOKENS, stride=8), :]
            picked = jnp.where(lax.div(lane, 32) == j, value, picked)
        skip = jnp.concatenate([skip_ref[g : g + 1, :] for g in range(side * 8, side * 8 + 8)], axis=1)
        lanes = slice(side * 128, side * 128 + 128)
        read_out = picked + skip * x_ref[:, lanes].astype(jnp.float32)
        mixed[:, lanes] = jax.nn.gelu(read_out).astype(jnp.bfloat16)

    def tp_copy(k):
        peer = lax.rem(tp + k, TP)
        rows = pl.ds(pl.multiple_of(peer * ROWS, ROWS), ROWS)
        return remote(mixed.at[rows, :], whole.at[tp], tp_send.at[k], tp_recv.at[tp], tp=peer)

    def send_tp(k, _):
        tp_copy(k).start()
        return 0

    def tp_arrived(k, _):
        source = lax.rem(tp + k, TP)
        rows = pl.ds(pl.multiple_of(tp * ROWS, ROWS), ROWS)
        remote(mixed.at[rows, :], whole.at[source], tp_send.at[k], tp_recv.at[source], tp=source).wait_recv()
        return 0

    lax.fori_loop(1, TP, send_tp, 0)
    whole[tp] = mixed[pl.ds(pl.multiple_of(tp * ROWS, ROWS), ROWS), :]

    from_left_hi.wait_recv()
    from_right_lo.wait_recv()
    twin_left_hi = twin_copy(left, piece_hi, 2)
    twin_right_lo = twin_copy(right, piece_lo, 3)
    twin_left_hi.start()
    twin_right_lo.start()
    across_lo = ring(across, piece_lo, 0, 4)
    across_hi = ring(across, piece_hi, 1, 5)
    across_lo.wait_recv()
    twin_across_lo = twin_copy(across, piece_lo, 4)
    twin_across_lo.start()
    across_hi.wait_recv()
    twin_across_hi = twin_copy(across, piece_hi, 5)
    twin_across_hi.start()

    other = 2 * PIECE - half
    other_lo = pl.ds(pl.multiple_of(other, PIECE), PIECE)
    other_hi = pl.ds(pl.multiple_of(other + PIECE, PIECE), PIECE)
    lax.fori_loop(1, TP, tp_arrived, 0)
    for slot, (block, piece) in enumerate(
        (
            (left, other_lo),
            (right, other_hi),
            (left, other_hi),
            (right, other_lo),
            (across, other_lo),
            (across, other_hi),
        )
    ):
        twin_copy(block, piece, slot).wait_recv()

    squares = jnp.zeros((ROWS, 1), jnp.float32)
    scaled = []
    for q in range(TP):
        rows = whole[q].astype(jnp.float32)
        squares += jnp.sum(rows * rows, axis=1, keepdims=True)
        scaled.append((rows * gain_ref[:, q * 256 : (q + 1) * 256]).astype(jnp.bfloat16))
    inverse = lax.rsqrt(squares / MIX_WIDTH + 1e-06)
    mix = jnp.zeros((ROWS, WIDTH), jnp.float32)
    for q in range(TP):
        mix += jnp.dot(scaled[q], gathered[q], preferred_element_type=jnp.float32)
    mix = deep_alpha * residual_ref[...].astype(jnp.float32) + mix * inverse
    hidden_ref[...] = layer_norm(mix, mix_gain_ref[...]).astype(jnp.bfloat16)

    def plane_left(k, _):
        plane_copy(k).wait_send()
        return 0

    def column_left(p, _):
        column_copy(p).wait_send()
        return 0

    def tp_left(k, _):
        tp_copy(k).wait_send()
        return 0

    lax.fori_loop(1, PLANE, plane_left, 0)
    lax.fori_loop(plane + 1, PLANES, column_left, 0)
    lax.fori_loop(1, TP, tp_left, 0)
    for copy in (to_right_lo, to_left_hi, to_right_hi, to_left_lo, pass_right, pass_left):
        copy.wait_send()
    for copy in (twin_left_lo, twin_right_hi, twin_left_hi, twin_right_lo, twin_across_lo, twin_across_hi):
        copy.wait_send()


def mixer(
    mixer_input,
    retention,
    decay_real,
    decay_freq,
    log_step,
    input_real,
    input_imag,
    readout_real,
    readout_imaginary,
    skip_weight,
    norm_gain,
    projection,
    residual,
    mix_gain,
):
    vmem = pl.BlockSpec(memory_space=pltpu.VMEM)
    smem = pl.BlockSpec(memory_space=pltpu.SMEM)
    hbm = pl.BlockSpec(memory_space=pltpu.HBM)
    f32 = jnp.float32
    bf16 = jnp.bfloat16
    dma = pltpu.SemaphoreType.DMA
    return pl.pallas_call(
        mixer_kernel,
        out_shape=jax.ShapeDtypeStruct((ROWS, WIDTH), bf16),
        in_specs=[vmem, vmem, vmem, vmem, smem, vmem, vmem, vmem, vmem, vmem, vmem, hbm, vmem, vmem],
        out_specs=vmem,
        scratch_shapes=[
            pltpu.VMEM((8, 256, 256), bf16),
            pltpu.VMEM((256, 256), bf16),
            pltpu.VMEM((TOKENS * 8, 128), f32),
            pltpu.VMEM((TOKENS * 8, 128), f32),
            pltpu.VMEM((TOKENS * 8, 128), f32),
            pltpu.VMEM((TOKENS * 8, 256), f32),
            pltpu.VMEM((3, 8, 128), f32),
            pltpu.VMEM((PLANE, 3, 8, 128), f32),
            pltpu.VMEM((3, 8, 128), f32),
            pltpu.VMEM((PLANES, 3, 8, 128), f32),
            pltpu.VMEM((TOKENS, 256), bf16),
            pltpu.VMEM((TP, ROWS, 256), bf16),
            pltpu.VMEM((TP, 256, WIDTH), bf16),
            pltpu.VMEM((2, GROUPS, STATE), f32),
            dma((PLANE,)),
            dma((PLANE,)),
            dma((PLANES,)),
            dma((PLANES,)),
            dma((TP,)),
            dma((TP,)),
            dma(()),
            dma((6,)),
            dma((6,)),
            dma((6,)),
            dma((6,)),
        ],
        compiler_params=pltpu.CompilerParams(
            collective_id=0, has_side_effects=True, vmem_limit_bytes=40 * 1024 * 1024
        ),
        name="mixer",
    )(
        mixer_input,
        retention,
        decay_real,
        decay_freq,
        log_step,
        input_real,
        input_imag,
        readout_real,
        readout_imaginary,
        skip_weight,
        norm_gain.reshape(1, -1),
        projection,
        residual,
        mix_gain.reshape(1, -1),
    )


def local(
    mixer_input,
    retention,
    decay_real,
    decay_freq,
    log_step,
    input_real,
    input_imag,
    readout_real,
    readout_imaginary,
    skip_weight,
    norm_gain,
    projection,
    residual,
    mix_gain,
    routes,
    route_weight,
    expert_gate,
    expert_up,
    expert_down,
    final_gain,
):
    hidden = mixer(
        mixer_input,
        retention,
        decay_real,
        decay_freq,
        log_step,
        input_real,
        input_imag,
        readout_real,
        readout_imaginary,
        skip_weight,
        norm_gain,
        projection,
        residual,
        mix_gain,
    )
    row_count = hidden.shape[0]
    expert_count = lax.axis_size("sp")
    capacity = max(2, 2 * row_count * PICKS // expert_count)
    chosen = routes.reshape(-1)
    onehot = (chosen[:, None] == jnp.arange(expert_count, dtype=jnp.int32)[None, :]).astype(
        jnp.int32
    )
    slot_index = jnp.sum((jnp.cumsum(onehot, axis=0) - 1) * onehot, axis=1)
    target = chosen * capacity + slot_index
    source_row = jnp.full((expert_count * capacity,), row_count, jnp.int32)
    source_row = source_row.at[target].set(jnp.arange(row_count * PICKS, dtype=jnp.int32) // PICKS)
    padded = jnp.concatenate([hidden, jnp.zeros((1, hidden.shape[1]), hidden.dtype)], axis=0)
    outgoing = padded[source_row].reshape(expert_count, capacity, -1)
    received = lax.all_to_all(outgoing, "sp", split_axis=0, concat_axis=0, tiled=True)
    arrived = received.reshape(-1, received.shape[2])
    gate_act = jnp.dot(arrived, expert_gate[0], preferred_element_type=jnp.float32)
    up_act = jnp.dot(arrived, expert_up[0], preferred_element_type=jnp.float32)
    active = (jax.nn.silu(gate_act) * up_act).astype(jnp.bfloat16)
    produced = jnp.dot(active, expert_down[0], preferred_element_type=jnp.float32).astype(
        jnp.bfloat16
    )
    returned = lax.all_to_all(
        produced.reshape(received.shape), "sp", split_axis=0, concat_axis=0, tiled=True
    )
    gathered_rows = returned.reshape(expert_count * capacity, -1)[target].reshape(
        row_count, PICKS, -1
    )
    expert_mix = jnp.sum(route_weight[:, :, None] * gathered_rows.astype(jnp.float32), axis=1)
    layer_out = layer_norm(deep_alpha * hidden.astype(jnp.float32) + expert_mix, final_gain)
    return layer_out.astype(jnp.bfloat16)


def solution(mesh):
    in_specs = (
        P("sp", "tp"),
        P("tp", "sp"),
        P("tp", None),
        P("tp", None),
        P("tp"),
        P("tp", None, None),
        P("tp", None, None),
        P("tp", None, None),
        P("tp", None, None),
        P("tp", None),
        P(),
        P("tp", None),
        P(("sp", "tp"), None),
        P(),
        P(("sp", "tp"), None),
        P(("sp", "tp"), None),
        P("sp", None, None),
        P("sp", None, None),
        P("sp", None, None),
        P(),
    )
    out_specs = P(("sp", "tp"), None)
    return jax.shard_map(local, mesh=mesh, in_specs=in_specs, out_specs=out_specs, check_vma=False)
```

```python
import jax
import jax.numpy as jnp
from jax import lax
from jax.experimental import pallas as pl
from jax.experimental.pallas import tpu as pltpu
from jax.sharding import PartitionSpec as P

PICKS = 2
MIX_WIDTH = 1024
MESH = pl.DeviceIdType.MESH

deep_alpha = 2.0**0.25

TOKENS = 256
GROUPS = 16
CHANNELS = 16
STATE = 64
WIDTH = 2048
ROWS = 64
PLANES = 8
PLANE = 8
TP = 4
PIECE = 64
EXPERTS = 64
CAPACITY = 4
SLOTS = EXPERTS * CAPACITY
HIDDEN = 512


def times(ar, ai, br, bi):
    return ar * br - ai * bi, ar * bi + ai * br


def layer_norm(values, scales):
    centered = values - jnp.mean(values, axis=-1, keepdims=True)
    variance = jnp.mean(centered * centered, axis=-1, keepdims=True)
    return centered * lax.rsqrt(variance + 1e-05) * scales


def pair_rows(ref):
    return jnp.concatenate(
        [ref[pl.ds(0, 8, stride=2), :], ref[pl.ds(1, 8, stride=2), :]], axis=1
    )


def remote(src, dst, send_sem, recv_sem, **where):
    return pltpu.make_async_remote_copy(
        src_ref=src,
        dst_ref=dst,
        send_sem=send_sem,
        recv_sem=recv_sem,
        device_id=where,
        device_id_type=MESH,
    )


def layer_kernel(
    step_ref,
    x_hbm,
    ret_hbm,
    real_hbm,
    freq_hbm,
    in_real_hbm,
    in_imag_hbm,
    out_real_hbm,
    out_imag_hbm,
    skip_hbm,
    gain_hbm,
    residual_hbm,
    mix_gain_hbm,
    routes_hbm,
    weight_hbm,
    final_gain_hbm,
    proj_ref,
    gate_hbm,
    up_hbm,
    down_hbm,
    layer_ref,
    x_ref,
    ret_ref,
    real_ref,
    freq_ref,
    in_real_ref,
    in_imag_ref,
    out_real_ref,
    out_imag_ref,
    skip_ref,
    gain_ref,
    residual_ref,
    mix_gain_ref,
    routes_ref,
    weight_ref,
    final_gain_ref,
    gate,
    up,
    down,
    drive_w,
    read_w,
    drive_re,
    drive_im,
    shrink,
    states,
    mine,
    plane_buf,
    plane_sum,
    column_buf,
    mixed,
    whole,
    gathered,
    param_buf,
    hidden_buf,
    combine_hi,
    outgoing,
    arrived,
    produced,
    returned,
    load_sem,
    plane_send,
    plane_recv,
    column_send,
    column_recv,
    tp_send,
    tp_recv,
    own_sem,
    ring_send,
    ring_recv,
    twin_send,
    twin_recv,
    out_send,
    out_recv,
    back_send,
    back_recv,
):
    sp = lax.axis_index("sp")
    tp = lax.axis_index("tp")
    plane = lax.div(sp, PLANE)
    place = lax.rem(sp, PLANE)
    core = lax.rem(sp, 2)
    twin = sp + 1 - 2 * core
    right = lax.rem(tp + 1, TP)
    left = lax.rem(tp + TP - 1, TP)
    across = lax.rem(tp + 2, TP)

    barrier = pltpu.get_barrier_semaphore()

    def greet_plane(k, _):
        peer = plane * PLANE + lax.rem(place + k, PLANE)
        pl.semaphore_signal(barrier, inc=1, device_id={"sp": peer}, device_id_type=MESH)
        return 0

    def greet_column(k, _):
        peer = lax.rem(plane + k, PLANES) * PLANE + place
        pl.semaphore_signal(barrier, inc=1, device_id={"sp": peer}, device_id_type=MESH)
        return 0

    def greet_tp(k, _):
        pl.semaphore_signal(
            barrier, inc=1, device_id={"tp": lax.rem(tp + k, TP)}, device_id_type=MESH
        )
        return 0

    lax.fori_loop(1, TP, greet_tp, 0)
    lax.fori_loop(1, PLANE, greet_plane, 0)
    lax.fori_loop(1, PLANES, greet_column, 0)

    own_copy = pltpu.make_async_copy(proj_ref, gathered.at[tp], own_sem)
    own_copy.start()
    loads = [
        pltpu.make_async_copy(source, target, load_sem.at[k])
        for k, (source, target) in enumerate(
            (
                (real_hbm, real_ref),
                (freq_hbm, freq_ref),
                (in_real_hbm, in_real_ref),
                (in_imag_hbm, in_imag_ref),
                (out_real_hbm, out_real_ref),
                (out_imag_hbm, out_imag_ref),
                (ret_hbm, ret_ref),
                (x_hbm, x_ref),
                (skip_hbm, skip_ref),
                (routes_hbm, routes_ref),
                (weight_hbm, weight_ref),
                (gain_hbm, gain_ref),
                (mix_gain_hbm, mix_gain_ref),
                (final_gain_hbm, final_gain_ref),
                (residual_hbm, residual_ref),
                (gate_hbm.at[0], gate),
                (up_hbm.at[0], up),
                (down_hbm.at[0], down),
            )
        )
    ]
    for load in loads:
        load.start()
    for load in loads[:8]:
        load.wait()

    group_row = lax.broadcasted_iota(jnp.int32, (GROUPS, STATE), 0)
    log_step = jnp.zeros((GROUPS, STATE), jnp.float32)
    for g in range(GROUPS):
        log_step = jnp.where(group_row == g, step_ref[g], log_step)
    stride = jnp.exp(log_step)
    decay_real = real_ref[...]
    decay_freq = freq_ref[...]
    growth = decay_real * stride
    turning = decay_freq * stride
    grown = jnp.exp(growth)
    cosine = jnp.cos(turning)
    sine = jnp.sin(turning)
    half_sine = jnp.sin(0.5 * turning)
    expm1 = jnp.tanh(0.5 * growth) * (grown + 1.0)
    upper_real = expm1 * cosine - 2.0 * half_sine * half_sine
    upper_imag = grown * sine
    denominator = decay_real * decay_real + decay_freq * decay_freq
    factor_real = (upper_real * decay_real + upper_imag * decay_freq) / denominator
    factor_imag = (upper_imag * decay_real - upper_real * decay_freq) / denominator
    param_buf[0] = grown * cosine
    param_buf[1] = grown * sine
    keep_re = pair_rows(param_buf.at[0])
    keep_im = pair_rows(param_buf.at[1])

    nothing = jnp.zeros((CHANNELS, STATE), jnp.float32)
    drive_w[...] = jnp.zeros(drive_w.shape, jnp.bfloat16)
    for g in range(GROUPS):
        rows = pl.ds(g * CHANNELS, CHANNELS)
        b_re = jnp.transpose(in_real_ref[g])
        b_im = jnp.transpose(in_imag_ref[g])
        c_re = out_real_ref[g]
        c_im = out_imag_ref[g]
        f_re = factor_real[g : g + 1, :]
        f_im = factor_imag[g : g + 1, :]
        r_re = c_re * f_re - c_im * f_im
        r_im = -(c_re * f_im + c_im * f_re)
        if g % 2 == 0:
            b_row = [b_re, nothing, b_im, nothing]
            r_row = [r_re, nothing, r_im, nothing]
        else:
            b_row = [nothing, b_re, nothing, b_im]
            r_row = [nothing, r_re, nothing, r_im]
        b_row = jnp.concatenate(b_row, axis=1)
        drive_w[g // 2, rows, :] = b_row.astype(jnp.bfloat16)
        read_w[rows, :] = jnp.concatenate(r_row, axis=1).astype(jnp.bfloat16)

    kept = jnp.transpose(jnp.exp(ret_ref[...]))
    kept_hi = kept.astype(jnp.bfloat16)
    rest = kept - kept_hi.astype(jnp.float32)
    kept_mid = rest.astype(jnp.bfloat16)
    kept_lo = (rest - kept_mid.astype(jnp.float32)).astype(jnp.bfloat16)
    select_row = lax.broadcasted_iota(jnp.int32, (GROUPS, 8 * 128), 0)
    select_lane = lax.broadcasted_iota(jnp.int32, (GROUPS, 8 * 128), 1)
    select = (select_row == lax.div(select_lane, STATE)).astype(jnp.bfloat16)
    spread = (
        jnp.dot(kept_hi, select, preferred_element_type=jnp.float32)
        + jnp.dot(kept_mid, select, preferred_element_type=jnp.float32)
        + jnp.dot(kept_lo, select, preferred_element_type=jnp.float32)
    )
    x = x_ref[...]
    for j in range(8):
        at = pl.ds(j, TOKENS, stride=8)
        driven = jnp.dot(x, drive_w[j], preferred_element_type=jnp.float32)
        drive_re[at, :] = driven[:, :128]
        drive_im[at, :] = driven[:, 128:]
        shrink[at, :] = spread[:, j * 128 : (j + 1) * 128]

    pl.semaphore_wait(barrier, (TP - 1) + (PLANE - 1) + (PLANES - 1))

    half = core * (2 * PIECE)
    piece_lo = pl.ds(pl.multiple_of(half, PIECE), PIECE)
    piece_hi = pl.ds(pl.multiple_of(half + PIECE, PIECE), PIECE)

    def ring(block, piece, way, slot):
        to = right if way == 0 else left
        return remote(
            gathered.at[block, piece, :],
            gathered.at[block, piece, :],
            ring_send.at[slot],
            ring_recv.at[slot],
            tp=to,
        )

    own_copy.wait()
    to_right_lo = ring(tp, piece_lo, 0, 0)
    to_left_hi = ring(tp, piece_hi, 1, 1)
    to_right_hi = ring(tp, piece_hi, 0, 2)
    to_left_lo = ring(tp, piece_lo, 1, 3)
    to_right_lo.start()
    to_left_hi.start()
    to_right_hi.start()
    to_left_lo.start()

    def advance(t, carried):
        s_re, s_im, decay = carried
        row = pl.ds(pl.multiple_of(t * 8, 8), 8)
        shr = shrink[row, :]
        a_re = shr * keep_re
        a_im = shr * keep_im
        n_re = (a_re * s_re - a_im * s_im) + drive_re[row, :]
        n_im = (a_re * s_im + a_im * s_re) + drive_im[row, :]
        return n_re, n_im, decay * shr

    zero = jnp.zeros((8, 128), jnp.float32)
    one = jnp.ones((8, 128), jnp.float32)
    end_re, end_im, decay = lax.fori_loop(0, TOKENS, advance, (zero, zero, one), unroll=8)
    mine[0] = end_re
    mine[1] = end_im
    mine[2] = decay

    power_re, power_im = keep_re, keep_im
    for _ in range(8):
        power_re, power_im = times(power_re, power_im, power_re, power_im)
    plane_re, plane_im = power_re, power_im
    for _ in range(3):
        plane_re, plane_im = times(plane_re, plane_im, plane_re, plane_im)

    def plane_copy(k):
        peer = plane * PLANE + lax.rem(place + k, PLANE)
        return remote(mine, plane_buf.at[place], plane_send.at[k], plane_recv.at[place], sp=peer)

    def send_plane(k, _):
        plane_copy(k).start()
        return 0

    def plane_arrived(k, _):
        source = lax.rem(place + k, PLANE)
        remote(
            mine, plane_buf.at[source], plane_send.at[k], plane_recv.at[source], sp=plane * PLANE + source
        ).wait_recv()
        return 0

    lax.fori_loop(1, PLANE, send_plane, 0)
    lax.fori_loop(1, PLANE, plane_arrived, 0)
    plane_buf[place] = mine[...]

    def join(buf, k, carried, p_re, p_im):
        s_re, s_im, decay = carried
        d = buf[k, 2]
        m_re, m_im = times(d * p_re, d * p_im, s_re, s_im)
        return m_re + buf[k, 0], m_im + buf[k, 1], decay * d

    def join_place(k, carried):
        return join(plane_buf, k, carried, power_re, power_im)

    total = lax.fori_loop(0, PLANE, join_place, (zero, zero, one))
    plane_sum[0] = total[0]
    plane_sum[1] = total[1]
    plane_sum[2] = total[2]

    def column_copy(p):
        return remote(
            plane_sum, column_buf.at[plane], column_send.at[p], column_recv.at[plane], sp=p * PLANE + place
        )

    def send_column(p, _):
        column_copy(p).start()
        return 0

    def column_arrived(p, _):
        remote(
            plane_sum, column_buf.at[p], column_send.at[p], column_recv.at[p], sp=p * PLANE + place
        ).wait_recv()
        return 0

    lax.fori_loop(plane + 1, PLANES, send_column, 0)

    for load in loads[8:15]:
        load.wait()
    slot = lax.broadcasted_iota(jnp.int32, (ROWS, SLOTS), 1)
    slot_plane = lax.rem(plane + lax.shift_right_logical(slot, 5), PLANES)
    slot_place = lax.rem(place + lax.rem(lax.shift_right_logical(slot, 2), PLANE), PLANE)
    slot_expert = slot_plane * PLANE + slot_place
    first = jnp.where(routes_ref[:, 0:1] == slot_expert, 1.0, 0.0)
    second = jnp.where(routes_ref[:, 1:2] == slot_expert, 1.0, 0.0)
    named = first + second
    row_at = lax.broadcasted_iota(jnp.int32, (ROWS, ROWS), 0)
    row_before = lax.broadcasted_iota(jnp.int32, (ROWS, ROWS), 1)
    earlier = jnp.where(row_before < row_at, 1.0, 0.0).astype(jnp.bfloat16)
    rank = jnp.dot(earlier, named.astype(jnp.bfloat16), preferred_element_type=jnp.float32)
    here = jnp.where(rank == lax.rem(slot, CAPACITY).astype(jnp.float32), 1.0, 0.0)
    weights = here * (weight_ref[:, 0:1] * first + weight_ref[:, 1:2] * second)
    weights_hi = weights.astype(jnp.bfloat16)
    combine_hi[:ROWS, :] = weights_hi
    combine_hi[ROWS:, :] = (weights - weights_hi.astype(jnp.float32)).astype(jnp.bfloat16)
    pick = jnp.transpose(here * named).astype(jnp.bfloat16)

    def twin_copy(block, piece, slot):
        return remote(
            gathered.at[block, piece, :],
            gathered.at[block, piece, :],
            twin_send.at[slot],
            twin_recv.at[slot],
            sp=twin,
        )

    from_left_lo = ring(left, piece_lo, 0, 0)
    from_right_hi = ring(right, piece_hi, 1, 1)
    from_left_hi = ring(left, piece_hi, 0, 2)
    from_right_lo = ring(right, piece_lo, 1, 3)
    from_left_lo.wait_recv()
    pass_right = ring(left, piece_lo, 0, 4)
    pass_right.start()
    from_right_hi.wait_recv()
    pass_left = ring(right, piece_hi, 1, 5)
    pass_left.start()
    twin_left_lo = twin_copy(left, piece_lo, 0)
    twin_right_hi = twin_copy(right, piece_hi, 1)
    twin_left_lo.start()
    twin_right_hi.start()

    lax.fori_loop(0, plane, column_arrived, 0)

    def join_plane(p, carried):
        return join(column_buf, p, carried, plane_re, plane_im)

    carried = lax.fori_loop(0, plane, join_plane, (zero, zero, one))
    carried = lax.fori_loop(0, place, join_place, carried)

    def record(t, carried):
        s_re, s_im = carried
        row = pl.ds(pl.multiple_of(t * 8, 8), 8)
        shr = shrink[row, :]
        a_re = shr * keep_re
        a_im = shr * keep_im
        n_re = (a_re * s_re - a_im * s_im) + drive_re[row, :]
        n_im = (a_re * s_im + a_im * s_re) + drive_im[row, :]
        states[row, :128] = n_re
        states[row, 128:] = n_im
        return n_re, n_im

    lax.fori_loop(0, TOKENS, record, (carried[0], carried[1]), unroll=8)

    def read(k, _):
        at = pl.ds(pl.multiple_of(k * 256, 256), 256)
        product = lax.dot_general(
            states[at, :].astype(jnp.bfloat16),
            read_w[...],
            (((1,), (1,)), ((), ())),
            preferred_element_type=jnp.float32,
        )
        drive_re[at, :] = product[:, :128]
        drive_im[at, :] = product[:, 128:]
        return 0

    lax.fori_loop(0, 8, read, 0)
    lane = lax.broadcasted_iota(jnp.int32, (TOKENS, 128), 1)
    for side, buf in ((0, drive_re), (1, drive_im)):
        picked = jnp.zeros((TOKENS, 128), jnp.float32)
        for j in range(4):
            value = buf[pl.ds(side * 4 + j, TOKENS, stride=8), :]
            picked = jnp.where(lax.div(lane, 32) == j, value, picked)
        skip = jnp.concatenate([skip_ref[g : g + 1, :] for g in range(side * 8, side * 8 + 8)], axis=1)
        lanes = slice(side * 128, side * 128 + 128)
        read_out = picked + skip * x_ref[:, lanes].astype(jnp.float32)
        mixed[:, lanes] = jax.nn.gelu(read_out).astype(jnp.bfloat16)

    def tp_copy(k):
        peer = lax.rem(tp + k, TP)
        rows = pl.ds(pl.multiple_of(peer * ROWS, ROWS), ROWS)
        return remote(mixed.at[rows, :], whole.at[tp], tp_send.at[k], tp_recv.at[tp], tp=peer)

    def send_tp(k, _):
        tp_copy(k).start()
        return 0

    def tp_arrived(k, _):
        source = lax.rem(tp + k, TP)
        rows = pl.ds(pl.multiple_of(tp * ROWS, ROWS), ROWS)
        remote(mixed.at[rows, :], whole.at[source], tp_send.at[k], tp_recv.at[source], tp=source).wait_recv()
        return 0

    lax.fori_loop(1, TP, send_tp, 0)
    whole[tp] = mixed[pl.ds(pl.multiple_of(tp * ROWS, ROWS), ROWS), :]

    from_left_hi.wait_recv()
    from_right_lo.wait_recv()
    twin_left_hi = twin_copy(left, piece_hi, 2)
    twin_right_lo = twin_copy(right, piece_lo, 3)
    twin_left_hi.start()
    twin_right_lo.start()
    across_lo = ring(across, piece_lo, 0, 4)
    across_hi = ring(across, piece_hi, 1, 5)
    across_lo.wait_recv()
    twin_across_lo = twin_copy(across, piece_lo, 4)
    twin_across_lo.start()
    across_hi.wait_recv()
    twin_across_hi = twin_copy(across, piece_hi, 5)
    twin_across_hi.start()

    other = 2 * PIECE - half
    other_lo = pl.ds(pl.multiple_of(other, PIECE), PIECE)
    other_hi = pl.ds(pl.multiple_of(other + PIECE, PIECE), PIECE)
    lax.fori_loop(1, TP, tp_arrived, 0)
    for slot, (block, piece) in enumerate(
        (
            (left, other_lo),
            (right, other_hi),
            (left, other_hi),
            (right, other_lo),
            (across, other_lo),
            (across, other_hi),
        )
    ):
        twin_copy(block, piece, slot).wait_recv()

    squares = jnp.zeros((ROWS, 1), jnp.float32)
    scaled = []
    for q in range(TP):
        rows = whole[q].astype(jnp.float32)
        squares += jnp.sum(rows * rows, axis=1, keepdims=True)
        scaled.append((rows * gain_ref[:, q * 256 : (q + 1) * 256]).astype(jnp.bfloat16))
    inverse = lax.rsqrt(squares / MIX_WIDTH + 1e-06)
    mix = jnp.zeros((ROWS, WIDTH), jnp.float32)
    for q in range(TP):
        mix += jnp.dot(scaled[q], gathered[q], preferred_element_type=jnp.float32)
    mix = deep_alpha * residual_ref[...].astype(jnp.float32) + mix * inverse
    hidden = layer_norm(mix, mix_gain_ref[...]).astype(jnp.bfloat16)
    hidden_buf[...] = hidden

    def expert_of(k):
        return lax.rem(plane + lax.div(k, PLANE), PLANES) * PLANE + lax.rem(place + k, PLANE)

    def source_of(k):
        return lax.rem(plane + PLANES - lax.div(k, PLANE), PLANES) * PLANE + lax.rem(
            place + PLANE - lax.rem(k, PLANE), PLANE
        )

    def out_copy(k):
        return remote(outgoing.at[k], arrived.at[k], out_send.at[k], out_recv.at[k], sp=expert_of(k))

    def back_copy(k):
        return remote(produced.at[k], returned.at[k], back_send.at[k], back_recv.at[k], sp=source_of(k))

    def send_out(k, _):
        out_copy(k).start()
        return 0

    for p in (4, 3, 5, 2, 6, 1, 7, 0):
        rows = jnp.dot(pick[p * 32 : (p + 1) * 32, :], hidden, preferred_element_type=jnp.float32)
        outgoing[p * PLANE : (p + 1) * PLANE] = rows.astype(jnp.bfloat16).reshape(PLANE, CAPACITY, WIDTH)
        lax.fori_loop(p * PLANE + (p == 0), (p + 1) * PLANE, send_out, 0)
    arrived[0] = outgoing[0]

    for load in loads[15:]:
        load.wait()

    def expert(c, _):
        far = (PLANES // 2 + c) * PLANE
        near = (PLANES // 2 - 1 - c) * PLANE
        near_first = jnp.maximum(near, 1)

        def out_arrived(k, _):
            out_copy(k).wait_recv()
            return 0

        def send_back(k, _):
            back_copy(k).start()
            return 0

        lax.fori_loop(far, far + PLANE, out_arrived, 0)
        lax.fori_loop(near_first, near + PLANE, out_arrived, 0)
        rows = jnp.concatenate(
            [
                arrived[pl.ds(far, PLANE)].reshape(PLANE * CAPACITY, WIDTH),
                arrived[pl.ds(near, PLANE)].reshape(PLANE * CAPACITY, WIDTH),
            ],
            axis=0,
        )
        gate_act = jnp.dot(rows, gate[...], preferred_element_type=jnp.float32)
        up_act = jnp.dot(rows, up[...], preferred_element_type=jnp.float32)
        active = (jax.nn.silu(gate_act) * up_act).astype(jnp.bfloat16)
        result = jnp.dot(active, down[...], preferred_element_type=jnp.float32).astype(jnp.bfloat16)
        produced[pl.ds(far, PLANE)] = result[: PLANE * CAPACITY].reshape(PLANE, CAPACITY, WIDTH)
        produced[pl.ds(near, PLANE)] = result[PLANE * CAPACITY :].reshape(PLANE, CAPACITY, WIDTH)
        lax.fori_loop(far, far + PLANE, send_back, 0)
        lax.fori_loop(near_first, near + PLANE, send_back, 0)
        return 0

    lax.fori_loop(0, PLANES // 2, expert, 0)
    returned[0] = produced[0]

    def back_arrived(k, _):
        back_copy(k).wait_recv()
        return 0

    lax.fori_loop(1, EXPERTS, back_arrived, 0)
    both = jnp.dot(
        combine_hi[...], returned[...].reshape(SLOTS, WIDTH), preferred_element_type=jnp.float32
    )
    expert_mix = both[:ROWS] + both[ROWS:]
    final = layer_norm(deep_alpha * hidden_buf[...].astype(jnp.float32) + expert_mix, final_gain_ref[...])
    layer_ref[...] = final.astype(jnp.bfloat16)

    def out_left(k, _):
        out_copy(k).wait_send()
        back_copy(k).wait_send()
        return 0

    lax.fori_loop(1, EXPERTS, out_left, 0)

    def plane_left(k, _):
        plane_copy(k).wait_send()
        return 0

    def column_left(p, _):
        column_copy(p).wait_send()
        return 0

    def tp_left(k, _):
        tp_copy(k).wait_send()
        return 0

    lax.fori_loop(1, PLANE, plane_left, 0)
    lax.fori_loop(plane + 1, PLANES, column_left, 0)
    lax.fori_loop(1, TP, tp_left, 0)
    for copy in (to_right_lo, to_left_hi, to_right_hi, to_left_lo, pass_right, pass_left):
        copy.wait_send()
    for copy in (twin_left_lo, twin_right_hi, twin_left_hi, twin_right_lo, twin_across_lo, twin_across_hi):
        copy.wait_send()


def local(
    mixer_input,
    retention,
    decay_real,
    decay_freq,
    log_step,
    input_real,
    input_imag,
    readout_real,
    readout_imaginary,
    skip_weight,
    norm_gain,
    projection,
    residual,
    mix_gain,
    routes,
    route_weight,
    expert_gate,
    expert_up,
    expert_down,
    final_gain,
):
    hbm = pl.BlockSpec(memory_space=pltpu.HBM)
    smem = pl.BlockSpec(memory_space=pltpu.SMEM)
    vmem = pl.BlockSpec(memory_space=pltpu.VMEM)
    f32 = jnp.float32
    bf16 = jnp.bfloat16
    dma = pltpu.SemaphoreType.DMA
    small = (
        mixer_input,
        retention,
        decay_real,
        decay_freq,
        input_real,
        input_imag,
        readout_real,
        readout_imaginary,
        skip_weight,
        norm_gain.reshape(1, -1),
        residual,
        mix_gain.reshape(1, -1),
        routes,
        route_weight,
        final_gain.reshape(1, -1),
    )
    large = (projection, expert_gate, expert_up, expert_down)
    return pl.pallas_call(
        layer_kernel,
        out_shape=jax.ShapeDtypeStruct((ROWS, WIDTH), bf16),
        in_specs=[smem] + [hbm] * (len(small) + len(large)),
        out_specs=vmem,
        scratch_shapes=[pltpu.VMEM(a.shape, a.dtype) for a in small]
        + [
            pltpu.VMEM((WIDTH, HIDDEN), bf16),
            pltpu.VMEM((WIDTH, HIDDEN), bf16),
            pltpu.VMEM((HIDDEN, WIDTH), bf16),
            pltpu.VMEM((8, 256, 256), bf16),
            pltpu.VMEM((256, 256), bf16),
            pltpu.VMEM((TOKENS * 8, 128), f32),
            pltpu.VMEM((TOKENS * 8, 128), f32),
            pltpu.VMEM((TOKENS * 8, 128), f32),
            pltpu.VMEM((TOKENS * 8, 256), f32),
            pltpu.VMEM((3, 8, 128), f32),
            pltpu.VMEM((PLANE, 3, 8, 128), f32),
            pltpu.VMEM((3, 8, 128), f32),
            pltpu.VMEM((PLANES, 3, 8, 128), f32),
            pltpu.VMEM((TOKENS, 256), bf16),
            pltpu.VMEM((TP, ROWS, 256), bf16),
            pltpu.VMEM((TP, 256, WIDTH), bf16),
            pltpu.VMEM((2, GROUPS, STATE), f32),
            pltpu.VMEM((ROWS, WIDTH), bf16),
            pltpu.VMEM((2 * ROWS, SLOTS), bf16),
            pltpu.VMEM((EXPERTS, CAPACITY, WIDTH), bf16),
            pltpu.VMEM((EXPERTS, CAPACITY, WIDTH), bf16),
            pltpu.VMEM((EXPERTS, CAPACITY, WIDTH), bf16),
            pltpu.VMEM((EXPERTS, CAPACITY, WIDTH), bf16),
            dma((18,)),
            dma((PLANE,)),
            dma((PLANE,)),
            dma((PLANES,)),
            dma((PLANES,)),
            dma((TP,)),
            dma((TP,)),
            dma(()),
            dma((6,)),
            dma((6,)),
            dma((6,)),
            dma((6,)),
            dma((EXPERTS,)),
            dma((EXPERTS,)),
            dma((EXPERTS,)),
            dma((EXPERTS,)),
        ],
        compiler_params=pltpu.CompilerParams(
            collective_id=0, has_side_effects=True, vmem_limit_bytes=56 * 1024 * 1024
        ),
        name="layer",
    )(log_step, *small, *large)


def solution(mesh):
    in_specs = (
        P("sp", "tp"),
        P("tp", "sp"),
        P("tp", None),
        P("tp", None),
        P("tp"),
        P("tp", None, None),
        P("tp", None, None),
        P("tp", None, None),
        P("tp", None, None),
        P("tp", None),
        P(),
        P("tp", None),
        P(("sp", "tp"), None),
        P(),
        P(("sp", "tp"), None),
        P(("sp", "tp"), None),
        P("sp", None, None),
        P("sp", None, None),
        P("sp", None, None),
        P(),
    )
    out_specs = P(("sp", "tp"), None)
    return jax.shard_map(local, mesh=mesh, in_specs=in_specs, out_specs=out_specs, check_vma=False)
```

```python
import jax
import jax.numpy as jnp
from jax import lax
from jax.experimental import pallas as pl
from jax.experimental.pallas import tpu as pltpu
from jax.sharding import PartitionSpec as P

PICKS = 2
MIX_WIDTH = 1024
MESH = pl.DeviceIdType.MESH

deep_alpha = 2.0**0.25

TOKENS = 256
GROUPS = 16
CHANNELS = 16
STATE = 64
WIDTH = 2048
ROWS = 64
PLANES = 8
PLANE = 8
TP = 4
PIECE = 64
EXPERTS = 64
CAPACITY = 4
SLOTS = EXPERTS * CAPACITY
HIDDEN = 512
FAR = 16
FAR_BLOCKS = 32


def times(ar, ai, br, bi):
    return ar * br - ai * bi, ar * bi + ai * br


def layer_norm(values, scales):
    centered = values - jnp.mean(values, axis=-1, keepdims=True)
    variance = jnp.mean(centered * centered, axis=-1, keepdims=True)
    return centered * lax.rsqrt(variance + 1e-05) * scales


def pair_rows(ref):
    return jnp.concatenate(
        [ref[pl.ds(0, 8, stride=2), :], ref[pl.ds(1, 8, stride=2), :]], axis=1
    )


def remote(src, dst, send_sem, recv_sem, **where):
    return pltpu.make_async_remote_copy(
        src_ref=src,
        dst_ref=dst,
        send_sem=send_sem,
        recv_sem=recv_sem,
        device_id=where,
        device_id_type=MESH,
    )


def layer_kernel(
    step_ref,
    x_hbm,
    ret_hbm,
    real_hbm,
    freq_hbm,
    in_real_hbm,
    in_imag_hbm,
    out_real_hbm,
    out_imag_hbm,
    skip_hbm,
    gain_hbm,
    residual_hbm,
    mix_gain_hbm,
    routes_hbm,
    weight_hbm,
    final_gain_hbm,
    proj_ref,
    gate_hbm,
    up_hbm,
    down_hbm,
    layer_ref,
    x_ref,
    ret_ref,
    real_ref,
    freq_ref,
    in_real_ref,
    in_imag_ref,
    out_real_ref,
    out_imag_ref,
    skip_ref,
    gain_ref,
    residual_ref,
    mix_gain_ref,
    routes_ref,
    weight_ref,
    final_gain_ref,
    gate,
    up,
    down,
    drive_w,
    read_w,
    drive_re,
    drive_im,
    shrink,
    states,
    mine,
    plane_buf,
    plane_sum,
    column_buf,
    mixed,
    whole,
    gathered,
    param_buf,
    hidden_buf,
    combine_hi,
    pick,
    mixed_out,
    mixed_in,
    outgoing,
    arrived,
    produced,
    returned,
    load_sem,
    plane_send,
    plane_recv,
    column_send,
    column_recv,
    tp_send,
    tp_recv,
    own_sem,
    ring_send,
    ring_recv,
    twin_send,
    twin_recv,
    out_send,
    out_recv,
    back_send,
    back_recv,
    mixed_send,
    mixed_recv,
):
    sp = lax.axis_index("sp")
    tp = lax.axis_index("tp")
    plane = lax.div(sp, PLANE)
    place = lax.rem(sp, PLANE)
    core = lax.rem(sp, 2)
    twin = sp + 1 - 2 * core
    right = lax.rem(tp + 1, TP)
    left = lax.rem(tp + TP - 1, TP)
    across = lax.rem(tp + 2, TP)

    barrier = pltpu.get_barrier_semaphore()

    def greet_plane(k, _):
        peer = plane * PLANE + lax.rem(place + k, PLANE)
        pl.semaphore_signal(barrier, inc=1, device_id={"sp": peer}, device_id_type=MESH)
        return 0

    def greet_column(k, _):
        peer = lax.rem(plane + k, PLANES) * PLANE + place
        pl.semaphore_signal(barrier, inc=1, device_id={"sp": peer}, device_id_type=MESH)
        return 0

    def greet_tp(k, _):
        pl.semaphore_signal(
            barrier, inc=1, device_id={"tp": lax.rem(tp + k, TP)}, device_id_type=MESH
        )
        return 0

    lax.fori_loop(1, TP, greet_tp, 0)
    lax.fori_loop(1, PLANE, greet_plane, 0)
    lax.fori_loop(1, PLANES, greet_column, 0)

    own_copy = pltpu.make_async_copy(proj_ref, gathered.at[tp], own_sem)
    own_copy.start()
    loads = [
        pltpu.make_async_copy(source, target, load_sem.at[k])
        for k, (source, target) in enumerate(
            (
                (real_hbm, real_ref),
                (freq_hbm, freq_ref),
                (in_real_hbm, in_real_ref),
                (in_imag_hbm, in_imag_ref),
                (out_real_hbm, out_real_ref),
                (out_imag_hbm, out_imag_ref),
                (ret_hbm, ret_ref),
                (x_hbm, x_ref),
                (skip_hbm, skip_ref),
                (routes_hbm, routes_ref),
                (weight_hbm, weight_ref),
                (gain_hbm, gain_ref),
                (mix_gain_hbm, mix_gain_ref),
                (final_gain_hbm, final_gain_ref),
                (residual_hbm, residual_ref),
                (gate_hbm.at[0], gate),
                (up_hbm.at[0], up),
                (down_hbm.at[0], down),
            )
        )
    ]
    for load in loads:
        load.start()
    for load in loads[:8]:
        load.wait()

    group_row = lax.broadcasted_iota(jnp.int32, (GROUPS, STATE), 0)
    log_step = jnp.zeros((GROUPS, STATE), jnp.float32)
    for g in range(GROUPS):
        log_step = jnp.where(group_row == g, step_ref[g], log_step)
    stride = jnp.exp(log_step)
    decay_real = real_ref[...]
    decay_freq = freq_ref[...]
    growth = decay_real * stride
    turning = decay_freq * stride
    grown = jnp.exp(growth)
    cosine = jnp.cos(turning)
    sine = jnp.sin(turning)
    half_sine = jnp.sin(0.5 * turning)
    expm1 = jnp.tanh(0.5 * growth) * (grown + 1.0)
    upper_real = expm1 * cosine - 2.0 * half_sine * half_sine
    upper_imag = grown * sine
    denominator = decay_real * decay_real + decay_freq * decay_freq
    factor_real = (upper_real * decay_real + upper_imag * decay_freq) / denominator
    factor_imag = (upper_imag * decay_real - upper_real * decay_freq) / denominator
    param_buf[0] = grown * cosine
    param_buf[1] = grown * sine
    keep_re = pair_rows(param_buf.at[0])
    keep_im = pair_rows(param_buf.at[1])

    nothing = jnp.zeros((CHANNELS, STATE), jnp.float32)
    drive_w[...] = jnp.zeros(drive_w.shape, jnp.bfloat16)
    for g in range(GROUPS):
        rows = pl.ds(g * CHANNELS, CHANNELS)
        b_re = in_real_ref[g]
        b_im = in_imag_ref[g]
        c_re = out_real_ref[g]
        c_im = out_imag_ref[g]
        f_re = factor_real[g : g + 1, :]
        f_im = factor_imag[g : g + 1, :]
        r_re = c_re * f_re - c_im * f_im
        r_im = -(c_re * f_im + c_im * f_re)
        if g % 2 == 0:
            b_row = [b_re, nothing, b_im, nothing]
            r_row = [r_re, nothing, r_im, nothing]
        else:
            b_row = [nothing, b_re, nothing, b_im]
            r_row = [nothing, r_re, nothing, r_im]
        b_row = jnp.concatenate(b_row, axis=1)
        drive_w[g // 2, rows, :] = b_row.astype(jnp.bfloat16)
        read_w[rows, :] = jnp.concatenate(r_row, axis=1).astype(jnp.bfloat16)

    kept = jnp.transpose(jnp.exp(ret_ref[...]))
    kept_hi = kept.astype(jnp.bfloat16)
    rest = kept - kept_hi.astype(jnp.float32)
    kept_mid = rest.astype(jnp.bfloat16)
    kept_lo = (rest - kept_mid.astype(jnp.float32)).astype(jnp.bfloat16)
    select_row = lax.broadcasted_iota(jnp.int32, (GROUPS, 8 * 128), 0)
    select_lane = lax.broadcasted_iota(jnp.int32, (GROUPS, 8 * 128), 1)
    select = (select_row == lax.div(select_lane, STATE)).astype(jnp.bfloat16)
    spread = (
        jnp.dot(kept_hi, select, preferred_element_type=jnp.float32)
        + jnp.dot(kept_mid, select, preferred_element_type=jnp.float32)
        + jnp.dot(kept_lo, select, preferred_element_type=jnp.float32)
    )
    x = x_ref[...]
    for j in range(8):
        at = pl.ds(j, TOKENS, stride=8)
        driven = jnp.dot(x, drive_w[j], preferred_element_type=jnp.float32)
        drive_re[at, :] = driven[:, :128]
        drive_im[at, :] = driven[:, 128:]
        shrink[at, :] = spread[:, j * 128 : (j + 1) * 128]

    pl.semaphore_wait(barrier, (TP - 1) + (PLANE - 1) + (PLANES - 1))

    half = core * (2 * PIECE)
    piece_lo = pl.ds(pl.multiple_of(half, PIECE), PIECE)
    piece_hi = pl.ds(pl.multiple_of(half + PIECE, PIECE), PIECE)

    def ring(block, piece, way, slot):
        to = right if way == 0 else left
        return remote(
            gathered.at[block, piece, :],
            gathered.at[block, piece, :],
            ring_send.at[slot],
            ring_recv.at[slot],
            tp=to,
        )

    own_copy.wait()
    to_right_lo = ring(tp, piece_lo, 0, 0)
    to_left_hi = ring(tp, piece_hi, 1, 1)
    to_right_hi = ring(tp, piece_hi, 0, 2)
    to_left_lo = ring(tp, piece_lo, 1, 3)
    to_right_lo.start()
    to_left_hi.start()
    to_right_hi.start()
    to_left_lo.start()

    def advance(t, carried):
        s_re, s_im, decay = carried
        row = pl.ds(pl.multiple_of(t * 8, 8), 8)
        shr = shrink[row, :]
        a_re = shr * keep_re
        a_im = shr * keep_im
        n_re = (a_re * s_re - a_im * s_im) + drive_re[row, :]
        n_im = (a_re * s_im + a_im * s_re) + drive_im[row, :]
        return n_re, n_im, decay * shr

    zero = jnp.zeros((8, 128), jnp.float32)
    one = jnp.ones((8, 128), jnp.float32)
    end_re, end_im, decay = lax.fori_loop(0, TOKENS, advance, (zero, zero, one), unroll=8)
    mine[0] = end_re
    mine[1] = end_im
    mine[2] = decay

    power_re, power_im = keep_re, keep_im
    for _ in range(8):
        power_re, power_im = times(power_re, power_im, power_re, power_im)
    plane_re, plane_im = power_re, power_im
    for _ in range(3):
        plane_re, plane_im = times(plane_re, plane_im, plane_re, plane_im)

    def plane_copy(k):
        peer = plane * PLANE + lax.rem(place + k, PLANE)
        return remote(mine, plane_buf.at[place], plane_send.at[k], plane_recv.at[place], sp=peer)

    def send_plane(k, _):
        plane_copy(k).start()
        return 0

    def plane_arrived(k, _):
        source = lax.rem(place + k, PLANE)
        remote(
            mine, plane_buf.at[source], plane_send.at[k], plane_recv.at[source], sp=plane * PLANE + source
        ).wait_recv()
        return 0

    lax.fori_loop(1, PLANE, send_plane, 0)
    lax.fori_loop(1, PLANE, plane_arrived, 0)
    plane_buf[place] = mine[...]

    def join(buf, k, carried, p_re, p_im):
        s_re, s_im, decay = carried
        d = buf[k, 2]
        m_re, m_im = times(d * p_re, d * p_im, s_re, s_im)
        return m_re + buf[k, 0], m_im + buf[k, 1], decay * d

    def join_place(k, carried):
        return join(plane_buf, k, carried, power_re, power_im)

    total = lax.fori_loop(0, PLANE, join_place, (zero, zero, one))
    plane_sum[0] = total[0]
    plane_sum[1] = total[1]
    plane_sum[2] = total[2]

    def column_copy(p):
        return remote(
            plane_sum, column_buf.at[plane], column_send.at[p], column_recv.at[plane], sp=p * PLANE + place
        )

    def send_column(p, _):
        column_copy(p).start()
        return 0

    def column_arrived(p, _):
        remote(
            plane_sum, column_buf.at[p], column_send.at[p], column_recv.at[p], sp=p * PLANE + place
        ).wait_recv()
        return 0

    lax.fori_loop(plane + 1, PLANES, send_column, 0)

    for load in loads[8:15]:
        load.wait()
    slot = lax.broadcasted_iota(jnp.int32, (SLOTS, ROWS), 0)
    slot_plane = lax.rem(plane + lax.shift_right_logical(slot, 5), PLANES)
    slot_place = lax.rem(place + lax.rem(lax.shift_right_logical(slot, 2), PLANE), PLANE)
    slot_expert = slot_plane * PLANE + slot_place
    first = jnp.where(routes_ref[0:1, :] == slot_expert, 1.0, 0.0)
    second = jnp.where(routes_ref[1:2, :] == slot_expert, 1.0, 0.0)
    named = first + second
    row_before = lax.broadcasted_iota(jnp.int32, (ROWS, ROWS), 0)
    row_at = lax.broadcasted_iota(jnp.int32, (ROWS, ROWS), 1)
    earlier = jnp.where(row_before < row_at, 1.0, 0.0).astype(jnp.bfloat16)
    rank = jnp.dot(named.astype(jnp.bfloat16), earlier, preferred_element_type=jnp.float32)
    here = jnp.where(rank == lax.rem(slot, CAPACITY).astype(jnp.float32), 1.0, 0.0)
    weights = jnp.transpose(here * (weight_ref[0:1, :] * first + weight_ref[1:2, :] * second))
    weights_hi = weights.astype(jnp.bfloat16)
    combine_hi[:ROWS, :] = weights_hi
    combine_hi[ROWS:, :] = (weights - weights_hi.astype(jnp.float32)).astype(jnp.bfloat16)
    pick[...] = (here * named).astype(jnp.bfloat16)

    def expert_of(k):
        return lax.rem(plane + lax.div(k, PLANE), PLANES) * PLANE + lax.rem(place + k, PLANE)

    def source_of(k):
        return lax.rem(plane + PLANES - lax.div(k, PLANE), PLANES) * PLANE + lax.rem(
            place + PLANE - lax.rem(k, PLANE), PLANE
        )

    def out_copy(k):
        return remote(outgoing.at[k], arrived.at[k], out_send.at[k], out_recv.at[k], sp=expert_of(k))

    def mixed_copy(k):
        return remote(
            mixed_out.at[k], mixed_in.at[k], mixed_send.at[k], mixed_recv.at[k], sp=expert_of(k + FAR)
        )

    def back_copy(k):
        return remote(produced.at[k], returned.at[k], back_send.at[k], back_recv.at[k], sp=source_of(k))

    def send_out(k, _):
        out_copy(k).start()
        return 0

    def send_mixed(k, _):
        mixed_copy(k).start()
        return 0

    def blocks(p, rows):
        picked = jnp.dot(pick[p * 32 : (p + 1) * 32, :], rows, preferred_element_type=jnp.float32)
        return picked.astype(jnp.bfloat16).reshape(PLANE, CAPACITY, rows.shape[1])

    for p in (4, 3, 5, 2):
        outgoing[p * PLANE : (p + 1) * PLANE] = blocks(p, residual_ref[...])
        lax.fori_loop(p * PLANE, (p + 1) * PLANE, send_out, 0)

    def twin_copy(block, piece, slot):
        return remote(
            gathered.at[block, piece, :],
            gathered.at[block, piece, :],
            twin_send.at[slot],
            twin_recv.at[slot],
            sp=twin,
        )

    from_left_lo = ring(left, piece_lo, 0, 0)
    from_right_hi = ring(right, piece_hi, 1, 1)
    from_left_hi = ring(left, piece_hi, 0, 2)
    from_right_lo = ring(right, piece_lo, 1, 3)
    from_left_lo.wait_recv()
    pass_right = ring(left, piece_lo, 0, 4)
    pass_right.start()
    from_right_hi.wait_recv()
    pass_left = ring(right, piece_hi, 1, 5)
    pass_left.start()
    twin_left_lo = twin_copy(left, piece_lo, 0)
    twin_right_hi = twin_copy(right, piece_hi, 1)
    twin_left_lo.start()
    twin_right_hi.start()

    lax.fori_loop(0, plane, column_arrived, 0)

    def join_plane(p, carried):
        return join(column_buf, p, carried, plane_re, plane_im)

    carried = lax.fori_loop(0, plane, join_plane, (zero, zero, one))
    carried = lax.fori_loop(0, place, join_place, carried)

    def record(t, carried):
        s_re, s_im = carried
        row = pl.ds(pl.multiple_of(t * 8, 8), 8)
        shr = shrink[row, :]
        a_re = shr * keep_re
        a_im = shr * keep_im
        n_re = (a_re * s_re - a_im * s_im) + drive_re[row, :]
        n_im = (a_re * s_im + a_im * s_re) + drive_im[row, :]
        states[row, :128] = n_re
        states[row, 128:] = n_im
        return n_re, n_im

    lax.fori_loop(0, TOKENS, record, (carried[0], carried[1]), unroll=8)

    def read(k, _):
        at = pl.ds(pl.multiple_of(k * 256, 256), 256)
        product = lax.dot_general(
            states[at, :].astype(jnp.bfloat16),
            read_w[...],
            (((1,), (1,)), ((), ())),
            preferred_element_type=jnp.float32,
        )
        drive_re[at, :] = product[:, :128]
        drive_im[at, :] = product[:, 128:]
        return 0

    lax.fori_loop(0, 8, read, 0)
    lane = lax.broadcasted_iota(jnp.int32, (TOKENS, 128), 1)
    for side, buf in ((0, drive_re), (1, drive_im)):
        picked = jnp.zeros((TOKENS, 128), jnp.float32)
        for j in range(4):
            value = buf[pl.ds(side * 4 + j, TOKENS, stride=8), :]
            picked = jnp.where(lax.div(lane, 32) == j, value, picked)
        skip = jnp.concatenate([skip_ref[g : g + 1, :] for g in range(side * 8, side * 8 + 8)], axis=1)
        lanes = slice(side * 128, side * 128 + 128)
        read_out = picked + skip * x_ref[:, lanes].astype(jnp.float32)
        mixed[:, lanes] = jax.nn.gelu(read_out).astype(jnp.bfloat16)

    def tp_copy(k):
        peer = lax.rem(tp + k, TP)
        rows = pl.ds(pl.multiple_of(peer * ROWS, ROWS), ROWS)
        return remote(mixed.at[rows, :], whole.at[tp], tp_send.at[k], tp_recv.at[tp], tp=peer)

    def send_tp(k, _):
        tp_copy(k).start()
        return 0

    def tp_arrived(k, _):
        source = lax.rem(tp + k, TP)
        rows = pl.ds(pl.multiple_of(tp * ROWS, ROWS), ROWS)
        remote(mixed.at[rows, :], whole.at[source], tp_send.at[k], tp_recv.at[source], tp=source).wait_recv()
        return 0

    lax.fori_loop(1, TP, send_tp, 0)
    whole[tp] = mixed[pl.ds(pl.multiple_of(tp * ROWS, ROWS), ROWS), :]

    from_left_hi.wait_recv()
    from_right_lo.wait_recv()
    twin_left_hi = twin_copy(left, piece_hi, 2)
    twin_right_lo = twin_copy(right, piece_lo, 3)
    twin_left_hi.start()
    twin_right_lo.start()
    across_lo = ring(across, piece_lo, 0, 4)
    across_hi = ring(across, piece_hi, 1, 5)
    across_lo.wait_recv()
    twin_across_lo = twin_copy(across, piece_lo, 4)
    twin_across_lo.start()
    across_hi.wait_recv()
    twin_across_hi = twin_copy(across, piece_hi, 5)
    twin_across_hi.start()

    other = 2 * PIECE - half
    other_lo = pl.ds(pl.multiple_of(other, PIECE), PIECE)
    other_hi = pl.ds(pl.multiple_of(other + PIECE, PIECE), PIECE)
    lax.fori_loop(1, TP, tp_arrived, 0)

    for p in (4, 3, 5, 2):
        q = p - FAR // PLANE
        for piece in range(TP):
            lanes = slice(piece * 256, (piece + 1) * 256)
            mixed_out[q * PLANE : (q + 1) * PLANE, :, lanes] = blocks(p, whole[piece])
        lax.fori_loop(q * PLANE, (q + 1) * PLANE, send_mixed, 0)

    def hidden_of(pieces, residual_rows):
        squares = jnp.zeros((ROWS, 1), jnp.float32)
        mix = jnp.zeros((ROWS, WIDTH), jnp.float32)
        for q in range(TP):
            rows = pieces[q].astype(jnp.float32)
            squares += jnp.sum(rows * rows, axis=1, keepdims=True)
            scaled = (rows * gain_ref[:, q * 256 : (q + 1) * 256]).astype(jnp.bfloat16)
            mix += jnp.dot(scaled, gathered[q], preferred_element_type=jnp.float32)
        inverse = lax.rsqrt(squares / MIX_WIDTH + 1e-06)
        mix = deep_alpha * residual_rows.astype(jnp.float32) + mix * inverse
        return layer_norm(mix, mix_gain_ref[...]).astype(jnp.bfloat16)

    for slot, (block, piece) in enumerate(
        (
            (left, other_lo),
            (right, other_hi),
            (left, other_hi),
            (right, other_lo),
            (across, other_lo),
            (across, other_hi),
        )
    ):
        twin_copy(block, piece, slot).wait_recv()
    hidden_buf[...] = hidden_of([whole[q] for q in range(TP)], residual_ref[...])

    for p in (6, 1, 7, 0):
        outgoing[p * PLANE : (p + 1) * PLANE] = blocks(p, hidden_buf[...])
        lax.fori_loop(p * PLANE + (p == 0), (p + 1) * PLANE, send_out, 0)
    arrived[0] = outgoing[0]

    for load in loads[15:]:
        load.wait()

    def rows_of(buf, far, near):
        size = PLANE * CAPACITY
        return jnp.concatenate(
            [buf[pl.ds(far, PLANE)].reshape(size, -1), buf[pl.ds(near, PLANE)].reshape(size, -1)], axis=0
        )

    def expert(c, is_far):
        far = (PLANES // 2 + c) * PLANE
        near = (PLANES // 2 - 1 - c) * PLANE
        near_first = jnp.maximum(near, 1)

        def out_arrived(k, _):
            out_copy(k).wait_recv()
            return 0

        def mixed_arrived(k, _):
            mixed_copy(k).wait_recv()
            return 0

        def send_back(k, _):
            back_copy(k).start()
            return 0

        lax.fori_loop(far, far + PLANE, out_arrived, 0)
        lax.fori_loop(near_first, near + PLANE, out_arrived, 0)
        rows = rows_of(arrived, far, near)
        if is_far:
            lax.fori_loop(far - FAR, far - FAR + PLANE, mixed_arrived, 0)
            lax.fori_loop(near - FAR, near - FAR + PLANE, mixed_arrived, 0)
            mixed_rows = rows_of(mixed_in, far - FAR, near - FAR)
            rows = hidden_of([mixed_rows[:, q * 256 : (q + 1) * 256] for q in range(TP)], rows)
        gate_act = jnp.dot(rows, gate[...], preferred_element_type=jnp.float32)
        up_act = jnp.dot(rows, up[...], preferred_element_type=jnp.float32)
        active = (jax.nn.silu(gate_act) * up_act).astype(jnp.bfloat16)
        result = jnp.dot(active, down[...], preferred_element_type=jnp.float32).astype(jnp.bfloat16)
        produced[pl.ds(far, PLANE)] = result[: PLANE * CAPACITY].reshape(PLANE, CAPACITY, WIDTH)
        produced[pl.ds(near, PLANE)] = result[PLANE * CAPACITY :].reshape(PLANE, CAPACITY, WIDTH)
        lax.fori_loop(far, far + PLANE, send_back, 0)
        lax.fori_loop(near_first, near + PLANE, send_back, 0)

    def far_expert(c, _):
        expert(c, True)
        return 0

    def near_expert(c, _):
        expert(c, False)
        return 0

    lax.fori_loop(0, 2, far_expert, 0)
    lax.fori_loop(2, 4, near_expert, 0)
    returned[0] = produced[0]

    def back_arrived(k, _):
        back_copy(k).wait_recv()
        return 0

    lax.fori_loop(1, EXPERTS, back_arrived, 0)
    both = jnp.dot(
        combine_hi[...], returned[...].reshape(SLOTS, WIDTH), preferred_element_type=jnp.float32
    )
    expert_mix = both[:ROWS] + both[ROWS:]
    final = layer_norm(deep_alpha * hidden_buf[...].astype(jnp.float32) + expert_mix, final_gain_ref[...])
    layer_ref[...] = final.astype(jnp.bfloat16)

    def out_left(k, _):
        out_copy(k).wait_send()
        back_copy(k).wait_send()
        return 0

    def mixed_left(k, _):
        mixed_copy(k).wait_send()
        return 0

    lax.fori_loop(1, EXPERTS, out_left, 0)
    lax.fori_loop(0, FAR_BLOCKS, mixed_left, 0)

    def plane_left(k, _):
        plane_copy(k).wait_send()
        return 0

    def column_left(p, _):
        column_copy(p).wait_send()
        return 0

    def tp_left(k, _):
        tp_copy(k).wait_send()
        return 0

    lax.fori_loop(1, PLANE, plane_left, 0)
    lax.fori_loop(plane + 1, PLANES, column_left, 0)
    lax.fori_loop(1, TP, tp_left, 0)
    for copy in (to_right_lo, to_left_hi, to_right_hi, to_left_lo, pass_right, pass_left):
        copy.wait_send()
    for copy in (twin_left_lo, twin_right_hi, twin_left_hi, twin_right_lo, twin_across_lo, twin_across_hi):
        copy.wait_send()


def local(
    mixer_input,
    retention,
    decay_real,
    decay_freq,
    log_step,
    input_real,
    input_imag,
    readout_real,
    readout_imaginary,
    skip_weight,
    norm_gain,
    projection,
    residual,
    mix_gain,
    routes,
    route_weight,
    expert_gate,
    expert_up,
    expert_down,
    final_gain,
):
    hbm = pl.BlockSpec(memory_space=pltpu.HBM)
    smem = pl.BlockSpec(memory_space=pltpu.SMEM)
    vmem = pl.BlockSpec(memory_space=pltpu.VMEM)
    f32 = jnp.float32
    bf16 = jnp.bfloat16
    dma = pltpu.SemaphoreType.DMA
    small = (
        mixer_input,
        retention,
        decay_real,
        decay_freq,
        jnp.transpose(input_real, (0, 2, 1)),
        jnp.transpose(input_imag, (0, 2, 1)),
        readout_real,
        readout_imaginary,
        skip_weight,
        norm_gain.reshape(1, -1),
        residual,
        mix_gain.reshape(1, -1),
        jnp.transpose(routes),
        jnp.transpose(route_weight),
        final_gain.reshape(1, -1),
    )
    large = (projection, expert_gate, expert_up, expert_down)
    return pl.pallas_call(
        layer_kernel,
        out_shape=jax.ShapeDtypeStruct((ROWS, WIDTH), bf16),
        in_specs=[smem] + [hbm] * (len(small) + len(large)),
        out_specs=vmem,
        scratch_shapes=[pltpu.VMEM(a.shape, a.dtype) for a in small]
        + [
            pltpu.VMEM((WIDTH, HIDDEN), bf16),
            pltpu.VMEM((WIDTH, HIDDEN), bf16),
            pltpu.VMEM((HIDDEN, WIDTH), bf16),
            pltpu.VMEM((8, 256, 256), bf16),
            pltpu.VMEM((256, 256), bf16),
            pltpu.VMEM((TOKENS * 8, 128), f32),
            pltpu.VMEM((TOKENS * 8, 128), f32),
            pltpu.VMEM((TOKENS * 8, 128), f32),
            pltpu.VMEM((TOKENS * 8, 256), f32),
            pltpu.VMEM((3, 8, 128), f32),
            pltpu.VMEM((PLANE, 3, 8, 128), f32),
            pltpu.VMEM((3, 8, 128), f32),
            pltpu.VMEM((PLANES, 3, 8, 128), f32),
            pltpu.VMEM((TOKENS, 256), bf16),
            pltpu.VMEM((TP, ROWS, 256), bf16),
            pltpu.VMEM((TP, 256, WIDTH), bf16),
            pltpu.VMEM((2, GROUPS, STATE), f32),
            pltpu.VMEM((ROWS, WIDTH), bf16),
            pltpu.VMEM((2 * ROWS, SLOTS), bf16),
            pltpu.VMEM((SLOTS, ROWS), bf16),
            pltpu.VMEM((FAR_BLOCKS, CAPACITY, MIX_WIDTH), bf16),
            pltpu.VMEM((FAR_BLOCKS, CAPACITY, MIX_WIDTH), bf16),
            pltpu.VMEM((EXPERTS, CAPACITY, WIDTH), bf16),
            pltpu.VMEM((EXPERTS, CAPACITY, WIDTH), bf16),
            pltpu.VMEM((EXPERTS, CAPACITY, WIDTH), bf16),
            pltpu.VMEM((EXPERTS, CAPACITY, WIDTH), bf16),
            dma((18,)),
            dma((PLANE,)),
            dma((PLANE,)),
            dma((PLANES,)),
            dma((PLANES,)),
            dma((TP,)),
            dma((TP,)),
            dma(()),
            dma((6,)),
            dma((6,)),
            dma((6,)),
            dma((6,)),
            dma((EXPERTS,)),
            dma((EXPERTS,)),
            dma((EXPERTS,)),
            dma((EXPERTS,)),
            dma((FAR_BLOCKS,)),
            dma((FAR_BLOCKS,)),
        ],
        compiler_params=pltpu.CompilerParams(
            collective_id=0, has_side_effects=True, vmem_limit_bytes=62 * 1024 * 1024
        ),
        name="layer",
    )(log_step, *small, *large)


def solution(mesh):
    in_specs = (
        P("sp", "tp"),
        P("tp", "sp"),
        P("tp", None),
        P("tp", None),
        P("tp"),
        P("tp", None, None),
        P("tp", None, None),
        P("tp", None, None),
        P("tp", None, None),
        P("tp", None),
        P(),
        P("tp", None),
        P(("sp", "tp"), None),
        P(),
        P(("sp", "tp"), None),
        P(("sp", "tp"), None),
        P("sp", None, None),
        P("sp", None, None),
        P("sp", None, None),
        P(),
    )
    out_specs = P(("sp", "tp"), None)
    return jax.shard_map(local, mesh=mesh, in_specs=in_specs, out_specs=out_specs, check_vma=False)
```

```python
import jax
import jax.numpy as jnp
from jax import lax
from jax.experimental import pallas as pl
from jax.experimental.pallas import tpu as pltpu
from jax.sharding import PartitionSpec as P

PICKS = 2
MIX_WIDTH = 1024
MESH = pl.DeviceIdType.MESH

deep_alpha = 2.0**0.25

TOKENS = 256
GROUPS = 16
CHANNELS = 16
STATE = 64
WIDTH = 2048
ROWS = 64
PLANES = 8
PLANE = 8
TP = 4
PIECE = 64
EXPERTS = 64
CAPACITY = 4
SLOTS = EXPERTS * CAPACITY
HIDDEN = 512


def times(ar, ai, br, bi):
    return ar * br - ai * bi, ar * bi + ai * br


def layer_norm(values, scales):
    centered = values - jnp.mean(values, axis=-1, keepdims=True)
    variance = jnp.mean(centered * centered, axis=-1, keepdims=True)
    return centered * lax.rsqrt(variance + 1e-05) * scales


def pair_rows(ref):
    return jnp.concatenate(
        [ref[pl.ds(0, 8, stride=2), :], ref[pl.ds(1, 8, stride=2), :]], axis=1
    )


def remote(src, dst, send_sem, recv_sem, **where):
    return pltpu.make_async_remote_copy(
        src_ref=src,
        dst_ref=dst,
        send_sem=send_sem,
        recv_sem=recv_sem,
        device_id=where,
        device_id_type=MESH,
    )


def layer_kernel(
    step_ref,
    x_hbm,
    ret_hbm,
    real_hbm,
    freq_hbm,
    in_real_hbm,
    in_imag_hbm,
    out_real_hbm,
    out_imag_hbm,
    skip_hbm,
    gain_hbm,
    residual_hbm,
    mix_gain_hbm,
    routes_hbm,
    weight_hbm,
    final_gain_hbm,
    proj_ref,
    gate_hbm,
    up_hbm,
    down_hbm,
    layer_ref,
    x_ref,
    ret_ref,
    real_ref,
    freq_ref,
    in_real_ref,
    in_imag_ref,
    out_real_ref,
    out_imag_ref,
    skip_ref,
    gain_ref,
    residual_ref,
    mix_gain_ref,
    routes_ref,
    weight_ref,
    final_gain_ref,
    gate,
    up,
    down,
    drive_w,
    read_w,
    drive_re,
    drive_im,
    shrink,
    states,
    mine,
    plane_buf,
    plane_sum,
    column_buf,
    mixed,
    whole,
    gathered,
    param_buf,
    hidden_buf,
    combine_hi,
    pick,
    mixed_out,
    mixed_in,
    outgoing,
    arrived,
    produced,
    returned,
    load_sem,
    plane_send,
    plane_recv,
    column_send,
    column_recv,
    tp_send,
    tp_recv,
    own_sem,
    ring_send,
    ring_recv,
    twin_send,
    twin_recv,
    out_send,
    out_recv,
    back_send,
    back_recv,
    mixed_send,
    mixed_recv,
):
    sp = lax.axis_index("sp")
    tp = lax.axis_index("tp")
    plane = lax.div(sp, PLANE)
    place = lax.rem(sp, PLANE)
    core = lax.rem(sp, 2)
    twin = sp + 1 - 2 * core
    right = lax.rem(tp + 1, TP)
    left = lax.rem(tp + TP - 1, TP)
    across = lax.rem(tp + 2, TP)

    barrier = pltpu.get_barrier_semaphore()

    def greet_plane(k, _):
        peer = plane * PLANE + lax.rem(place + k, PLANE)
        pl.semaphore_signal(barrier, inc=1, device_id={"sp": peer}, device_id_type=MESH)
        return 0

    def greet_column(k, _):
        peer = lax.rem(plane + k, PLANES) * PLANE + place
        pl.semaphore_signal(barrier, inc=1, device_id={"sp": peer}, device_id_type=MESH)
        return 0

    def greet_tp(k, _):
        pl.semaphore_signal(
            barrier, inc=1, device_id={"tp": lax.rem(tp + k, TP)}, device_id_type=MESH
        )
        return 0

    lax.fori_loop(1, TP, greet_tp, 0)
    lax.fori_loop(1, PLANE, greet_plane, 0)
    lax.fori_loop(1, PLANES, greet_column, 0)

    own_copy = pltpu.make_async_copy(proj_ref, gathered.at[tp], own_sem)
    own_copy.start()
    loads = [
        pltpu.make_async_copy(source, target, load_sem.at[k])
        for k, (source, target) in enumerate(
            (
                (real_hbm, real_ref),
                (freq_hbm, freq_ref),
                (in_real_hbm, in_real_ref),
                (in_imag_hbm, in_imag_ref),
                (out_real_hbm, out_real_ref),
                (out_imag_hbm, out_imag_ref),
                (ret_hbm, ret_ref),
                (x_hbm, x_ref),
                (skip_hbm, skip_ref),
                (routes_hbm, routes_ref),
                (weight_hbm, weight_ref),
                (gain_hbm, gain_ref),
                (mix_gain_hbm, mix_gain_ref),
                (final_gain_hbm, final_gain_ref),
                (residual_hbm, residual_ref),
                (gate_hbm.at[0], gate),
                (up_hbm.at[0], up),
                (down_hbm.at[0], down),
            )
        )
    ]
    for load in loads:
        load.start()
    for load in loads[:8]:
        load.wait()

    group_row = lax.broadcasted_iota(jnp.int32, (GROUPS, STATE), 0)
    log_step = jnp.zeros((GROUPS, STATE), jnp.float32)
    for g in range(GROUPS):
        log_step = jnp.where(group_row == g, step_ref[g], log_step)
    stride = jnp.exp(log_step)
    decay_real = real_ref[...]
    decay_freq = freq_ref[...]
    growth = decay_real * stride
    turning = decay_freq * stride
    grown = jnp.exp(growth)
    cosine = jnp.cos(turning)
    sine = jnp.sin(turning)
    half_sine = jnp.sin(0.5 * turning)
    expm1 = jnp.tanh(0.5 * growth) * (grown + 1.0)
    upper_real = expm1 * cosine - 2.0 * half_sine * half_sine
    upper_imag = grown * sine
    denominator = decay_real * decay_real + decay_freq * decay_freq
    factor_real = (upper_real * decay_real + upper_imag * decay_freq) / denominator
    factor_imag = (upper_imag * decay_real - upper_real * decay_freq) / denominator
    param_buf[0] = grown * cosine
    param_buf[1] = grown * sine
    keep_re = pair_rows(param_buf.at[0])
    keep_im = pair_rows(param_buf.at[1])

    nothing = jnp.zeros((CHANNELS, STATE), jnp.float32)
    drive_w[...] = jnp.zeros(drive_w.shape, jnp.bfloat16)
    for g in range(GROUPS):
        rows = pl.ds(g * CHANNELS, CHANNELS)
        b_re = in_real_ref[g]
        b_im = in_imag_ref[g]
        c_re = out_real_ref[g]
        c_im = out_imag_ref[g]
        f_re = factor_real[g : g + 1, :]
        f_im = factor_imag[g : g + 1, :]
        r_re = c_re * f_re - c_im * f_im
        r_im = -(c_re * f_im + c_im * f_re)
        if g % 2 == 0:
            b_row = [b_re, nothing, b_im, nothing]
            r_row = [r_re, nothing, r_im, nothing]
        else:
            b_row = [nothing, b_re, nothing, b_im]
            r_row = [nothing, r_re, nothing, r_im]
        b_row = jnp.concatenate(b_row, axis=1)
        drive_w[g // 2, rows, :] = b_row.astype(jnp.bfloat16)
        read_w[rows, :] = jnp.concatenate(r_row, axis=1).astype(jnp.bfloat16)

    kept = jnp.transpose(jnp.exp(ret_ref[...]))
    kept_hi = kept.astype(jnp.bfloat16)
    rest = kept - kept_hi.astype(jnp.float32)
    kept_mid = rest.astype(jnp.bfloat16)
    kept_lo = (rest - kept_mid.astype(jnp.float32)).astype(jnp.bfloat16)
    select_row = lax.broadcasted_iota(jnp.int32, (GROUPS, 8 * 128), 0)
    select_lane = lax.broadcasted_iota(jnp.int32, (GROUPS, 8 * 128), 1)
    select = (select_row == lax.div(select_lane, STATE)).astype(jnp.bfloat16)
    spread = (
        jnp.dot(kept_hi, select, preferred_element_type=jnp.float32)
        + jnp.dot(kept_mid, select, preferred_element_type=jnp.float32)
        + jnp.dot(kept_lo, select, preferred_element_type=jnp.float32)
    )
    x = x_ref[...]
    for j in range(8):
        at = pl.ds(j, TOKENS, stride=8)
        driven = jnp.dot(x, drive_w[j], preferred_element_type=jnp.float32)
        drive_re[at, :] = driven[:, :128]
        drive_im[at, :] = driven[:, 128:]
        shrink[at, :] = spread[:, j * 128 : (j + 1) * 128]

    pl.semaphore_wait(barrier, (TP - 1) + (PLANE - 1) + (PLANES - 1))

    half = core * (2 * PIECE)
    piece_lo = pl.ds(pl.multiple_of(half, PIECE), PIECE)
    piece_hi = pl.ds(pl.multiple_of(half + PIECE, PIECE), PIECE)

    def ring(block, piece, way, slot):
        to = right if way == 0 else left
        return remote(
            gathered.at[block, piece, :],
            gathered.at[block, piece, :],
            ring_send.at[slot],
            ring_recv.at[slot],
            tp=to,
        )

    own_copy.wait()
    to_right_lo = ring(tp, piece_lo, 0, 0)
    to_left_hi = ring(tp, piece_hi, 1, 1)
    to_right_hi = ring(tp, piece_hi, 0, 2)
    to_left_lo = ring(tp, piece_lo, 1, 3)
    to_right_lo.start()
    to_left_hi.start()
    to_right_hi.start()
    to_left_lo.start()

    def advance(t, carried):
        s_re, s_im, decay = carried
        row = pl.ds(pl.multiple_of(t * 8, 8), 8)
        shr = shrink[row, :]
        a_re = shr * keep_re
        a_im = shr * keep_im
        n_re = (a_re * s_re - a_im * s_im) + drive_re[row, :]
        n_im = (a_re * s_im + a_im * s_re) + drive_im[row, :]
        return n_re, n_im, decay * shr

    zero = jnp.zeros((8, 128), jnp.float32)
    one = jnp.ones((8, 128), jnp.float32)
    end_re, end_im, decay = lax.fori_loop(0, TOKENS, advance, (zero, zero, one), unroll=8)
    mine[0] = end_re
    mine[1] = end_im
    mine[2] = decay

    power_re, power_im = keep_re, keep_im
    for _ in range(8):
        power_re, power_im = times(power_re, power_im, power_re, power_im)
    plane_re, plane_im = power_re, power_im
    for _ in range(3):
        plane_re, plane_im = times(plane_re, plane_im, plane_re, plane_im)

    def plane_copy(k):
        peer = plane * PLANE + lax.rem(place + k, PLANE)
        return remote(mine, plane_buf.at[place], plane_send.at[k], plane_recv.at[place], sp=peer)

    def send_plane(k, _):
        plane_copy(k).start()
        return 0

    def plane_arrived(k, _):
        source = lax.rem(place + k, PLANE)
        remote(
            mine, plane_buf.at[source], plane_send.at[k], plane_recv.at[source], sp=plane * PLANE + source
        ).wait_recv()
        return 0

    lax.fori_loop(1, PLANE, send_plane, 0)

    for load in loads[8:15]:
        load.wait()
    slot = lax.broadcasted_iota(jnp.int32, (SLOTS, ROWS), 0)
    slot_plane = lax.rem(plane + lax.shift_right_logical(slot, 5), PLANES)
    slot_place = lax.rem(place + lax.rem(lax.shift_right_logical(slot, 2), PLANE), PLANE)
    slot_expert = slot_plane * PLANE + slot_place
    first = jnp.where(routes_ref[0:1, :] == slot_expert, 1.0, 0.0)
    second = jnp.where(routes_ref[1:2, :] == slot_expert, 1.0, 0.0)
    named = first + second
    row_before = lax.broadcasted_iota(jnp.int32, (ROWS, ROWS), 0)
    row_at = lax.broadcasted_iota(jnp.int32, (ROWS, ROWS), 1)
    earlier = jnp.where(row_before < row_at, 1.0, 0.0).astype(jnp.bfloat16)
    rank = jnp.dot(named.astype(jnp.bfloat16), earlier, preferred_element_type=jnp.float32)
    here = jnp.where(rank == lax.rem(slot, CAPACITY).astype(jnp.float32), 1.0, 0.0)
    weights = jnp.transpose(here * (weight_ref[0:1, :] * first + weight_ref[1:2, :] * second))
    weights_hi = weights.astype(jnp.bfloat16)
    combine_hi[:ROWS, :] = weights_hi
    combine_hi[ROWS:, :] = (weights - weights_hi.astype(jnp.float32)).astype(jnp.bfloat16)
    pick[...] = (here * named).astype(jnp.bfloat16)

    def expert_of(k):
        return lax.rem(plane + lax.div(k, PLANE), PLANES) * PLANE + lax.rem(place + k, PLANE)

    def source_of(k):
        return lax.rem(plane + PLANES - lax.div(k, PLANE), PLANES) * PLANE + lax.rem(
            place + PLANE - lax.rem(k, PLANE), PLANE
        )

    def out_copy(k):
        return remote(outgoing.at[k], arrived.at[k], out_send.at[k], out_recv.at[k], sp=expert_of(k))

    def mixed_copy(k):
        return remote(
            mixed_out.at[k], mixed_in.at[k], mixed_send.at[k], mixed_recv.at[k], sp=expert_of(k)
        )

    def back_copy(k):
        return remote(produced.at[k], returned.at[k], back_send.at[k], back_recv.at[k], sp=source_of(k))

    def send_out(k, _):
        out_copy(k).start()
        return 0

    def send_mixed(k, _):
        mixed_copy(k).start()
        return 0

    def blocks(p, rows):
        picked = jnp.dot(pick[p * 32 : (p + 1) * 32, :], rows, preferred_element_type=jnp.float32)
        return picked.astype(jnp.bfloat16).reshape(PLANE, CAPACITY, rows.shape[1])

    for p in (2, 6, 3, 5):
        outgoing[p * PLANE : (p + 1) * PLANE] = blocks(p, residual_ref[...])

    lax.fori_loop(1, PLANE, plane_arrived, 0)
    plane_buf[place] = mine[...]

    def join(buf, k, carried, p_re, p_im):
        s_re, s_im, decay = carried
        d = buf[k, 2]
        m_re, m_im = times(d * p_re, d * p_im, s_re, s_im)
        return m_re + buf[k, 0], m_im + buf[k, 1], decay * d

    def join_place(k, carried):
        return join(plane_buf, k, carried, power_re, power_im)

    total = lax.fori_loop(0, PLANE, join_place, (zero, zero, one))
    plane_sum[0] = total[0]
    plane_sum[1] = total[1]
    plane_sum[2] = total[2]

    def column_copy(p):
        return remote(
            plane_sum, column_buf.at[plane], column_send.at[p], column_recv.at[plane], sp=p * PLANE + place
        )

    def send_column(p, _):
        column_copy(p).start()
        return 0

    def column_arrived(p, _):
        remote(
            plane_sum, column_buf.at[p], column_send.at[p], column_recv.at[p], sp=p * PLANE + place
        ).wait_recv()
        return 0

    lax.fori_loop(plane + 1, PLANES, send_column, 0)

    for p in (2, 6):
        lax.fori_loop(p * PLANE, (p + 1) * PLANE, send_out, 0)

    lax.fori_loop(0, plane, column_arrived, 0)

    for p in (3, 5):
        lax.fori_loop(p * PLANE, (p + 1) * PLANE, send_out, 0)

    def join_plane(p, carried):
        return join(column_buf, p, carried, plane_re, plane_im)

    carried = lax.fori_loop(0, plane, join_plane, (zero, zero, one))
    carried = lax.fori_loop(0, place, join_place, carried)

    def record(t, carried):
        s_re, s_im = carried
        row = pl.ds(pl.multiple_of(t * 8, 8), 8)
        shr = shrink[row, :]
        a_re = shr * keep_re
        a_im = shr * keep_im
        n_re = (a_re * s_re - a_im * s_im) + drive_re[row, :]
        n_im = (a_re * s_im + a_im * s_re) + drive_im[row, :]
        states[row, :128] = n_re
        states[row, 128:] = n_im
        return n_re, n_im

    lax.fori_loop(0, TOKENS, record, (carried[0], carried[1]), unroll=8)

    def read(k, _):
        at = pl.ds(pl.multiple_of(k * 256, 256), 256)
        product = lax.dot_general(
            states[at, :].astype(jnp.bfloat16),
            read_w[...],
            (((1,), (1,)), ((), ())),
            preferred_element_type=jnp.float32,
        )
        drive_re[at, :] = product[:, :128]
        drive_im[at, :] = product[:, 128:]
        return 0

    lax.fori_loop(0, 8, read, 0)
    lane = lax.broadcasted_iota(jnp.int32, (TOKENS, 128), 1)
    for side, buf in ((0, drive_re), (1, drive_im)):
        picked = jnp.zeros((TOKENS, 128), jnp.float32)
        for j in range(4):
            value = buf[pl.ds(side * 4 + j, TOKENS, stride=8), :]
            picked = jnp.where(lax.div(lane, 32) == j, value, picked)
        skip = jnp.concatenate([skip_ref[g : g + 1, :] for g in range(side * 8, side * 8 + 8)], axis=1)
        lanes = slice(side * 128, side * 128 + 128)
        read_out = picked + skip * x_ref[:, lanes].astype(jnp.float32)
        mixed[:, lanes] = jax.nn.gelu(read_out).astype(jnp.bfloat16)

    def tp_copy(k):
        peer = lax.rem(tp + k, TP)
        rows = pl.ds(pl.multiple_of(peer * ROWS, ROWS), ROWS)
        return remote(mixed.at[rows, :], whole.at[tp], tp_send.at[k], tp_recv.at[tp], tp=peer)

    def send_tp(k, _):
        tp_copy(k).start()
        return 0

    def tp_arrived(k, _):
        source = lax.rem(tp + k, TP)
        rows = pl.ds(pl.multiple_of(tp * ROWS, ROWS), ROWS)
        remote(mixed.at[rows, :], whole.at[source], tp_send.at[k], tp_recv.at[source], tp=source).wait_recv()
        return 0

    lax.fori_loop(1, TP, send_tp, 0)
    whole[tp] = mixed[pl.ds(pl.multiple_of(tp * ROWS, ROWS), ROWS), :]

    def twin_copy(block, piece, slot):
        return remote(
            gathered.at[block, piece, :],
            gathered.at[block, piece, :],
            twin_send.at[slot],
            twin_recv.at[slot],
            sp=twin,
        )

    from_left_lo = ring(left, piece_lo, 0, 0)
    from_right_hi = ring(right, piece_hi, 1, 1)
    from_left_hi = ring(left, piece_hi, 0, 2)
    from_right_lo = ring(right, piece_lo, 1, 3)
    from_left_lo.wait_recv()
    pass_right = ring(left, piece_lo, 0, 4)
    pass_right.start()
    from_right_hi.wait_recv()
    pass_left = ring(right, piece_hi, 1, 5)
    pass_left.start()
    twin_left_lo = twin_copy(left, piece_lo, 0)
    twin_right_hi = twin_copy(right, piece_hi, 1)
    twin_left_lo.start()
    twin_right_hi.start()
    from_left_hi.wait_recv()
    from_right_lo.wait_recv()
    twin_left_hi = twin_copy(left, piece_hi, 2)
    twin_right_lo = twin_copy(right, piece_lo, 3)
    twin_left_hi.start()
    twin_right_lo.start()

    lax.fori_loop(1, TP, tp_arrived, 0)

    for p in (3, 5, 2, 6):
        for piece in range(TP):
            lanes = slice(piece * 256, (piece + 1) * 256)
            mixed_out[p * PLANE : (p + 1) * PLANE, :, lanes] = blocks(p, whole[piece])
        lax.fori_loop(p * PLANE, (p + 1) * PLANE, send_mixed, 0)

    def hidden_of(pieces, residual_rows):
        squares = jnp.zeros((ROWS, 1), jnp.float32)
        mix = jnp.zeros((ROWS, WIDTH), jnp.float32)
        for q in range(TP):
            rows = pieces[q].astype(jnp.float32)
            squares += jnp.sum(rows * rows, axis=1, keepdims=True)
            scaled = (rows * gain_ref[:, q * 256 : (q + 1) * 256]).astype(jnp.bfloat16)
            mix += jnp.dot(scaled, gathered[q], preferred_element_type=jnp.float32)
        inverse = lax.rsqrt(squares / MIX_WIDTH + 1e-06)
        mix = deep_alpha * residual_rows.astype(jnp.float32) + mix * inverse
        return layer_norm(mix, mix_gain_ref[...]).astype(jnp.bfloat16)

    across_lo = ring(across, piece_lo, 0, 4)
    across_hi = ring(across, piece_hi, 1, 5)
    across_lo.wait_recv()
    twin_across_lo = twin_copy(across, piece_lo, 4)
    twin_across_lo.start()
    across_hi.wait_recv()
    twin_across_hi = twin_copy(across, piece_hi, 5)
    twin_across_hi.start()

    other = 2 * PIECE - half
    other_lo = pl.ds(pl.multiple_of(other, PIECE), PIECE)
    other_hi = pl.ds(pl.multiple_of(other + PIECE, PIECE), PIECE)
    for slot, (block, piece) in enumerate(
        (
            (left, other_lo),
            (right, other_hi),
            (left, other_hi),
            (right, other_lo),
            (across, other_lo),
            (across, other_hi),
        )
    ):
        twin_copy(block, piece, slot).wait_recv()
    hidden_buf[...] = hidden_of([whole[q] for q in range(TP)], residual_ref[...])

    for p in (4, 1, 7, 0):
        outgoing[p * PLANE : (p + 1) * PLANE] = blocks(p, hidden_buf[...])
        lax.fori_loop(p * PLANE + (p == 0), (p + 1) * PLANE, send_out, 0)
    arrived[0] = outgoing[0]

    for load in loads[15:]:
        load.wait()

    def rows_of(buf, far, near):
        size = PLANE * CAPACITY
        return jnp.concatenate(
            [buf[pl.ds(far, PLANE)].reshape(size, -1), buf[pl.ds(near, PLANE)].reshape(size, -1)], axis=0
        )

    def expert(far, near, is_far):
        near_first = jnp.maximum(near, 1)

        def out_arrived(k, _):
            out_copy(k).wait_recv()
            return 0

        def mixed_arrived(k, _):
            mixed_copy(k).wait_recv()
            return 0

        def send_back(k, _):
            back_copy(k).start()
            return 0

        lax.fori_loop(far, far + PLANE, out_arrived, 0)
        lax.fori_loop(near_first, near + PLANE, out_arrived, 0)
        rows = rows_of(arrived, far, near)
        if is_far:
            lax.fori_loop(far, far + PLANE, mixed_arrived, 0)
            lax.fori_loop(near, near + PLANE, mixed_arrived, 0)
            mixed_rows = rows_of(mixed_in, far, near)
            rows = hidden_of([mixed_rows[:, q * 256 : (q + 1) * 256] for q in range(TP)], rows)
        gate_act = jnp.dot(rows, gate[...], preferred_element_type=jnp.float32)
        up_act = jnp.dot(rows, up[...], preferred_element_type=jnp.float32)
        active = (jax.nn.silu(gate_act) * up_act).astype(jnp.bfloat16)
        result = jnp.dot(active, down[...], preferred_element_type=jnp.float32).astype(jnp.bfloat16)
        produced[pl.ds(far, PLANE)] = result[: PLANE * CAPACITY].reshape(PLANE, CAPACITY, WIDTH)
        produced[pl.ds(near, PLANE)] = result[PLANE * CAPACITY :].reshape(PLANE, CAPACITY, WIDTH)
        lax.fori_loop(far, far + PLANE, send_back, 0)
        lax.fori_loop(near_first, near + PLANE, send_back, 0)

    def far_expert(c, _):
        expert((5 + c) * PLANE, (3 - c) * PLANE, True)
        return 0

    def near_expert(c, _):
        expert((4 + 3 * c) * PLANE, c * PLANE, False)
        return 0

    lax.fori_loop(0, 2, far_expert, 0)
    lax.fori_loop(0, 2, near_expert, 0)
    returned[0] = produced[0]

    def out_left(k, _):
        out_copy(k).wait_send()
        back_copy(k).wait_send()
        return 0

    def mixed_left(k, _):
        mixed_copy(k).wait_send()
        return 0

    lax.fori_loop(1, EXPERTS, out_left, 0)
    for p in (2, 3, 5, 6):
        lax.fori_loop(p * PLANE, (p + 1) * PLANE, mixed_left, 0)

    def plane_left(k, _):
        plane_copy(k).wait_send()
        return 0

    def column_left(p, _):
        column_copy(p).wait_send()
        return 0

    def tp_left(k, _):
        tp_copy(k).wait_send()
        return 0

    lax.fori_loop(1, PLANE, plane_left, 0)
    lax.fori_loop(plane + 1, PLANES, column_left, 0)
    lax.fori_loop(1, TP, tp_left, 0)
    for copy in (to_right_lo, to_left_hi, to_right_hi, to_left_lo, pass_right, pass_left):
        copy.wait_send()
    for copy in (twin_left_lo, twin_right_hi, twin_left_hi, twin_right_lo, twin_across_lo, twin_across_hi):
        copy.wait_send()

    def back_arrived(k, _):
        back_copy(k).wait_recv()
        return 0

    lax.fori_loop(1, EXPERTS, back_arrived, 0)
    both = jnp.dot(
        combine_hi[...], returned[...].reshape(SLOTS, WIDTH), preferred_element_type=jnp.float32
    )
    expert_mix = both[:ROWS] + both[ROWS:]
    final = layer_norm(deep_alpha * hidden_buf[...].astype(jnp.float32) + expert_mix, final_gain_ref[...])
    layer_ref[...] = final.astype(jnp.bfloat16)


def local(
    mixer_input,
    retention,
    decay_real,
    decay_freq,
    log_step,
    input_real,
    input_imag,
    readout_real,
    readout_imaginary,
    skip_weight,
    norm_gain,
    projection,
    residual,
    mix_gain,
    routes,
    route_weight,
    expert_gate,
    expert_up,
    expert_down,
    final_gain,
):
    hbm = pl.BlockSpec(memory_space=pltpu.HBM)
    smem = pl.BlockSpec(memory_space=pltpu.SMEM)
    vmem = pl.BlockSpec(memory_space=pltpu.VMEM)
    f32 = jnp.float32
    bf16 = jnp.bfloat16
    dma = pltpu.SemaphoreType.DMA
    small = (
        mixer_input,
        retention,
        decay_real,
        decay_freq,
        jnp.transpose(input_real, (0, 2, 1)),
        jnp.transpose(input_imag, (0, 2, 1)),
        readout_real,
        readout_imaginary,
        skip_weight,
        norm_gain.reshape(1, -1),
        residual,
        mix_gain.reshape(1, -1),
        jnp.transpose(routes),
        jnp.transpose(route_weight),
        final_gain.reshape(1, -1),
    )
    large = (projection, expert_gate, expert_up, expert_down)
    return pl.pallas_call(
        layer_kernel,
        out_shape=jax.ShapeDtypeStruct((ROWS, WIDTH), bf16),
        in_specs=[smem] + [hbm] * (len(small) + len(large)),
        out_specs=vmem,
        scratch_shapes=[pltpu.VMEM(a.shape, a.dtype) for a in small]
        + [
            pltpu.VMEM((WIDTH, HIDDEN), bf16),
            pltpu.VMEM((WIDTH, HIDDEN), bf16),
            pltpu.VMEM((HIDDEN, WIDTH), bf16),
            pltpu.VMEM((8, 256, 256), bf16),
            pltpu.VMEM((256, 256), bf16),
            pltpu.VMEM((TOKENS * 8, 128), f32),
            pltpu.VMEM((TOKENS * 8, 128), f32),
            pltpu.VMEM((TOKENS * 8, 128), f32),
            pltpu.VMEM((TOKENS * 8, 256), f32),
            pltpu.VMEM((3, 8, 128), f32),
            pltpu.VMEM((PLANE, 3, 8, 128), f32),
            pltpu.VMEM((3, 8, 128), f32),
            pltpu.VMEM((PLANES, 3, 8, 128), f32),
            pltpu.VMEM((TOKENS, 256), bf16),
            pltpu.VMEM((TP, ROWS, 256), bf16),
            pltpu.VMEM((TP, 256, WIDTH), bf16),
            pltpu.VMEM((2, GROUPS, STATE), f32),
            pltpu.VMEM((ROWS, WIDTH), bf16),
            pltpu.VMEM((2 * ROWS, SLOTS), bf16),
            pltpu.VMEM((SLOTS, ROWS), bf16),
            pltpu.VMEM((EXPERTS, CAPACITY, MIX_WIDTH), bf16),
            pltpu.VMEM((EXPERTS, CAPACITY, MIX_WIDTH), bf16),
            pltpu.VMEM((EXPERTS, CAPACITY, WIDTH), bf16),
            pltpu.VMEM((EXPERTS, CAPACITY, WIDTH), bf16),
            pltpu.VMEM((EXPERTS, CAPACITY, WIDTH), bf16),
            pltpu.VMEM((EXPERTS, CAPACITY, WIDTH), bf16),
            dma((18,)),
            dma((PLANE,)),
            dma((PLANE,)),
            dma((PLANES,)),
            dma((PLANES,)),
            dma((TP,)),
            dma((TP,)),
            dma(()),
            dma((6,)),
            dma((6,)),
            dma((6,)),
            dma((6,)),
            dma((EXPERTS,)),
            dma((EXPERTS,)),
            dma((EXPERTS,)),
            dma((EXPERTS,)),
            dma((EXPERTS,)),
            dma((EXPERTS,)),
        ],
        compiler_params=pltpu.CompilerParams(
            collective_id=0, has_side_effects=True, vmem_limit_bytes=62 * 1024 * 1024
        ),
        name="layer",
    )(log_step, *small, *large)


def solution(mesh):
    in_specs = (
        P("sp", "tp"),
        P("tp", "sp"),
        P("tp", None),
        P("tp", None),
        P("tp"),
        P("tp", None, None),
        P("tp", None, None),
        P("tp", None, None),
        P("tp", None, None),
        P("tp", None),
        P(),
        P("tp", None),
        P(("sp", "tp"), None),
        P(),
        P(("sp", "tp"), None),
        P(("sp", "tp"), None),
        P("sp", None, None),
        P("sp", None, None),
        P("sp", None, None),
        P(),
    )
    out_specs = P(("sp", "tp"), None)
    return jax.shard_map(local, mesh=mesh, in_specs=in_specs, out_specs=out_specs, check_vma=False)
```

```python
import jax
import jax.numpy as jnp
from jax import lax
from jax.experimental import pallas as pl
from jax.experimental.pallas import tpu as pltpu
from jax.sharding import PartitionSpec as P

PICKS = 2
MIX_WIDTH = 1024
MESH = pl.DeviceIdType.MESH

deep_alpha = 2.0**0.25

TOKENS = 256
GROUPS = 16
CHANNELS = 16
STATE = 64
WIDTH = 2048
ROWS = 64
PLANES = 8
PLANE = 8
TP = 4
PIECE = 64
EXPERTS = 64
CAPACITY = 4
SLOTS = EXPERTS * CAPACITY
HIDDEN = 512


def times(ar, ai, br, bi):
    return ar * br - ai * bi, ar * bi + ai * br


def layer_norm(values, scales):
    centered = values - jnp.mean(values, axis=-1, keepdims=True)
    variance = jnp.mean(centered * centered, axis=-1, keepdims=True)
    return centered * lax.rsqrt(variance + 1e-05) * scales


def pair_rows(ref):
    return jnp.concatenate(
        [ref[pl.ds(0, 8, stride=2), :], ref[pl.ds(1, 8, stride=2), :]], axis=1
    )


def remote(src, dst, send_sem, recv_sem, **where):
    return pltpu.make_async_remote_copy(
        src_ref=src,
        dst_ref=dst,
        send_sem=send_sem,
        recv_sem=recv_sem,
        device_id=where,
        device_id_type=MESH,
    )


def layer_kernel(
    step_ref,
    x_hbm,
    ret_hbm,
    real_hbm,
    freq_hbm,
    in_real_hbm,
    in_imag_hbm,
    out_real_hbm,
    out_imag_hbm,
    skip_hbm,
    gain_hbm,
    residual_hbm,
    mix_gain_hbm,
    routes_hbm,
    weight_hbm,
    final_gain_hbm,
    proj_ref,
    gate_hbm,
    up_hbm,
    down_hbm,
    layer_ref,
    x_ref,
    ret_ref,
    real_ref,
    freq_ref,
    in_real_ref,
    in_imag_ref,
    out_real_ref,
    out_imag_ref,
    skip_ref,
    gain_ref,
    residual_ref,
    mix_gain_ref,
    routes_ref,
    weight_ref,
    final_gain_ref,
    gate,
    up,
    down,
    drive_w,
    read_w,
    drive_re,
    drive_im,
    shrink,
    states,
    mine,
    plane_buf,
    plane_sum,
    column_buf,
    mixed,
    whole,
    gathered,
    param_buf,
    hidden_buf,
    combine_hi,
    pick,
    mixed_out,
    mixed_in,
    outgoing,
    arrived,
    produced,
    returned,
    load_sem,
    plane_send,
    plane_recv,
    column_send,
    column_recv,
    tp_send,
    tp_recv,
    own_sem,
    ring_send,
    ring_recv,
    twin_send,
    twin_recv,
    out_send,
    out_recv,
    back_send,
    back_recv,
    mixed_send,
    mixed_recv,
):
    sp = lax.axis_index("sp")
    tp = lax.axis_index("tp")
    plane = lax.div(sp, PLANE)
    place = lax.rem(sp, PLANE)
    core = lax.rem(sp, 2)
    twin = sp + 1 - 2 * core
    right = lax.rem(tp + 1, TP)
    left = lax.rem(tp + TP - 1, TP)
    across = lax.rem(tp + 2, TP)

    barrier = pltpu.get_barrier_semaphore()

    def greet_plane(k, _):
        peer = plane * PLANE + lax.rem(place + k, PLANE)
        pl.semaphore_signal(barrier, inc=1, device_id={"sp": peer}, device_id_type=MESH)
        return 0

    def greet_column(k, _):
        peer = lax.rem(plane + k, PLANES) * PLANE + place
        pl.semaphore_signal(barrier, inc=1, device_id={"sp": peer}, device_id_type=MESH)
        return 0

    def greet_tp(k, _):
        pl.semaphore_signal(
            barrier, inc=1, device_id={"tp": lax.rem(tp + k, TP)}, device_id_type=MESH
        )
        return 0

    lax.fori_loop(1, TP, greet_tp, 0)
    lax.fori_loop(1, PLANE, greet_plane, 0)
    lax.fori_loop(1, PLANES, greet_column, 0)

    own_copy = pltpu.make_async_copy(proj_ref, gathered.at[tp], own_sem)
    own_copy.start()
    loads = [
        pltpu.make_async_copy(source, target, load_sem.at[k])
        for k, (source, target) in enumerate(
            (
                (real_hbm, real_ref),
                (freq_hbm, freq_ref),
                (in_real_hbm, in_real_ref),
                (in_imag_hbm, in_imag_ref),
                (out_real_hbm, out_real_ref),
                (out_imag_hbm, out_imag_ref),
                (ret_hbm, ret_ref),
                (x_hbm, x_ref),
                (skip_hbm, skip_ref),
                (routes_hbm, routes_ref),
                (weight_hbm, weight_ref),
                (gain_hbm, gain_ref),
                (mix_gain_hbm, mix_gain_ref),
                (final_gain_hbm, final_gain_ref),
                (residual_hbm, residual_ref),
                (gate_hbm.at[0], gate),
                (up_hbm.at[0], up),
                (down_hbm.at[0], down),
            )
        )
    ]
    for load in loads:
        load.start()
    for load in loads[:8]:
        load.wait()

    group_row = lax.broadcasted_iota(jnp.int32, (GROUPS, STATE), 0)
    log_step = jnp.zeros((GROUPS, STATE), jnp.float32)
    for g in range(GROUPS):
        log_step = jnp.where(group_row == g, step_ref[g], log_step)
    stride = jnp.exp(log_step)
    decay_real = real_ref[...]
    decay_freq = freq_ref[...]
    growth = decay_real * stride
    turning = decay_freq * stride
    grown = jnp.exp(growth)
    cosine = jnp.cos(turning)
    sine = jnp.sin(turning)
    half_sine = jnp.sin(0.5 * turning)
    expm1 = jnp.tanh(0.5 * growth) * (grown + 1.0)
    upper_real = expm1 * cosine - 2.0 * half_sine * half_sine
    upper_imag = grown * sine
    denominator = decay_real * decay_real + decay_freq * decay_freq
    factor_real = (upper_real * decay_real + upper_imag * decay_freq) / denominator
    factor_imag = (upper_imag * decay_real - upper_real * decay_freq) / denominator
    param_buf[0] = grown * cosine
    param_buf[1] = grown * sine
    keep_re = pair_rows(param_buf.at[0])
    keep_im = pair_rows(param_buf.at[1])

    nothing = jnp.zeros((CHANNELS, STATE), jnp.float32)
    drive_w[...] = jnp.zeros(drive_w.shape, jnp.bfloat16)
    for g in range(GROUPS):
        rows = pl.ds(g * CHANNELS, CHANNELS)
        b_re = in_real_ref[g]
        b_im = in_imag_ref[g]
        c_re = out_real_ref[g]
        c_im = out_imag_ref[g]
        f_re = factor_real[g : g + 1, :]
        f_im = factor_imag[g : g + 1, :]
        r_re = c_re * f_re - c_im * f_im
        r_im = -(c_re * f_im + c_im * f_re)
        if g % 2 == 0:
            b_row = [b_re, nothing, b_im, nothing]
            r_row = [r_re, nothing, r_im, nothing]
        else:
            b_row = [nothing, b_re, nothing, b_im]
            r_row = [nothing, r_re, nothing, r_im]
        b_row = jnp.concatenate(b_row, axis=1)
        drive_w[g // 2, rows, :] = b_row.astype(jnp.bfloat16)
        read_w[rows, :] = jnp.concatenate(r_row, axis=1).astype(jnp.bfloat16)

    kept = jnp.transpose(jnp.exp(ret_ref[...]))
    kept_hi = kept.astype(jnp.bfloat16)
    rest = kept - kept_hi.astype(jnp.float32)
    kept_mid = rest.astype(jnp.bfloat16)
    kept_lo = (rest - kept_mid.astype(jnp.float32)).astype(jnp.bfloat16)
    select_row = lax.broadcasted_iota(jnp.int32, (GROUPS, 8 * 128), 0)
    select_lane = lax.broadcasted_iota(jnp.int32, (GROUPS, 8 * 128), 1)
    select = (select_row == lax.div(select_lane, STATE)).astype(jnp.bfloat16)
    spread = (
        jnp.dot(kept_hi, select, preferred_element_type=jnp.float32)
        + jnp.dot(kept_mid, select, preferred_element_type=jnp.float32)
        + jnp.dot(kept_lo, select, preferred_element_type=jnp.float32)
    )
    x = x_ref[...]
    for j in range(8):
        at = pl.ds(j, TOKENS, stride=8)
        driven = jnp.dot(x, drive_w[j], preferred_element_type=jnp.float32)
        drive_re[at, :] = driven[:, :128]
        drive_im[at, :] = driven[:, 128:]
        shrink[at, :] = spread[:, j * 128 : (j + 1) * 128]

    pl.semaphore_wait(barrier, (TP - 1) + (PLANE - 1) + (PLANES - 1))

    half = core * (2 * PIECE)
    piece_lo = pl.ds(pl.multiple_of(half, PIECE), PIECE)
    piece_hi = pl.ds(pl.multiple_of(half + PIECE, PIECE), PIECE)

    def ring(block, piece, way, slot):
        to = right if way == 0 else left
        return remote(
            gathered.at[block, piece, :],
            gathered.at[block, piece, :],
            ring_send.at[slot],
            ring_recv.at[slot],
            tp=to,
        )

    own_copy.wait()
    to_right_lo = ring(tp, piece_lo, 0, 0)
    to_left_hi = ring(tp, piece_hi, 1, 1)
    to_right_hi = ring(tp, piece_hi, 0, 2)
    to_left_lo = ring(tp, piece_lo, 1, 3)
    to_right_lo.start()
    to_left_hi.start()
    to_right_hi.start()
    to_left_lo.start()

    def advance(t, carried):
        s_re, s_im, decay = carried
        row = pl.ds(pl.multiple_of(t * 8, 8), 8)
        shr = shrink[row, :]
        a_re = shr * keep_re
        a_im = shr * keep_im
        n_re = (a_re * s_re - a_im * s_im) + drive_re[row, :]
        n_im = (a_re * s_im + a_im * s_re) + drive_im[row, :]
        return n_re, n_im, decay * shr

    zero = jnp.zeros((8, 128), jnp.float32)
    one = jnp.ones((8, 128), jnp.float32)
    end_re, end_im, decay = lax.fori_loop(0, TOKENS, advance, (zero, zero, one), unroll=8)
    mine[0] = end_re
    mine[1] = end_im
    mine[2] = decay

    power_re, power_im = keep_re, keep_im
    for _ in range(8):
        power_re, power_im = times(power_re, power_im, power_re, power_im)
    plane_re, plane_im = power_re, power_im
    for _ in range(3):
        plane_re, plane_im = times(plane_re, plane_im, plane_re, plane_im)

    def plane_copy(k):
        peer = plane * PLANE + lax.rem(place + k, PLANE)
        return remote(mine, plane_buf.at[place], plane_send.at[k], plane_recv.at[place], sp=peer)

    def send_plane(k, _):
        plane_copy(k).start()
        return 0

    def plane_arrived(k, _):
        source = lax.rem(place + k, PLANE)
        remote(
            mine, plane_buf.at[source], plane_send.at[k], plane_recv.at[source], sp=plane * PLANE + source
        ).wait_recv()
        return 0

    lax.fori_loop(1, PLANE, send_plane, 0)

    for load in loads[8:15]:
        load.wait()
    slot = lax.broadcasted_iota(jnp.int32, (SLOTS, ROWS), 0)
    slot_plane = lax.rem(plane + lax.shift_right_logical(slot, 5), PLANES)
    slot_place = lax.rem(place + lax.rem(lax.shift_right_logical(slot, 2), PLANE), PLANE)
    slot_expert = slot_plane * PLANE + slot_place
    first = jnp.where(routes_ref[0:1, :] == slot_expert, 1.0, 0.0)
    second = jnp.where(routes_ref[1:2, :] == slot_expert, 1.0, 0.0)
    named = first + second
    row_before = lax.broadcasted_iota(jnp.int32, (ROWS, ROWS), 0)
    row_at = lax.broadcasted_iota(jnp.int32, (ROWS, ROWS), 1)
    earlier = jnp.where(row_before < row_at, 1.0, 0.0).astype(jnp.bfloat16)
    rank = jnp.dot(named.astype(jnp.bfloat16), earlier, preferred_element_type=jnp.float32)
    here = jnp.where(rank == lax.rem(slot, CAPACITY).astype(jnp.float32), 1.0, 0.0)
    weights = jnp.transpose(here * (weight_ref[0:1, :] * first + weight_ref[1:2, :] * second))
    weights_hi = weights.astype(jnp.bfloat16)
    combine_hi[:ROWS, :] = weights_hi
    combine_hi[ROWS:, :] = (weights - weights_hi.astype(jnp.float32)).astype(jnp.bfloat16)
    pick[...] = (here * named).astype(jnp.bfloat16)

    def expert_of(k):
        return lax.rem(plane + lax.div(k, PLANE), PLANES) * PLANE + lax.rem(place + k, PLANE)

    def source_of(k):
        return lax.rem(plane + PLANES - lax.div(k, PLANE), PLANES) * PLANE + lax.rem(
            place + PLANE - lax.rem(k, PLANE), PLANE
        )

    def out_copy(k):
        return remote(outgoing.at[k], arrived.at[k], out_send.at[k], out_recv.at[k], sp=expert_of(k))

    def mixed_copy(k):
        return remote(
            mixed_out.at[k], mixed_in.at[k], mixed_send.at[k], mixed_recv.at[k], sp=expert_of(k)
        )

    def back_copy(k):
        return remote(produced.at[k], returned.at[k], back_send.at[k], back_recv.at[k], sp=source_of(k))

    def send_out(k, _):
        out_copy(k).start()
        return 0

    def send_mixed(k, _):
        mixed_copy(k).start()
        return 0

    def blocks(p, rows):
        picked = jnp.dot(pick[p * 32 : (p + 1) * 32, :], rows, preferred_element_type=jnp.float32)
        return picked.astype(jnp.bfloat16).reshape(PLANE, CAPACITY, rows.shape[1])

    for p in (2, 6, 3, 5):
        outgoing[p * PLANE : (p + 1) * PLANE] = blocks(p, residual_ref[...])

    lax.fori_loop(1, PLANE, plane_arrived, 0)
    plane_buf[place] = mine[...]

    def join(buf, k, carried, p_re, p_im):
        s_re, s_im, decay = carried
        d = buf[k, 2]
        m_re, m_im = times(d * p_re, d * p_im, s_re, s_im)
        return m_re + buf[k, 0], m_im + buf[k, 1], decay * d

    def join_place(k, carried):
        return join(plane_buf, k, carried, power_re, power_im)

    total = lax.fori_loop(0, PLANE, join_place, (zero, zero, one))
    plane_sum[0] = total[0]
    plane_sum[1] = total[1]
    plane_sum[2] = total[2]

    def column_copy(p):
        return remote(
            plane_sum, column_buf.at[plane], column_send.at[p], column_recv.at[plane], sp=p * PLANE + place
        )

    def send_column(p, _):
        column_copy(p).start()
        return 0

    def column_arrived(p, _):
        remote(
            plane_sum, column_buf.at[p], column_send.at[p], column_recv.at[p], sp=p * PLANE + place
        ).wait_recv()
        return 0

    lax.fori_loop(plane + 1, PLANES, send_column, 0)

    for p in (2, 6):
        lax.fori_loop(p * PLANE, (p + 1) * PLANE, send_out, 0)

    lax.fori_loop(0, plane, column_arrived, 0)

    for p in (3, 5):
        lax.fori_loop(p * PLANE, (p + 1) * PLANE, send_out, 0)

    def join_plane(p, carried):
        return join(column_buf, p, carried, plane_re, plane_im)

    carried = lax.fori_loop(0, plane, join_plane, (zero, zero, one))
    carried = lax.fori_loop(0, place, join_place, carried)

    def record(t, carried):
        s_re, s_im = carried
        row = pl.ds(pl.multiple_of(t * 8, 8), 8)
        shr = shrink[row, :]
        a_re = shr * keep_re
        a_im = shr * keep_im
        n_re = (a_re * s_re - a_im * s_im) + drive_re[row, :]
        n_im = (a_re * s_im + a_im * s_re) + drive_im[row, :]
        states[row, :128] = n_re
        states[row, 128:] = n_im
        return n_re, n_im

    lax.fori_loop(0, TOKENS, record, (carried[0], carried[1]), unroll=8)

    def read(k, _):
        at = pl.ds(pl.multiple_of(k * 1024, 1024), 1024)
        product = lax.dot_general(
            states[at, :].astype(jnp.bfloat16),
            read_w[...],
            (((1,), (1,)), ((), ())),
            preferred_element_type=jnp.float32,
        )
        drive_re[at, :] = product[:, :128]
        drive_im[at, :] = product[:, 128:]
        return 0

    lax.fori_loop(0, 2, read, 0)
    lane = lax.broadcasted_iota(jnp.int32, (TOKENS, 128), 1)
    for side, buf in ((0, drive_re), (1, drive_im)):
        picked = jnp.zeros((TOKENS, 128), jnp.float32)
        for j in range(4):
            value = buf[pl.ds(side * 4 + j, TOKENS, stride=8), :]
            picked = jnp.where(lax.div(lane, 32) == j, value, picked)
        skip = jnp.concatenate([skip_ref[g : g + 1, :] for g in range(side * 8, side * 8 + 8)], axis=1)
        lanes = slice(side * 128, side * 128 + 128)
        read_out = picked + skip * x_ref[:, lanes].astype(jnp.float32)
        mixed[:, lanes] = jax.nn.gelu(read_out).astype(jnp.bfloat16)

    def tp_copy(k):
        peer = lax.rem(tp + k, TP)
        rows = pl.ds(pl.multiple_of(peer * ROWS, ROWS), ROWS)
        return remote(mixed.at[rows, :], whole.at[tp], tp_send.at[k], tp_recv.at[tp], tp=peer)

    def send_tp(k, _):
        tp_copy(k).start()
        return 0

    def tp_arrived(k, _):
        source = lax.rem(tp + k, TP)
        rows = pl.ds(pl.multiple_of(tp * ROWS, ROWS), ROWS)
        remote(mixed.at[rows, :], whole.at[source], tp_send.at[k], tp_recv.at[source], tp=source).wait_recv()
        return 0

    lax.fori_loop(1, TP, send_tp, 0)
    whole[tp] = mixed[pl.ds(pl.multiple_of(tp * ROWS, ROWS), ROWS), :]

    def twin_copy(block, piece, slot):
        return remote(
            gathered.at[block, piece, :],
            gathered.at[block, piece, :],
            twin_send.at[slot],
            twin_recv.at[slot],
            sp=twin,
        )

    from_left_lo = ring(left, piece_lo, 0, 0)
    from_right_hi = ring(right, piece_hi, 1, 1)
    from_left_hi = ring(left, piece_hi, 0, 2)
    from_right_lo = ring(right, piece_lo, 1, 3)
    from_left_lo.wait_recv()
    pass_right = ring(left, piece_lo, 0, 4)
    pass_right.start()
    from_right_hi.wait_recv()
    pass_left = ring(right, piece_hi, 1, 5)
    pass_left.start()
    twin_left_lo = twin_copy(left, piece_lo, 0)
    twin_right_hi = twin_copy(right, piece_hi, 1)
    twin_left_lo.start()
    twin_right_hi.start()
    from_left_hi.wait_recv()
    from_right_lo.wait_recv()
    twin_left_hi = twin_copy(left, piece_hi, 2)
    twin_right_lo = twin_copy(right, piece_lo, 3)
    twin_left_hi.start()
    twin_right_lo.start()

    lax.fori_loop(1, TP, tp_arrived, 0)

    for p in (3, 5, 2, 6):
        for piece in range(TP):
            lanes = slice(piece * 256, (piece + 1) * 256)
            mixed_out[p * PLANE : (p + 1) * PLANE, :, lanes] = blocks(p, whole[piece])
        lax.fori_loop(p * PLANE, (p + 1) * PLANE, send_mixed, 0)

    def hidden_of(pieces, residual_rows):
        squares = jnp.zeros((ROWS, 1), jnp.float32)
        mix = jnp.zeros((ROWS, WIDTH), jnp.float32)
        for q in range(TP):
            rows = pieces[q].astype(jnp.float32)
            squares += jnp.sum(rows * rows, axis=1, keepdims=True)
            scaled = (rows * gain_ref[:, q * 256 : (q + 1) * 256]).astype(jnp.bfloat16)
            mix += jnp.dot(scaled, gathered[q], preferred_element_type=jnp.float32)
        inverse = lax.rsqrt(squares / MIX_WIDTH + 1e-06)
        mix = deep_alpha * residual_rows.astype(jnp.float32) + mix * inverse
        return layer_norm(mix, mix_gain_ref[...]).astype(jnp.bfloat16)

    across_lo = ring(across, piece_lo, 0, 4)
    across_hi = ring(across, piece_hi, 1, 5)
    across_lo.wait_recv()
    twin_across_lo = twin_copy(across, piece_lo, 4)
    twin_across_lo.start()
    across_hi.wait_recv()
    twin_across_hi = twin_copy(across, piece_hi, 5)
    twin_across_hi.start()

    other = 2 * PIECE - half
    other_lo = pl.ds(pl.multiple_of(other, PIECE), PIECE)
    other_hi = pl.ds(pl.multiple_of(other + PIECE, PIECE), PIECE)
    for slot, (block, piece) in enumerate(
        (
            (left, other_lo),
            (right, other_hi),
            (left, other_hi),
            (right, other_lo),
            (across, other_lo),
            (across, other_hi),
        )
    ):
        twin_copy(block, piece, slot).wait_recv()
    hidden_buf[...] = hidden_of([whole[q] for q in range(TP)], residual_ref[...])

    for p in (4, 1, 7, 0):
        outgoing[p * PLANE : (p + 1) * PLANE] = blocks(p, hidden_buf[...])
        lax.fori_loop(p * PLANE + (p == 0), (p + 1) * PLANE, send_out, 0)
    arrived[0] = outgoing[0]

    for load in loads[15:]:
        load.wait()

    def rows_of(buf, far, near):
        size = PLANE * CAPACITY
        return jnp.concatenate(
            [buf[pl.ds(far, PLANE)].reshape(size, -1), buf[pl.ds(near, PLANE)].reshape(size, -1)], axis=0
        )

    def expert(far, near, is_far):
        near_first = jnp.maximum(near, 1)

        def out_arrived(k, _):
            out_copy(k).wait_recv()
            return 0

        def mixed_arrived(k, _):
            mixed_copy(k).wait_recv()
            return 0

        def send_back(k, _):
            back_copy(k).start()
            return 0

        lax.fori_loop(far, far + PLANE, out_arrived, 0)
        lax.fori_loop(near_first, near + PLANE, out_arrived, 0)
        rows = rows_of(arrived, far, near)
        if is_far:
            lax.fori_loop(far, far + PLANE, mixed_arrived, 0)
            lax.fori_loop(near, near + PLANE, mixed_arrived, 0)
            mixed_rows = rows_of(mixed_in, far, near)
            rows = hidden_of([mixed_rows[:, q * 256 : (q + 1) * 256] for q in range(TP)], rows)
        gate_act = jnp.dot(rows, gate[...], preferred_element_type=jnp.float32)
        up_act = jnp.dot(rows, up[...], preferred_element_type=jnp.float32)
        active = (jax.nn.silu(gate_act) * up_act).astype(jnp.bfloat16)
        result = jnp.dot(active, down[...], preferred_element_type=jnp.float32).astype(jnp.bfloat16)
        produced[pl.ds(far, PLANE)] = result[: PLANE * CAPACITY].reshape(PLANE, CAPACITY, WIDTH)
        produced[pl.ds(near, PLANE)] = result[PLANE * CAPACITY :].reshape(PLANE, CAPACITY, WIDTH)
        lax.fori_loop(far, far + PLANE, send_back, 0)
        lax.fori_loop(near_first, near + PLANE, send_back, 0)

    def far_expert(c, _):
        expert((5 + c) * PLANE, (3 - c) * PLANE, True)
        return 0

    def near_expert(c, _):
        expert((4 + 3 * c) * PLANE, c * PLANE, False)
        return 0

    lax.fori_loop(0, 2, far_expert, 0)
    lax.fori_loop(0, 2, near_expert, 0)
    returned[0] = produced[0]

    def out_left(k, _):
        out_copy(k).wait_send()
        back_copy(k).wait_send()
        return 0

    def mixed_left(k, _):
        mixed_copy(k).wait_send()
        return 0

    lax.fori_loop(1, EXPERTS, out_left, 0)
    for p in (2, 3, 5, 6):
        lax.fori_loop(p * PLANE, (p + 1) * PLANE, mixed_left, 0)

    def plane_left(k, _):
        plane_copy(k).wait_send()
        return 0

    def column_left(p, _):
        column_copy(p).wait_send()
        return 0

    def tp_left(k, _):
        tp_copy(k).wait_send()
        return 0

    lax.fori_loop(1, PLANE, plane_left, 0)
    lax.fori_loop(plane + 1, PLANES, column_left, 0)
    lax.fori_loop(1, TP, tp_left, 0)
    for copy in (to_right_lo, to_left_hi, to_right_hi, to_left_lo, pass_right, pass_left):
        copy.wait_send()
    for copy in (twin_left_lo, twin_right_hi, twin_left_hi, twin_right_lo, twin_across_lo, twin_across_hi):
        copy.wait_send()

    def back_arrived(k, _):
        back_copy(k).wait_recv()
        return 0

    lax.fori_loop(1, EXPERTS, back_arrived, 0)
    both = jnp.dot(
        combine_hi[...], returned[...].reshape(SLOTS, WIDTH), preferred_element_type=jnp.float32
    )
    expert_mix = both[:ROWS] + both[ROWS:]
    final = layer_norm(deep_alpha * hidden_buf[...].astype(jnp.float32) + expert_mix, final_gain_ref[...])
    layer_ref[...] = final.astype(jnp.bfloat16)


def local(
    mixer_input,
    retention,
    decay_real,
    decay_freq,
    log_step,
    input_real,
    input_imag,
    readout_real,
    readout_imaginary,
    skip_weight,
    norm_gain,
    projection,
    residual,
    mix_gain,
    routes,
    route_weight,
    expert_gate,
    expert_up,
    expert_down,
    final_gain,
):
    hbm = pl.BlockSpec(memory_space=pltpu.HBM)
    smem = pl.BlockSpec(memory_space=pltpu.SMEM)
    vmem = pl.BlockSpec(memory_space=pltpu.VMEM)
    f32 = jnp.float32
    bf16 = jnp.bfloat16
    dma = pltpu.SemaphoreType.DMA
    small = (
        mixer_input,
        retention,
        decay_real,
        decay_freq,
        jnp.transpose(input_real, (0, 2, 1)),
        jnp.transpose(input_imag, (0, 2, 1)),
        readout_real,
        readout_imaginary,
        skip_weight,
        norm_gain.reshape(1, -1),
        residual,
        mix_gain.reshape(1, -1),
        jnp.transpose(routes),
        jnp.transpose(route_weight),
        final_gain.reshape(1, -1),
    )
    large = (projection, expert_gate, expert_up, expert_down)
    return pl.pallas_call(
        layer_kernel,
        out_shape=pltpu.VMEM((ROWS, WIDTH), bf16),
        in_specs=[smem] + [hbm] * (len(small) + len(large)),
        out_specs=vmem,
        scratch_shapes=[pltpu.VMEM(a.shape, a.dtype) for a in small]
        + [
            pltpu.VMEM((WIDTH, HIDDEN), bf16),
            pltpu.VMEM((WIDTH, HIDDEN), bf16),
            pltpu.VMEM((HIDDEN, WIDTH), bf16),
            pltpu.VMEM((8, 256, 256), bf16),
            pltpu.VMEM((256, 256), bf16),
            pltpu.VMEM((TOKENS * 8, 128), f32),
            pltpu.VMEM((TOKENS * 8, 128), f32),
            pltpu.VMEM((TOKENS * 8, 128), f32),
            pltpu.VMEM((TOKENS * 8, 256), f32),
            pltpu.VMEM((3, 8, 128), f32),
            pltpu.VMEM((PLANE, 3, 8, 128), f32),
            pltpu.VMEM((3, 8, 128), f32),
            pltpu.VMEM((PLANES, 3, 8, 128), f32),
            pltpu.VMEM((TOKENS, 256), bf16),
            pltpu.VMEM((TP, ROWS, 256), bf16),
            pltpu.VMEM((TP, 256, WIDTH), bf16),
            pltpu.VMEM((2, GROUPS, STATE), f32),
            pltpu.VMEM((ROWS, WIDTH), bf16),
            pltpu.VMEM((2 * ROWS, SLOTS), bf16),
            pltpu.VMEM((SLOTS, ROWS), bf16),
            pltpu.VMEM((EXPERTS, CAPACITY, MIX_WIDTH), bf16),
            pltpu.VMEM((EXPERTS, CAPACITY, MIX_WIDTH), bf16),
            pltpu.VMEM((EXPERTS, CAPACITY, WIDTH), bf16),
            pltpu.VMEM((EXPERTS, CAPACITY, WIDTH), bf16),
            pltpu.VMEM((EXPERTS, CAPACITY, WIDTH), bf16),
            pltpu.VMEM((EXPERTS, CAPACITY, WIDTH), bf16),
            dma((18,)),
            dma((PLANE,)),
            dma((PLANE,)),
            dma((PLANES,)),
            dma((PLANES,)),
            dma((TP,)),
            dma((TP,)),
            dma(()),
            dma((6,)),
            dma((6,)),
            dma((6,)),
            dma((6,)),
            dma((EXPERTS,)),
            dma((EXPERTS,)),
            dma((EXPERTS,)),
            dma((EXPERTS,)),
            dma((EXPERTS,)),
            dma((EXPERTS,)),
        ],
        compiler_params=pltpu.CompilerParams(
            collective_id=0, has_side_effects=True, vmem_limit_bytes=62 * 1024 * 1024
        ),
        name="layer",
    )(log_step, *small, *large)


def solution(mesh):
    in_specs = (
        P("sp", "tp"),
        P("tp", "sp"),
        P("tp", None),
        P("tp", None),
        P("tp"),
        P("tp", None, None),
        P("tp", None, None),
        P("tp", None, None),
        P("tp", None, None),
        P("tp", None),
        P(),
        P("tp", None),
        P(("sp", "tp"), None),
        P(),
        P(("sp", "tp"), None),
        P(("sp", "tp"), None),
        P("sp", None, None),
        P("sp", None, None),
        P("sp", None, None),
        P(),
    )
    out_specs = P(("sp", "tp"), None)
    return jax.shard_map(local, mesh=mesh, in_specs=in_specs, out_specs=out_specs, check_vma=False)
```

```python
import jax
import jax.numpy as jnp
from jax import lax
from jax.experimental import pallas as pl
from jax.experimental.pallas import tpu as pltpu
from jax.sharding import PartitionSpec as P

PICKS = 2
MIX_WIDTH = 1024
MESH = pl.DeviceIdType.MESH

deep_alpha = 2.0**0.25

TOKENS = 256
GROUPS = 16
CHANNELS = 16
STATE = 64
WIDTH = 2048
ROWS = 64
PLANES = 8
PLANE = 8
TP = 4
PIECE = 64
EXPERTS = 64
CAPACITY = 4
SLOTS = EXPERTS * CAPACITY
HIDDEN = 512


def times(ar, ai, br, bi):
    return ar * br - ai * bi, ar * bi + ai * br


def layer_norm(values, scales):
    centered = values - jnp.mean(values, axis=-1, keepdims=True)
    variance = jnp.mean(centered * centered, axis=-1, keepdims=True)
    return centered * lax.rsqrt(variance + 1e-05) * scales


def pair_rows(ref):
    return jnp.concatenate(
        [ref[pl.ds(0, 8, stride=2), :], ref[pl.ds(1, 8, stride=2), :]], axis=1
    )


def remote(src, dst, send_sem, recv_sem, **where):
    return pltpu.make_async_remote_copy(
        src_ref=src,
        dst_ref=dst,
        send_sem=send_sem,
        recv_sem=recv_sem,
        device_id=where,
        device_id_type=MESH,
    )


def layer_kernel(
    step_ref,
    x_hbm,
    ret_hbm,
    real_hbm,
    freq_hbm,
    in_real_hbm,
    in_imag_hbm,
    out_real_hbm,
    out_imag_hbm,
    skip_hbm,
    gain_hbm,
    residual_hbm,
    mix_gain_hbm,
    routes_hbm,
    weight_hbm,
    final_gain_hbm,
    proj_ref,
    gate_hbm,
    up_hbm,
    down_hbm,
    layer_ref,
    x_ref,
    ret_ref,
    real_ref,
    freq_ref,
    in_real_ref,
    in_imag_ref,
    out_real_ref,
    out_imag_ref,
    skip_ref,
    gain_ref,
    residual_ref,
    mix_gain_ref,
    routes_ref,
    weight_ref,
    final_gain_ref,
    gate,
    up,
    down,
    drive_w,
    read_w,
    drive_re,
    drive_im,
    shrink,
    states,
    mine,
    plane_buf,
    plane_sum,
    column_buf,
    mixed,
    whole,
    gathered,
    param_buf,
    hidden_buf,
    combine_hi,
    pick,
    mixed_out,
    mixed_in,
    outgoing,
    arrived,
    produced,
    returned,
    load_sem,
    plane_send,
    plane_recv,
    column_send,
    column_recv,
    tp_send,
    tp_recv,
    own_sem,
    ring_send,
    ring_recv,
    twin_send,
    twin_recv,
    out_send,
    out_recv,
    back_send,
    back_recv,
    mixed_send,
    mixed_recv,
):
    sp = lax.axis_index("sp")
    tp = lax.axis_index("tp")
    plane = lax.div(sp, PLANE)
    place = lax.rem(sp, PLANE)
    core = lax.rem(sp, 2)
    twin = sp + 1 - 2 * core
    right = lax.rem(tp + 1, TP)
    left = lax.rem(tp + TP - 1, TP)
    across = lax.rem(tp + 2, TP)

    own_copy = pltpu.make_async_copy(proj_ref, gathered.at[tp], own_sem)
    loads = [
        pltpu.make_async_copy(source, target, load_sem.at[k])
        for k, (source, target) in enumerate(
            (
                (real_hbm, real_ref),
                (freq_hbm, freq_ref),
                (in_real_hbm, in_real_ref),
                (in_imag_hbm, in_imag_ref),
                (out_real_hbm, out_real_ref),
                (out_imag_hbm, out_imag_ref),
                (ret_hbm, ret_ref),
                (x_hbm, x_ref),
                (skip_hbm, skip_ref),
                (routes_hbm, routes_ref),
                (weight_hbm, weight_ref),
                (gain_hbm, gain_ref),
                (mix_gain_hbm, mix_gain_ref),
                (final_gain_hbm, final_gain_ref),
                (residual_hbm, residual_ref),
                (gate_hbm.at[0], gate),
                (up_hbm.at[0], up),
                (down_hbm.at[0], down),
            )
        )
    ]
    for load in loads[:8]:
        load.start()
    own_copy.start()

    barrier = pltpu.get_barrier_semaphore()

    def greet_plane(k, _):
        peer = plane * PLANE + lax.rem(place + k, PLANE)
        pl.semaphore_signal(barrier, inc=1, device_id={"sp": peer}, device_id_type=MESH)
        return 0

    def greet_column(k, _):
        peer = lax.rem(plane + k, PLANES) * PLANE + place
        pl.semaphore_signal(barrier, inc=1, device_id={"sp": peer}, device_id_type=MESH)
        return 0

    def greet_tp(k, _):
        pl.semaphore_signal(
            barrier, inc=1, device_id={"tp": lax.rem(tp + k, TP)}, device_id_type=MESH
        )
        return 0

    lax.fori_loop(1, TP, greet_tp, 0)
    lax.fori_loop(1, PLANE, greet_plane, 0)
    lax.fori_loop(1, PLANES, greet_column, 0)

    for load in loads[8:]:
        load.start()
    for load in loads[:8]:
        load.wait()

    group_row = lax.broadcasted_iota(jnp.int32, (GROUPS, STATE), 0)
    log_step = jnp.zeros((GROUPS, STATE), jnp.float32)
    for g in range(GROUPS):
        log_step = jnp.where(group_row == g, step_ref[g], log_step)
    stride = jnp.exp(log_step)
    decay_real = real_ref[...]
    decay_freq = freq_ref[...]
    growth = decay_real * stride
    turning = decay_freq * stride
    grown = jnp.exp(growth)
    cosine = jnp.cos(turning)
    sine = jnp.sin(turning)
    half_sine = jnp.sin(0.5 * turning)
    expm1 = jnp.tanh(0.5 * growth) * (grown + 1.0)
    upper_real = expm1 * cosine - 2.0 * half_sine * half_sine
    upper_imag = grown * sine
    denominator = decay_real * decay_real + decay_freq * decay_freq
    factor_real = (upper_real * decay_real + upper_imag * decay_freq) / denominator
    factor_imag = (upper_imag * decay_real - upper_real * decay_freq) / denominator
    param_buf[0] = grown * cosine
    param_buf[1] = grown * sine
    keep_re = pair_rows(param_buf.at[0])
    keep_im = pair_rows(param_buf.at[1])

    nothing = jnp.zeros((CHANNELS, STATE), jnp.float32)
    drive_w[...] = jnp.zeros(drive_w.shape, jnp.bfloat16)
    for g in range(GROUPS):
        rows = pl.ds(g * CHANNELS, CHANNELS)
        b_re = in_real_ref[g]
        b_im = in_imag_ref[g]
        c_re = out_real_ref[g]
        c_im = out_imag_ref[g]
        f_re = factor_real[g : g + 1, :]
        f_im = factor_imag[g : g + 1, :]
        r_re = c_re * f_re - c_im * f_im
        r_im = -(c_re * f_im + c_im * f_re)
        if g % 2 == 0:
            b_row = [b_re, nothing, b_im, nothing]
            r_row = [r_re, nothing, r_im, nothing]
        else:
            b_row = [nothing, b_re, nothing, b_im]
            r_row = [nothing, r_re, nothing, r_im]
        b_row = jnp.concatenate(b_row, axis=1)
        drive_w[g // 2, rows, :] = b_row.astype(jnp.bfloat16)
        read_w[rows, :] = jnp.concatenate(r_row, axis=1).astype(jnp.bfloat16)

    kept = jnp.transpose(jnp.exp(ret_ref[...]))
    kept_hi = kept.astype(jnp.bfloat16)
    rest = kept - kept_hi.astype(jnp.float32)
    kept_mid = rest.astype(jnp.bfloat16)
    kept_lo = (rest - kept_mid.astype(jnp.float32)).astype(jnp.bfloat16)
    select_row = lax.broadcasted_iota(jnp.int32, (GROUPS, 8 * 128), 0)
    select_lane = lax.broadcasted_iota(jnp.int32, (GROUPS, 8 * 128), 1)
    select = (select_row == lax.div(select_lane, STATE)).astype(jnp.bfloat16)
    spread = (
        jnp.dot(kept_hi, select, preferred_element_type=jnp.float32)
        + jnp.dot(kept_mid, select, preferred_element_type=jnp.float32)
        + jnp.dot(kept_lo, select, preferred_element_type=jnp.float32)
    )
    x = x_ref[...]
    for j in range(8):
        at = pl.ds(j, TOKENS, stride=8)
        driven = jnp.dot(x, drive_w[j], preferred_element_type=jnp.float32)
        drive_re[at, :] = driven[:, :128]
        drive_im[at, :] = driven[:, 128:]
        shrink[at, :] = spread[:, j * 128 : (j + 1) * 128]

    pl.semaphore_wait(barrier, (TP - 1) + (PLANE - 1) + (PLANES - 1))

    half = core * (2 * PIECE)
    piece_lo = pl.ds(pl.multiple_of(half, PIECE), PIECE)
    piece_hi = pl.ds(pl.multiple_of(half + PIECE, PIECE), PIECE)

    def ring(block, piece, way, slot):
        to = right if way == 0 else left
        return remote(
            gathered.at[block, piece, :],
            gathered.at[block, piece, :],
            ring_send.at[slot],
            ring_recv.at[slot],
            tp=to,
        )

    own_copy.wait()
    to_right_lo = ring(tp, piece_lo, 0, 0)
    to_left_hi = ring(tp, piece_hi, 1, 1)
    to_right_hi = ring(tp, piece_hi, 0, 2)
    to_left_lo = ring(tp, piece_lo, 1, 3)
    to_right_lo.start()
    to_left_hi.start()
    to_right_hi.start()
    to_left_lo.start()

    def advance(t, carried):
        s_re, s_im, decay = carried
        row = pl.ds(pl.multiple_of(t * 8, 8), 8)
        shr = shrink[row, :]
        a_re = shr * keep_re
        a_im = shr * keep_im
        n_re = (a_re * s_re - a_im * s_im) + drive_re[row, :]
        n_im = (a_re * s_im + a_im * s_re) + drive_im[row, :]
        return n_re, n_im, decay * shr

    zero = jnp.zeros((8, 128), jnp.float32)
    one = jnp.ones((8, 128), jnp.float32)
    end_re, end_im, decay = lax.fori_loop(0, TOKENS, advance, (zero, zero, one), unroll=8)
    mine[0] = end_re
    mine[1] = end_im
    mine[2] = decay

    power_re, power_im = keep_re, keep_im
    for _ in range(8):
        power_re, power_im = times(power_re, power_im, power_re, power_im)
    plane_re, plane_im = power_re, power_im
    for _ in range(3):
        plane_re, plane_im = times(plane_re, plane_im, plane_re, plane_im)

    def plane_copy(k):
        peer = plane * PLANE + lax.rem(place + k, PLANE)
        return remote(mine, plane_buf.at[place], plane_send.at[k], plane_recv.at[place], sp=peer)

    def send_plane(k, _):
        plane_copy(k).start()
        return 0

    def plane_arrived(k, _):
        source = lax.rem(place + k, PLANE)
        remote(
            mine, plane_buf.at[source], plane_send.at[k], plane_recv.at[source], sp=plane * PLANE + source
        ).wait_recv()
        return 0

    lax.fori_loop(1, PLANE, send_plane, 0)

    for load in loads[8:15]:
        load.wait()
    slot = lax.broadcasted_iota(jnp.int32, (SLOTS, ROWS), 0)
    slot_plane = lax.rem(plane + lax.shift_right_logical(slot, 5), PLANES)
    slot_place = lax.rem(place + lax.rem(lax.shift_right_logical(slot, 2), PLANE), PLANE)
    slot_expert = slot_plane * PLANE + slot_place
    first = jnp.where(routes_ref[0:1, :] == slot_expert, 1.0, 0.0)
    second = jnp.where(routes_ref[1:2, :] == slot_expert, 1.0, 0.0)
    named = first + second
    row_before = lax.broadcasted_iota(jnp.int32, (ROWS, ROWS), 0)
    row_at = lax.broadcasted_iota(jnp.int32, (ROWS, ROWS), 1)
    earlier = jnp.where(row_before < row_at, 1.0, 0.0).astype(jnp.bfloat16)
    rank = jnp.dot(named.astype(jnp.bfloat16), earlier, preferred_element_type=jnp.float32)
    here = jnp.where(rank == lax.rem(slot, CAPACITY).astype(jnp.float32), 1.0, 0.0)
    weights = jnp.transpose(here * (weight_ref[0:1, :] * first + weight_ref[1:2, :] * second))
    weights_hi = weights.astype(jnp.bfloat16)
    combine_hi[:ROWS, :] = weights_hi
    combine_hi[ROWS:, :] = (weights - weights_hi.astype(jnp.float32)).astype(jnp.bfloat16)
    pick[...] = (here * named).astype(jnp.bfloat16)

    def expert_of(k):
        return lax.rem(plane + lax.div(k, PLANE), PLANES) * PLANE + lax.rem(place + k, PLANE)

    def source_of(k):
        return lax.rem(plane + PLANES - lax.div(k, PLANE), PLANES) * PLANE + lax.rem(
            place + PLANE - lax.rem(k, PLANE), PLANE
        )

    def out_copy(k):
        return remote(outgoing.at[k], arrived.at[k], out_send.at[k], out_recv.at[k], sp=expert_of(k))

    def mixed_copy(k):
        return remote(
            mixed_out.at[k], mixed_in.at[k], mixed_send.at[k], mixed_recv.at[k], sp=expert_of(k)
        )

    def back_copy(k):
        return remote(produced.at[k], returned.at[k], back_send.at[k], back_recv.at[k], sp=source_of(k))

    def send_out(k, _):
        out_copy(k).start()
        return 0

    def send_mixed(k, _):
        mixed_copy(k).start()
        return 0

    def blocks(p, rows):
        picked = jnp.dot(pick[p * 32 : (p + 1) * 32, :], rows, preferred_element_type=jnp.float32)
        return picked.astype(jnp.bfloat16).reshape(PLANE, CAPACITY, rows.shape[1])

    for p in (2, 6, 3, 5):
        outgoing[p * PLANE : (p + 1) * PLANE] = blocks(p, residual_ref[...])

    lax.fori_loop(1, PLANE, plane_arrived, 0)
    plane_buf[place] = mine[...]

    def join(buf, k, carried, p_re, p_im):
        s_re, s_im, decay = carried
        d = buf[k, 2]
        m_re, m_im = times(d * p_re, d * p_im, s_re, s_im)
        return m_re + buf[k, 0], m_im + buf[k, 1], decay * d

    def join_place(k, carried):
        return join(plane_buf, k, carried, power_re, power_im)

    total = lax.fori_loop(0, PLANE, join_place, (zero, zero, one))
    plane_sum[0] = total[0]
    plane_sum[1] = total[1]
    plane_sum[2] = total[2]

    def column_copy(p):
        return remote(
            plane_sum, column_buf.at[plane], column_send.at[p], column_recv.at[plane], sp=p * PLANE + place
        )

    def send_column(p, _):
        column_copy(p).start()
        return 0

    def column_arrived(p, _):
        remote(
            plane_sum, column_buf.at[p], column_send.at[p], column_recv.at[p], sp=p * PLANE + place
        ).wait_recv()
        return 0

    lax.fori_loop(plane + 1, PLANES, send_column, 0)

    for p in (2, 6):
        lax.fori_loop(p * PLANE, (p + 1) * PLANE, send_out, 0)

    lax.fori_loop(0, plane, column_arrived, 0)

    for p in (3, 5):
        lax.fori_loop(p * PLANE, (p + 1) * PLANE, send_out, 0)

    def join_plane(p, carried):
        return join(column_buf, p, carried, plane_re, plane_im)

    carried = lax.fori_loop(0, plane, join_plane, (zero, zero, one))
    carried = lax.fori_loop(0, place, join_place, carried)

    def record(t, carried):
        s_re, s_im = carried
        row = pl.ds(pl.multiple_of(t * 8, 8), 8)
        shr = shrink[row, :]
        a_re = shr * keep_re
        a_im = shr * keep_im
        n_re = (a_re * s_re - a_im * s_im) + drive_re[row, :]
        n_im = (a_re * s_im + a_im * s_re) + drive_im[row, :]
        states[row, :128] = n_re
        states[row, 128:] = n_im
        return n_re, n_im

    lax.fori_loop(0, TOKENS, record, (carried[0], carried[1]), unroll=8)

    def read(k, _):
        at = pl.ds(pl.multiple_of(k * 1024, 1024), 1024)
        product = lax.dot_general(
            states[at, :].astype(jnp.bfloat16),
            read_w[...],
            (((1,), (1,)), ((), ())),
            preferred_element_type=jnp.float32,
        )
        drive_re[at, :] = product[:, :128]
        drive_im[at, :] = product[:, 128:]
        return 0

    lax.fori_loop(0, 2, read, 0)
    lane = lax.broadcasted_iota(jnp.int32, (TOKENS, 128), 1)
    for side, buf in ((0, drive_re), (1, drive_im)):
        picked = jnp.zeros((TOKENS, 128), jnp.float32)
        for j in range(4):
            value = buf[pl.ds(side * 4 + j, TOKENS, stride=8), :]
            picked = jnp.where(lax.div(lane, 32) == j, value, picked)
        skip = jnp.concatenate([skip_ref[g : g + 1, :] for g in range(side * 8, side * 8 + 8)], axis=1)
        lanes = slice(side * 128, side * 128 + 128)
        read_out = picked + skip * x_ref[:, lanes].astype(jnp.float32)
        mixed[:, lanes] = jax.nn.gelu(read_out).astype(jnp.bfloat16)

    def tp_copy(k):
        peer = lax.rem(tp + k, TP)
        rows = pl.ds(pl.multiple_of(peer * ROWS, ROWS), ROWS)
        return remote(mixed.at[rows, :], whole.at[tp], tp_send.at[k], tp_recv.at[tp], tp=peer)

    def send_tp(k, _):
        tp_copy(k).start()
        return 0

    def tp_arrived(k, _):
        source = lax.rem(tp + k, TP)
        rows = pl.ds(pl.multiple_of(tp * ROWS, ROWS), ROWS)
        remote(mixed.at[rows, :], whole.at[source], tp_send.at[k], tp_recv.at[source], tp=source).wait_recv()
        return 0

    lax.fori_loop(1, TP, send_tp, 0)
    whole[tp] = mixed[pl.ds(pl.multiple_of(tp * ROWS, ROWS), ROWS), :]

    def twin_copy(block, piece, slot):
        return remote(
            gathered.at[block, piece, :],
            gathered.at[block, piece, :],
            twin_send.at[slot],
            twin_recv.at[slot],
            sp=twin,
        )

    from_left_lo = ring(left, piece_lo, 0, 0)
    from_right_hi = ring(right, piece_hi, 1, 1)
    from_left_hi = ring(left, piece_hi, 0, 2)
    from_right_lo = ring(right, piece_lo, 1, 3)
    from_left_lo.wait_recv()
    pass_right = ring(left, piece_lo, 0, 4)
    pass_right.start()
    from_right_hi.wait_recv()
    pass_left = ring(right, piece_hi, 1, 5)
    pass_left.start()
    twin_left_lo = twin_copy(left, piece_lo, 0)
    twin_right_hi = twin_copy(right, piece_hi, 1)
    twin_left_lo.start()
    twin_right_hi.start()
    from_left_hi.wait_recv()
    from_right_lo.wait_recv()
    twin_left_hi = twin_copy(left, piece_hi, 2)
    twin_right_lo = twin_copy(right, piece_lo, 3)
    twin_left_hi.start()
    twin_right_lo.start()

    lax.fori_loop(1, TP, tp_arrived, 0)

    for p in (3, 5, 2, 6):
        for piece in range(TP):
            lanes = slice(piece * 256, (piece + 1) * 256)
            mixed_out[p * PLANE : (p + 1) * PLANE, :, lanes] = blocks(p, whole[piece])
        lax.fori_loop(p * PLANE, (p + 1) * PLANE, send_mixed, 0)

    def hidden_of(pieces, residual_rows):
        squares = jnp.zeros((ROWS, 1), jnp.float32)
        mix = jnp.zeros((ROWS, WIDTH), jnp.float32)
        for q in range(TP):
            rows = pieces[q].astype(jnp.float32)
            squares += jnp.sum(rows * rows, axis=1, keepdims=True)
            scaled = (rows * gain_ref[:, q * 256 : (q + 1) * 256]).astype(jnp.bfloat16)
            mix += jnp.dot(scaled, gathered[q], preferred_element_type=jnp.float32)
        inverse = lax.rsqrt(squares / MIX_WIDTH + 1e-06)
        mix = deep_alpha * residual_rows.astype(jnp.float32) + mix * inverse
        return layer_norm(mix, mix_gain_ref[...]).astype(jnp.bfloat16)

    across_lo = ring(across, piece_lo, 0, 4)
    across_hi = ring(across, piece_hi, 1, 5)
    across_lo.wait_recv()
    twin_across_lo = twin_copy(across, piece_lo, 4)
    twin_across_lo.start()
    across_hi.wait_recv()
    twin_across_hi = twin_copy(across, piece_hi, 5)
    twin_across_hi.start()

    other = 2 * PIECE - half
    other_lo = pl.ds(pl.multiple_of(other, PIECE), PIECE)
    other_hi = pl.ds(pl.multiple_of(other + PIECE, PIECE), PIECE)
    for slot, (block, piece) in enumerate(
        (
            (left, other_lo),
            (right, other_hi),
            (left, other_hi),
            (right, other_lo),
            (across, other_lo),
            (across, other_hi),
        )
    ):
        twin_copy(block, piece, slot).wait_recv()
    hidden_buf[...] = hidden_of([whole[q] for q in range(TP)], residual_ref[...])

    for p in (4, 1, 7, 0):
        outgoing[p * PLANE : (p + 1) * PLANE] = blocks(p, hidden_buf[...])
        lax.fori_loop(p * PLANE + (p == 0), (p + 1) * PLANE, send_out, 0)
    arrived[0] = outgoing[0]

    for load in loads[15:]:
        load.wait()

    def rows_of(buf, far, near):
        size = PLANE * CAPACITY
        return jnp.concatenate(
            [buf[pl.ds(far, PLANE)].reshape(size, -1), buf[pl.ds(near, PLANE)].reshape(size, -1)], axis=0
        )

    def expert(far, near, is_far):
        near_first = jnp.maximum(near, 1)

        def out_arrived(k, _):
            out_copy(k).wait_recv()
            return 0

        def mixed_arrived(k, _):
            mixed_copy(k).wait_recv()
            return 0

        def send_back(k, _):
            back_copy(k).start()
            return 0

        lax.fori_loop(far, far + PLANE, out_arrived, 0)
        lax.fori_loop(near_first, near + PLANE, out_arrived, 0)
        rows = rows_of(arrived, far, near)
        if is_far:
            lax.fori_loop(far, far + PLANE, mixed_arrived, 0)
            lax.fori_loop(near, near + PLANE, mixed_arrived, 0)
            mixed_rows = rows_of(mixed_in, far, near)
            rows = hidden_of([mixed_rows[:, q * 256 : (q + 1) * 256] for q in range(TP)], rows)
        gate_act = jnp.dot(rows, gate[...], preferred_element_type=jnp.float32)
        up_act = jnp.dot(rows, up[...], preferred_element_type=jnp.float32)
        active = (jax.nn.silu(gate_act) * up_act).astype(jnp.bfloat16)
        result = jnp.dot(active, down[...], preferred_element_type=jnp.float32).astype(jnp.bfloat16)
        produced[pl.ds(far, PLANE)] = result[: PLANE * CAPACITY].reshape(PLANE, CAPACITY, WIDTH)
        produced[pl.ds(near, PLANE)] = result[PLANE * CAPACITY :].reshape(PLANE, CAPACITY, WIDTH)
        lax.fori_loop(far, far + PLANE, send_back, 0)
        lax.fori_loop(near_first, near + PLANE, send_back, 0)

    def far_expert(c, _):
        expert((5 + c) * PLANE, (3 - c) * PLANE, True)
        return 0

    def near_expert(c, _):
        expert((4 + 3 * c) * PLANE, c * PLANE, False)
        return 0

    lax.fori_loop(0, 2, far_expert, 0)
    lax.fori_loop(0, 2, near_expert, 0)
    returned[0] = produced[0]

    def out_left(k, _):
        out_copy(k).wait_send()
        back_copy(k).wait_send()
        return 0

    def mixed_left(k, _):
        mixed_copy(k).wait_send()
        return 0

    lax.fori_loop(1, EXPERTS, out_left, 0)
    for p in (2, 3, 5, 6):
        lax.fori_loop(p * PLANE, (p + 1) * PLANE, mixed_left, 0)

    def plane_left(k, _):
        plane_copy(k).wait_send()
        return 0

    def column_left(p, _):
        column_copy(p).wait_send()
        return 0

    def tp_left(k, _):
        tp_copy(k).wait_send()
        return 0

    lax.fori_loop(1, PLANE, plane_left, 0)
    lax.fori_loop(plane + 1, PLANES, column_left, 0)
    lax.fori_loop(1, TP, tp_left, 0)
    for copy in (to_right_lo, to_left_hi, to_right_hi, to_left_lo, pass_right, pass_left):
        copy.wait_send()
    for copy in (twin_left_lo, twin_right_hi, twin_left_hi, twin_right_lo, twin_across_lo, twin_across_hi):
        copy.wait_send()

    def back_arrived(k, _):
        back_copy(k).wait_recv()
        return 0

    lax.fori_loop(1, EXPERTS, back_arrived, 0)
    both = jnp.dot(
        combine_hi[...], returned[...].reshape(SLOTS, WIDTH), preferred_element_type=jnp.float32
    )
    expert_mix = both[:ROWS] + both[ROWS:]
    final = layer_norm(deep_alpha * hidden_buf[...].astype(jnp.float32) + expert_mix, final_gain_ref[...])
    layer_ref[...] = final.astype(jnp.bfloat16)


def local(
    mixer_input,
    retention,
    decay_real,
    decay_freq,
    log_step,
    input_real,
    input_imag,
    readout_real,
    readout_imaginary,
    skip_weight,
    norm_gain,
    projection,
    residual,
    mix_gain,
    routes,
    route_weight,
    expert_gate,
    expert_up,
    expert_down,
    final_gain,
):
    hbm = pl.BlockSpec(memory_space=pltpu.HBM)
    smem = pl.BlockSpec(memory_space=pltpu.SMEM)
    vmem = pl.BlockSpec(memory_space=pltpu.VMEM)
    f32 = jnp.float32
    bf16 = jnp.bfloat16
    dma = pltpu.SemaphoreType.DMA
    small = (
        mixer_input,
        retention,
        decay_real,
        decay_freq,
        jnp.transpose(input_real, (0, 2, 1)),
        jnp.transpose(input_imag, (0, 2, 1)),
        readout_real,
        readout_imaginary,
        skip_weight,
        norm_gain.reshape(1, -1),
        residual,
        mix_gain.reshape(1, -1),
        jnp.transpose(routes),
        jnp.transpose(route_weight),
        final_gain.reshape(1, -1),
    )
    large = (projection, expert_gate, expert_up, expert_down)
    return pl.pallas_call(
        layer_kernel,
        out_shape=pltpu.VMEM((ROWS, WIDTH), bf16),
        in_specs=[smem] + [hbm] * (len(small) + len(large)),
        out_specs=vmem,
        scratch_shapes=[pltpu.VMEM(a.shape, a.dtype) for a in small]
        + [
            pltpu.VMEM((WIDTH, HIDDEN), bf16),
            pltpu.VMEM((WIDTH, HIDDEN), bf16),
            pltpu.VMEM((HIDDEN, WIDTH), bf16),
            pltpu.VMEM((8, 256, 256), bf16),
            pltpu.VMEM((256, 256), bf16),
            pltpu.VMEM((TOKENS * 8, 128), f32),
            pltpu.VMEM((TOKENS * 8, 128), f32),
            pltpu.VMEM((TOKENS * 8, 128), f32),
            pltpu.VMEM((TOKENS * 8, 256), f32),
            pltpu.VMEM((3, 8, 128), f32),
            pltpu.VMEM((PLANE, 3, 8, 128), f32),
            pltpu.VMEM((3, 8, 128), f32),
            pltpu.VMEM((PLANES, 3, 8, 128), f32),
            pltpu.VMEM((TOKENS, 256), bf16),
            pltpu.VMEM((TP, ROWS, 256), bf16),
            pltpu.VMEM((TP, 256, WIDTH), bf16),
            pltpu.VMEM((2, GROUPS, STATE), f32),
            pltpu.VMEM((ROWS, WIDTH), bf16),
            pltpu.VMEM((2 * ROWS, SLOTS), bf16),
            pltpu.VMEM((SLOTS, ROWS), bf16),
            pltpu.VMEM((EXPERTS, CAPACITY, MIX_WIDTH), bf16),
            pltpu.VMEM((EXPERTS, CAPACITY, MIX_WIDTH), bf16),
            pltpu.VMEM((EXPERTS, CAPACITY, WIDTH), bf16),
            pltpu.VMEM((EXPERTS, CAPACITY, WIDTH), bf16),
            pltpu.VMEM((EXPERTS, CAPACITY, WIDTH), bf16),
            pltpu.VMEM((EXPERTS, CAPACITY, WIDTH), bf16),
            dma((18,)),
            dma((PLANE,)),
            dma((PLANE,)),
            dma((PLANES,)),
            dma((PLANES,)),
            dma((TP,)),
            dma((TP,)),
            dma(()),
            dma((6,)),
            dma((6,)),
            dma((6,)),
            dma((6,)),
            dma((EXPERTS,)),
            dma((EXPERTS,)),
            dma((EXPERTS,)),
            dma((EXPERTS,)),
            dma((EXPERTS,)),
            dma((EXPERTS,)),
        ],
        compiler_params=pltpu.CompilerParams(
            collective_id=0, has_side_effects=True, vmem_limit_bytes=62 * 1024 * 1024
        ),
        name="layer",
    )(log_step, *small, *large)


def solution(mesh):
    in_specs = (
        P("sp", "tp"),
        P("tp", "sp"),
        P("tp", None),
        P("tp", None),
        P("tp"),
        P("tp", None, None),
        P("tp", None, None),
        P("tp", None, None),
        P("tp", None, None),
        P("tp", None),
        P(),
        P("tp", None),
        P(("sp", "tp"), None),
        P(),
        P(("sp", "tp"), None),
        P(("sp", "tp"), None),
        P("sp", None, None),
        P("sp", None, None),
        P("sp", None, None),
        P(),
    )
    out_specs = P(("sp", "tp"), None)
    return jax.shard_map(local, mesh=mesh, in_specs=in_specs, out_specs=out_specs, check_vma=False)
```

```python
import jax
import jax.numpy as jnp
from jax import lax
from jax.experimental import pallas as pl
from jax.experimental.pallas import tpu as pltpu
from jax.sharding import PartitionSpec as P

PICKS = 2
MIX_WIDTH = 1024
MESH = pl.DeviceIdType.MESH

deep_alpha = 2.0**0.25

TOKENS = 256
HALF = TOKENS // 2
GROUPS = 16
CHANNELS = 16
STATE = 64
WIDTH = 2048
ROWS = 64
PLANES = 8
PLANE = 8
TP = 4
PIECE = 64
EXPERTS = 64
CAPACITY = 4
SLOTS = EXPERTS * CAPACITY
HIDDEN = 512


def times(ar, ai, br, bi):
    return ar * br - ai * bi, ar * bi + ai * br


def layer_norm(values, scales):
    centered = values - jnp.mean(values, axis=-1, keepdims=True)
    variance = jnp.mean(centered * centered, axis=-1, keepdims=True)
    return centered * lax.rsqrt(variance + 1e-05) * scales


def pair_rows(ref):
    return jnp.concatenate(
        [ref[pl.ds(0, 8, stride=2), :], ref[pl.ds(1, 8, stride=2), :]], axis=1
    )


def remote(src, dst, send_sem, recv_sem, **where):
    return pltpu.make_async_remote_copy(
        src_ref=src,
        dst_ref=dst,
        send_sem=send_sem,
        recv_sem=recv_sem,
        device_id=where,
        device_id_type=MESH,
    )


def layer_kernel(
    step_ref,
    x_hbm,
    ret_hbm,
    real_hbm,
    freq_hbm,
    in_real_hbm,
    in_imag_hbm,
    out_real_hbm,
    out_imag_hbm,
    skip_hbm,
    gain_hbm,
    residual_hbm,
    mix_gain_hbm,
    routes_hbm,
    weight_hbm,
    final_gain_hbm,
    proj_ref,
    gate_hbm,
    up_hbm,
    down_hbm,
    layer_ref,
    x_ref,
    ret_ref,
    real_ref,
    freq_ref,
    in_real_ref,
    in_imag_ref,
    out_real_ref,
    out_imag_ref,
    skip_ref,
    gain_ref,
    residual_ref,
    mix_gain_ref,
    routes_ref,
    weight_ref,
    final_gain_ref,
    gate,
    up,
    down,
    drive_w,
    read_w,
    drive_re,
    drive_im,
    shrink,
    states,
    mine,
    plane_buf,
    plane_sum,
    column_buf,
    mixed,
    whole,
    gathered,
    param_buf,
    hidden_buf,
    combine_hi,
    pick,
    mixed_out,
    mixed_in,
    outgoing,
    arrived,
    produced,
    returned,
    load_sem,
    plane_send,
    plane_recv,
    column_send,
    column_recv,
    tp_send,
    tp_recv,
    own_sem,
    ring_send,
    ring_recv,
    twin_send,
    twin_recv,
    out_send,
    out_recv,
    back_send,
    back_recv,
    mixed_send,
    mixed_recv,
):
    sp = lax.axis_index("sp")
    tp = lax.axis_index("tp")
    plane = lax.div(sp, PLANE)
    place = lax.rem(sp, PLANE)
    core = lax.rem(sp, 2)
    twin = sp + 1 - 2 * core
    right = lax.rem(tp + 1, TP)
    left = lax.rem(tp + TP - 1, TP)
    across = lax.rem(tp + 2, TP)

    own_copy = pltpu.make_async_copy(proj_ref, gathered.at[tp], own_sem)
    loads = [
        pltpu.make_async_copy(source, target, load_sem.at[k])
        for k, (source, target) in enumerate(
            (
                (real_hbm, real_ref),
                (freq_hbm, freq_ref),
                (in_real_hbm, in_real_ref),
                (in_imag_hbm, in_imag_ref),
                (out_real_hbm, out_real_ref),
                (out_imag_hbm, out_imag_ref),
                (ret_hbm, ret_ref),
                (x_hbm, x_ref),
                (skip_hbm, skip_ref),
                (routes_hbm, routes_ref),
                (weight_hbm, weight_ref),
                (gain_hbm, gain_ref),
                (mix_gain_hbm, mix_gain_ref),
                (final_gain_hbm, final_gain_ref),
                (residual_hbm, residual_ref),
                (gate_hbm.at[0], gate),
                (up_hbm.at[0], up),
                (down_hbm.at[0], down),
            )
        )
    ]
    for load in loads[:8]:
        load.start()
    own_copy.start()

    barrier = pltpu.get_barrier_semaphore()

    def greet_plane(k, _):
        peer = plane * PLANE + lax.rem(place + k, PLANE)
        pl.semaphore_signal(barrier, inc=1, device_id={"sp": peer}, device_id_type=MESH)
        return 0

    def greet_column(k, _):
        peer = lax.rem(plane + k, PLANES) * PLANE + place
        pl.semaphore_signal(barrier, inc=1, device_id={"sp": peer}, device_id_type=MESH)
        return 0

    def greet_tp(k, _):
        pl.semaphore_signal(
            barrier, inc=1, device_id={"tp": lax.rem(tp + k, TP)}, device_id_type=MESH
        )
        return 0

    lax.fori_loop(1, TP, greet_tp, 0)
    lax.fori_loop(1, PLANE, greet_plane, 0)
    lax.fori_loop(1, PLANES, greet_column, 0)

    for load in loads[8:]:
        load.start()
    for load in loads[:8]:
        load.wait()

    group_row = lax.broadcasted_iota(jnp.int32, (GROUPS, STATE), 0)
    log_step = jnp.zeros((GROUPS, STATE), jnp.float32)
    for g in range(GROUPS):
        log_step = jnp.where(group_row == g, step_ref[g], log_step)
    stride = jnp.exp(log_step)
    decay_real = real_ref[...]
    decay_freq = freq_ref[...]
    growth = decay_real * stride
    turning = decay_freq * stride
    grown = jnp.exp(growth)
    cosine = jnp.cos(turning)
    sine = jnp.sin(turning)
    half_sine = jnp.sin(0.5 * turning)
    expm1 = jnp.tanh(0.5 * growth) * (grown + 1.0)
    upper_real = expm1 * cosine - 2.0 * half_sine * half_sine
    upper_imag = grown * sine
    denominator = decay_real * decay_real + decay_freq * decay_freq
    factor_real = (upper_real * decay_real + upper_imag * decay_freq) / denominator
    factor_imag = (upper_imag * decay_real - upper_real * decay_freq) / denominator
    param_buf[0] = grown * cosine
    param_buf[1] = grown * sine
    keep_re = pair_rows(param_buf.at[0])
    keep_im = pair_rows(param_buf.at[1])

    nothing = jnp.zeros((CHANNELS, STATE), jnp.float32)
    drive_w[...] = jnp.zeros(drive_w.shape, jnp.bfloat16)
    for g in range(GROUPS):
        rows = pl.ds(g * CHANNELS, CHANNELS)
        b_re = in_real_ref[g]
        b_im = in_imag_ref[g]
        c_re = out_real_ref[g]
        c_im = out_imag_ref[g]
        f_re = factor_real[g : g + 1, :]
        f_im = factor_imag[g : g + 1, :]
        r_re = c_re * f_re - c_im * f_im
        r_im = -(c_re * f_im + c_im * f_re)
        if g % 2 == 0:
            b_row = [b_re, nothing, b_im, nothing]
            r_row = [r_re, nothing, r_im, nothing]
        else:
            b_row = [nothing, b_re, nothing, b_im]
            r_row = [nothing, r_re, nothing, r_im]
        b_row = jnp.concatenate(b_row, axis=1)
        drive_w[g // 2, rows, :] = b_row.astype(jnp.bfloat16)
        read_w[rows, :] = jnp.concatenate(r_row, axis=1).astype(jnp.bfloat16)

    kept = jnp.transpose(jnp.exp(ret_ref[...]))
    kept_hi = kept.astype(jnp.bfloat16)
    rest = kept - kept_hi.astype(jnp.float32)
    kept_mid = rest.astype(jnp.bfloat16)
    kept_lo = (rest - kept_mid.astype(jnp.float32)).astype(jnp.bfloat16)
    select_row = lax.broadcasted_iota(jnp.int32, (3 * GROUPS, 8 * 128), 0)
    select_lane = lax.broadcasted_iota(jnp.int32, (3 * GROUPS, 8 * 128), 1)
    select = (lax.rem(select_row, GROUPS) == lax.div(select_lane, STATE)).astype(jnp.bfloat16)
    spread = jnp.dot(
        jnp.concatenate([kept_hi, kept_mid, kept_lo], axis=1), select, preferred_element_type=jnp.float32
    )
    x = x_ref[...]
    for j in range(8):
        at = pl.ds(j, TOKENS, stride=8)
        driven = jnp.dot(x, drive_w[j], preferred_element_type=jnp.float32)
        drive_re[at, :] = driven[:, :128]
        drive_im[at, :] = driven[:, 128:]
        shrink[at, :] = spread[:, j * 128 : (j + 1) * 128]

    pl.semaphore_wait(barrier, (TP - 1) + (PLANE - 1) + (PLANES - 1))

    half = core * (2 * PIECE)
    piece_lo = pl.ds(pl.multiple_of(half, PIECE), PIECE)
    piece_hi = pl.ds(pl.multiple_of(half + PIECE, PIECE), PIECE)

    def ring(block, piece, way, slot):
        to = right if way == 0 else left
        return remote(
            gathered.at[block, piece, :],
            gathered.at[block, piece, :],
            ring_send.at[slot],
            ring_recv.at[slot],
            tp=to,
        )

    own_copy.wait()
    to_right_lo = ring(tp, piece_lo, 0, 0)
    to_left_hi = ring(tp, piece_hi, 1, 1)
    to_right_hi = ring(tp, piece_hi, 0, 2)
    to_left_lo = ring(tp, piece_lo, 1, 3)
    to_right_lo.start()
    to_left_hi.start()
    to_right_hi.start()
    to_left_lo.start()

    def step(t, s_re, s_im):
        row = pl.ds(pl.multiple_of(t * 8, 8), 8)
        shr = shrink[row, :]
        a_re = shr * keep_re
        a_im = shr * keep_im
        n_re = (a_re * s_re - a_im * s_im) + drive_re[row, :]
        n_im = (a_re * s_im + a_im * s_re) + drive_im[row, :]
        return n_re, n_im, shr, row

    def advance(t, carried):
        f_re, f_im, f_decay, s_re, s_im, s_decay = carried
        f_re, f_im, f_shr, _ = step(t, f_re, f_im)
        s_re, s_im, s_shr, _ = step(t + HALF, s_re, s_im)
        return f_re, f_im, f_decay * f_shr, s_re, s_im, s_decay * s_shr

    half_re, half_im = keep_re, keep_im
    for _ in range(7):
        half_re, half_im = times(half_re, half_im, half_re, half_im)
    power_re, power_im = times(half_re, half_im, half_re, half_im)

    zero = jnp.zeros((8, 128), jnp.float32)
    one = jnp.ones((8, 128), jnp.float32)
    first_re, first_im, first_decay, last_re, last_im, last_decay = lax.fori_loop(
        0, HALF, advance, (zero, zero, one, zero, zero, one), unroll=8
    )
    end_re, end_im = times(last_decay * half_re, last_decay * half_im, first_re, first_im)
    mine[0] = end_re + last_re
    mine[1] = end_im + last_im
    mine[2] = first_decay * last_decay

    plane_re, plane_im = power_re, power_im
    for _ in range(3):
        plane_re, plane_im = times(plane_re, plane_im, plane_re, plane_im)

    def plane_copy(k):
        peer = plane * PLANE + lax.rem(place + k, PLANE)
        return remote(mine, plane_buf.at[place], plane_send.at[k], plane_recv.at[place], sp=peer)

    def send_plane(k, _):
        plane_copy(k).start()
        return 0

    def plane_arrived(k, _):
        source = lax.rem(place + k, PLANE)
        remote(
            mine, plane_buf.at[source], plane_send.at[k], plane_recv.at[source], sp=plane * PLANE + source
        ).wait_recv()
        return 0

    lax.fori_loop(1, PLANE, send_plane, 0)

    for load in loads[8:15]:
        load.wait()
    slot = lax.broadcasted_iota(jnp.int32, (SLOTS, ROWS), 0)
    slot_plane = lax.rem(plane + lax.shift_right_logical(slot, 5), PLANES)
    slot_place = lax.rem(place + lax.rem(lax.shift_right_logical(slot, 2), PLANE), PLANE)
    slot_expert = slot_plane * PLANE + slot_place
    first = jnp.where(routes_ref[0:1, :] == slot_expert, 1.0, 0.0)
    second = jnp.where(routes_ref[1:2, :] == slot_expert, 1.0, 0.0)
    named = first + second
    row_before = lax.broadcasted_iota(jnp.int32, (ROWS, ROWS), 0)
    row_at = lax.broadcasted_iota(jnp.int32, (ROWS, ROWS), 1)
    earlier = jnp.where(row_before < row_at, 1.0, 0.0).astype(jnp.bfloat16)
    rank = jnp.dot(named.astype(jnp.bfloat16), earlier, preferred_element_type=jnp.float32)
    here = jnp.where(rank == lax.rem(slot, CAPACITY).astype(jnp.float32), 1.0, 0.0)
    weights = jnp.transpose(here * (weight_ref[0:1, :] * first + weight_ref[1:2, :] * second))
    weights_hi = weights.astype(jnp.bfloat16)
    combine_hi[:ROWS, :] = weights_hi
    combine_hi[ROWS:, :] = (weights - weights_hi.astype(jnp.float32)).astype(jnp.bfloat16)
    pick[...] = (here * named).astype(jnp.bfloat16)

    def expert_of(k):
        return lax.rem(plane + lax.div(k, PLANE), PLANES) * PLANE + lax.rem(place + k, PLANE)

    def source_of(k):
        return lax.rem(plane + PLANES - lax.div(k, PLANE), PLANES) * PLANE + lax.rem(
            place + PLANE - lax.rem(k, PLANE), PLANE
        )

    def out_copy(k):
        return remote(outgoing.at[k], arrived.at[k], out_send.at[k], out_recv.at[k], sp=expert_of(k))

    def mixed_copy(k):
        return remote(
            mixed_out.at[k], mixed_in.at[k], mixed_send.at[k], mixed_recv.at[k], sp=expert_of(k)
        )

    def back_copy(k):
        return remote(produced.at[k], returned.at[k], back_send.at[k], back_recv.at[k], sp=source_of(k))

    def send_out(k, _):
        out_copy(k).start()
        return 0

    def send_mixed(k, _):
        mixed_copy(k).start()
        return 0

    def blocks(p, rows):
        picked = jnp.dot(pick[p * 32 : (p + 1) * 32, :], rows, preferred_element_type=jnp.float32)
        return picked.astype(jnp.bfloat16).reshape(PLANE, CAPACITY, rows.shape[1])

    for p in (2, 6, 3, 5):
        outgoing[p * PLANE : (p + 1) * PLANE] = blocks(p, residual_ref[...])

    lax.fori_loop(1, PLANE, plane_arrived, 0)
    plane_buf[place] = mine[...]

    def join(buf, k, carried, p_re, p_im):
        s_re, s_im, decay = carried
        d = buf[k, 2]
        m_re, m_im = times(d * p_re, d * p_im, s_re, s_im)
        return m_re + buf[k, 0], m_im + buf[k, 1], decay * d

    def join_place(k, carried):
        return join(plane_buf, k, carried, power_re, power_im)

    total = lax.fori_loop(0, PLANE, join_place, (zero, zero, one))
    plane_sum[0] = total[0]
    plane_sum[1] = total[1]
    plane_sum[2] = total[2]

    def column_copy(p):
        return remote(
            plane_sum, column_buf.at[plane], column_send.at[p], column_recv.at[plane], sp=p * PLANE + place
        )

    def send_column(p, _):
        column_copy(p).start()
        return 0

    def column_arrived(p, _):
        remote(
            plane_sum, column_buf.at[p], column_send.at[p], column_recv.at[p], sp=p * PLANE + place
        ).wait_recv()
        return 0

    lax.fori_loop(plane + 1, PLANES, send_column, 0)

    for p in (2, 6):
        lax.fori_loop(p * PLANE, (p + 1) * PLANE, send_out, 0)

    lax.fori_loop(0, plane, column_arrived, 0)

    for p in (3, 5):
        lax.fori_loop(p * PLANE, (p + 1) * PLANE, send_out, 0)

    def join_plane(p, carried):
        return join(column_buf, p, carried, plane_re, plane_im)

    carried = lax.fori_loop(0, plane, join_plane, (zero, zero, one))
    carried = lax.fori_loop(0, place, join_place, carried)

    def record(t, carried):
        f_re, f_im, s_re, s_im = carried
        f_re, f_im, _, row = step(t, f_re, f_im)
        states[row, :128] = f_re
        states[row, 128:] = f_im
        s_re, s_im, _, row = step(t + HALF, s_re, s_im)
        states[row, :128] = s_re
        states[row, 128:] = s_im
        return f_re, f_im, s_re, s_im

    later_re, later_im = times(first_decay * half_re, first_decay * half_im, carried[0], carried[1])
    lax.fori_loop(
        0,
        HALF,
        record,
        (carried[0], carried[1], later_re + first_re, later_im + first_im),
        unroll=8,
    )

    def read(k, _):
        at = pl.ds(pl.multiple_of(k * 1024, 1024), 1024)
        product = lax.dot_general(
            states[at, :].astype(jnp.bfloat16),
            read_w[...],
            (((1,), (1,)), ((), ())),
            preferred_element_type=jnp.float32,
        )
        drive_re[at, :] = product[:, :128]
        drive_im[at, :] = product[:, 128:]
        return 0

    lax.fori_loop(0, 2, read, 0)
    lane = lax.broadcasted_iota(jnp.int32, (TOKENS, 128), 1)
    for side, buf in ((0, drive_re), (1, drive_im)):
        picked = jnp.zeros((TOKENS, 128), jnp.float32)
        for j in range(4):
            value = buf[pl.ds(side * 4 + j, TOKENS, stride=8), :]
            picked = jnp.where(lax.div(lane, 32) == j, value, picked)
        skip = jnp.concatenate([skip_ref[g : g + 1, :] for g in range(side * 8, side * 8 + 8)], axis=1)
        lanes = slice(side * 128, side * 128 + 128)
        read_out = picked + skip * x_ref[:, lanes].astype(jnp.float32)
        mixed[:, lanes] = jax.nn.gelu(read_out).astype(jnp.bfloat16)

    def tp_copy(k):
        peer = lax.rem(tp + k, TP)
        rows = pl.ds(pl.multiple_of(peer * ROWS, ROWS), ROWS)
        return remote(mixed.at[rows, :], whole.at[tp], tp_send.at[k], tp_recv.at[tp], tp=peer)

    def send_tp(k, _):
        tp_copy(k).start()
        return 0

    def tp_arrived(k, _):
        source = lax.rem(tp + k, TP)
        rows = pl.ds(pl.multiple_of(tp * ROWS, ROWS), ROWS)
        remote(mixed.at[rows, :], whole.at[source], tp_send.at[k], tp_recv.at[source], tp=source).wait_recv()
        return 0

    lax.fori_loop(1, TP, send_tp, 0)
    whole[tp] = mixed[pl.ds(pl.multiple_of(tp * ROWS, ROWS), ROWS), :]

    def twin_copy(block, piece, slot):
        return remote(
            gathered.at[block, piece, :],
            gathered.at[block, piece, :],
            twin_send.at[slot],
            twin_recv.at[slot],
            sp=twin,
        )

    from_left_lo = ring(left, piece_lo, 0, 0)
    from_right_hi = ring(right, piece_hi, 1, 1)
    from_left_hi = ring(left, piece_hi, 0, 2)
    from_right_lo = ring(right, piece_lo, 1, 3)
    from_left_lo.wait_recv()
    pass_right = ring(left, piece_lo, 0, 4)
    pass_right.start()
    from_right_hi.wait_recv()
    pass_left = ring(right, piece_hi, 1, 5)
    pass_left.start()
    twin_left_lo = twin_copy(left, piece_lo, 0)
    twin_right_hi = twin_copy(right, piece_hi, 1)
    twin_left_lo.start()
    twin_right_hi.start()
    from_left_hi.wait_recv()
    from_right_lo.wait_recv()
    twin_left_hi = twin_copy(left, piece_hi, 2)
    twin_right_lo = twin_copy(right, piece_lo, 3)
    twin_left_hi.start()
    twin_right_lo.start()

    lax.fori_loop(1, TP, tp_arrived, 0)

    for p in (3, 5, 2, 6):
        for piece in range(TP):
            lanes = slice(piece * 256, (piece + 1) * 256)
            mixed_out[p * PLANE : (p + 1) * PLANE, :, lanes] = blocks(p, whole[piece])
        lax.fori_loop(p * PLANE, (p + 1) * PLANE, send_mixed, 0)

    def hidden_of(pieces, residual_rows):
        squares = jnp.zeros((ROWS, 1), jnp.float32)
        mix = jnp.zeros((ROWS, WIDTH), jnp.float32)
        for q in range(TP):
            rows = pieces[q].astype(jnp.float32)
            squares += jnp.sum(rows * rows, axis=1, keepdims=True)
            scaled = (rows * gain_ref[:, q * 256 : (q + 1) * 256]).astype(jnp.bfloat16)
            mix += jnp.dot(scaled, gathered[q], preferred_element_type=jnp.float32)
        inverse = lax.rsqrt(squares / MIX_WIDTH + 1e-06)
        mix = deep_alpha * residual_rows.astype(jnp.float32) + mix * inverse
        return layer_norm(mix, mix_gain_ref[...]).astype(jnp.bfloat16)

    across_lo = ring(across, piece_lo, 0, 4)
    across_hi = ring(across, piece_hi, 1, 5)
    across_lo.wait_recv()
    twin_across_lo = twin_copy(across, piece_lo, 4)
    twin_across_lo.start()
    across_hi.wait_recv()
    twin_across_hi = twin_copy(across, piece_hi, 5)
    twin_across_hi.start()

    other = 2 * PIECE - half
    other_lo = pl.ds(pl.multiple_of(other, PIECE), PIECE)
    other_hi = pl.ds(pl.multiple_of(other + PIECE, PIECE), PIECE)
    for slot, (block, piece) in enumerate(
        (
            (left, other_lo),
            (right, other_hi),
            (left, other_hi),
            (right, other_lo),
            (across, other_lo),
            (across, other_hi),
        )
    ):
        twin_copy(block, piece, slot).wait_recv()
    hidden_buf[...] = hidden_of([whole[q] for q in range(TP)], residual_ref[...])

    for p in (4, 1, 7, 0):
        outgoing[p * PLANE : (p + 1) * PLANE] = blocks(p, hidden_buf[...])
        lax.fori_loop(p * PLANE + (p == 0), (p + 1) * PLANE, send_out, 0)
    arrived[0] = outgoing[0]

    for load in loads[15:]:
        load.wait()

    def rows_of(buf, far, near):
        size = PLANE * CAPACITY
        return jnp.concatenate(
            [buf[pl.ds(far, PLANE)].reshape(size, -1), buf[pl.ds(near, PLANE)].reshape(size, -1)], axis=0
        )

    def expert(far, near, is_far):
        near_first = jnp.maximum(near, 1)

        def out_arrived(k, _):
            out_copy(k).wait_recv()
            return 0

        def mixed_arrived(k, _):
            mixed_copy(k).wait_recv()
            return 0

        def send_back(k, _):
            back_copy(k).start()
            return 0

        lax.fori_loop(far, far + PLANE, out_arrived, 0)
        lax.fori_loop(near_first, near + PLANE, out_arrived, 0)
        rows = rows_of(arrived, far, near)
        if is_far:
            lax.fori_loop(far, far + PLANE, mixed_arrived, 0)
            lax.fori_loop(near, near + PLANE, mixed_arrived, 0)
            mixed_rows = rows_of(mixed_in, far, near)
            rows = hidden_of([mixed_rows[:, q * 256 : (q + 1) * 256] for q in range(TP)], rows)
        gate_act = jnp.dot(rows, gate[...], preferred_element_type=jnp.float32)
        up_act = jnp.dot(rows, up[...], preferred_element_type=jnp.float32)
        active = (jax.nn.silu(gate_act) * up_act).astype(jnp.bfloat16)
        result = jnp.dot(active, down[...], preferred_element_type=jnp.float32).astype(jnp.bfloat16)
        produced[pl.ds(far, PLANE)] = result[: PLANE * CAPACITY].reshape(PLANE, CAPACITY, WIDTH)
        produced[pl.ds(near, PLANE)] = result[PLANE * CAPACITY :].reshape(PLANE, CAPACITY, WIDTH)
        lax.fori_loop(far, far + PLANE, send_back, 0)
        lax.fori_loop(near_first, near + PLANE, send_back, 0)

    def far_expert(c, _):
        expert((5 + c) * PLANE, (3 - c) * PLANE, True)
        return 0

    def near_expert(c, _):
        expert((4 + 3 * c) * PLANE, c * PLANE, False)
        return 0

    lax.fori_loop(0, 2, far_expert, 0)
    lax.fori_loop(0, 2, near_expert, 0)
    returned[0] = produced[0]

    def out_left(k, _):
        out_copy(k).wait_send()
        back_copy(k).wait_send()
        return 0

    def mixed_left(k, _):
        mixed_copy(k).wait_send()
        return 0

    lax.fori_loop(1, EXPERTS, out_left, 0)
    for p in (2, 3, 5, 6):
        lax.fori_loop(p * PLANE, (p + 1) * PLANE, mixed_left, 0)

    def plane_left(k, _):
        plane_copy(k).wait_send()
        return 0

    def column_left(p, _):
        column_copy(p).wait_send()
        return 0

    def tp_left(k, _):
        tp_copy(k).wait_send()
        return 0

    lax.fori_loop(1, PLANE, plane_left, 0)
    lax.fori_loop(plane + 1, PLANES, column_left, 0)
    lax.fori_loop(1, TP, tp_left, 0)
    for copy in (to_right_lo, to_left_hi, to_right_hi, to_left_lo, pass_right, pass_left):
        copy.wait_send()
    for copy in (twin_left_lo, twin_right_hi, twin_left_hi, twin_right_lo, twin_across_lo, twin_across_hi):
        copy.wait_send()

    def back_arrived(k, _):
        back_copy(k).wait_recv()
        return 0

    lax.fori_loop(1, EXPERTS, back_arrived, 0)
    both = jnp.dot(
        combine_hi[...], returned[...].reshape(SLOTS, WIDTH), preferred_element_type=jnp.float32
    )
    expert_mix = both[:ROWS] + both[ROWS:]
    final = layer_norm(deep_alpha * hidden_buf[...].astype(jnp.float32) + expert_mix, final_gain_ref[...])
    layer_ref[...] = final.astype(jnp.bfloat16)


def local(
    mixer_input,
    retention,
    decay_real,
    decay_freq,
    log_step,
    input_real,
    input_imag,
    readout_real,
    readout_imaginary,
    skip_weight,
    norm_gain,
    projection,
    residual,
    mix_gain,
    routes,
    route_weight,
    expert_gate,
    expert_up,
    expert_down,
    final_gain,
):
    hbm = pl.BlockSpec(memory_space=pltpu.HBM)
    smem = pl.BlockSpec(memory_space=pltpu.SMEM)
    vmem = pl.BlockSpec(memory_space=pltpu.VMEM)
    f32 = jnp.float32
    bf16 = jnp.bfloat16
    dma = pltpu.SemaphoreType.DMA
    small = (
        mixer_input,
        retention,
        decay_real,
        decay_freq,
        jnp.transpose(input_real, (0, 2, 1)),
        jnp.transpose(input_imag, (0, 2, 1)),
        readout_real,
        readout_imaginary,
        skip_weight,
        norm_gain.reshape(1, -1),
        residual,
        mix_gain.reshape(1, -1),
        jnp.transpose(routes),
        jnp.transpose(route_weight),
        final_gain.reshape(1, -1),
    )
    large = (projection, expert_gate, expert_up, expert_down)
    return pl.pallas_call(
        layer_kernel,
        out_shape=pltpu.VMEM((ROWS, WIDTH), bf16),
        in_specs=[smem] + [hbm] * (len(small) + len(large)),
        out_specs=vmem,
        scratch_shapes=[pltpu.VMEM(a.shape, a.dtype) for a in small]
        + [
            pltpu.VMEM((WIDTH, HIDDEN), bf16),
            pltpu.VMEM((WIDTH, HIDDEN), bf16),
            pltpu.VMEM((HIDDEN, WIDTH), bf16),
            pltpu.VMEM((8, 256, 256), bf16),
            pltpu.VMEM((256, 256), bf16),
            pltpu.VMEM((TOKENS * 8, 128), f32),
            pltpu.VMEM((TOKENS * 8, 128), f32),
            pltpu.VMEM((TOKENS * 8, 128), f32),
            pltpu.VMEM((TOKENS * 8, 256), f32),
            pltpu.VMEM((3, 8, 128), f32),
            pltpu.VMEM((PLANE, 3, 8, 128), f32),
            pltpu.VMEM((3, 8, 128), f32),
            pltpu.VMEM((PLANES, 3, 8, 128), f32),
            pltpu.VMEM((TOKENS, 256), bf16),
            pltpu.VMEM((TP, ROWS, 256), bf16),
            pltpu.VMEM((TP, 256, WIDTH), bf16),
            pltpu.VMEM((2, GROUPS, STATE), f32),
            pltpu.VMEM((ROWS, WIDTH), bf16),
            pltpu.VMEM((2 * ROWS, SLOTS), bf16),
            pltpu.VMEM((SLOTS, ROWS), bf16),
            pltpu.VMEM((EXPERTS, CAPACITY, MIX_WIDTH), bf16),
            pltpu.VMEM((EXPERTS, CAPACITY, MIX_WIDTH), bf16),
            pltpu.VMEM((EXPERTS, CAPACITY, WIDTH), bf16),
            pltpu.VMEM((EXPERTS, CAPACITY, WIDTH), bf16),
            pltpu.VMEM((EXPERTS, CAPACITY, WIDTH), bf16),
            pltpu.VMEM((EXPERTS, CAPACITY, WIDTH), bf16),
            dma((18,)),
            dma((PLANE,)),
            dma((PLANE,)),
            dma((PLANES,)),
            dma((PLANES,)),
            dma((TP,)),
            dma((TP,)),
            dma(()),
            dma((6,)),
            dma((6,)),
            dma((6,)),
            dma((6,)),
            dma((EXPERTS,)),
            dma((EXPERTS,)),
            dma((EXPERTS,)),
            dma((EXPERTS,)),
            dma((EXPERTS,)),
            dma((EXPERTS,)),
        ],
        compiler_params=pltpu.CompilerParams(
            collective_id=0, has_side_effects=True, vmem_limit_bytes=62 * 1024 * 1024
        ),
        name="layer",
    )(log_step, *small, *large)


def solution(mesh):
    in_specs = (
        P("sp", "tp"),
        P("tp", "sp"),
        P("tp", None),
        P("tp", None),
        P("tp"),
        P("tp", None, None),
        P("tp", None, None),
        P("tp", None, None),
        P("tp", None, None),
        P("tp", None),
        P(),
        P("tp", None),
        P(("sp", "tp"), None),
        P(),
        P(("sp", "tp"), None),
        P(("sp", "tp"), None),
        P("sp", None, None),
        P("sp", None, None),
        P("sp", None, None),
        P(),
    )
    out_specs = P(("sp", "tp"), None)
    return jax.shard_map(local, mesh=mesh, in_specs=in_specs, out_specs=out_specs, check_vma=False)
```
